128 devices in a mesh: sp: 64 (over z, y, x), tp: 2 (over core).
Axes of the slice: x: 4, y: 4, z: 4, core: 2. Of those that a mesh axis runs over, the one named last changes fastest.
Arguments:
- mixer_output: bfloat16 [8192, 2048], P('sp'), may hold values from -6 to 6
- layer_cotangent: bfloat16 [8192, 2048], P('sp'), may hold values from -16 to 16
- expert_choice: int32 [8192, 2], P('sp'), may hold values from 0 to 63, all different within a row; in each aligned block of 128 rows (0 to 127, 128 to 255, ...) at most 8 rows name the same one
- route_weight: float32 [8192, 2], P('sp'), may hold values from 0.1 to 0.9
- gate_pre: bfloat16 [64, 512, 1024], P('sp', None, 'tp'), may hold values from -15 to 15
- up_pre: bfloat16 [64, 512, 1024], P('sp', None, 'tp'), may hold values from -15 to 15
- w_gate: bfloat16 [64, 2048, 1024], P('sp', None, 'tp'), may hold values from -0.125 to 0.125
- w_up: bfloat16 [64, 2048, 1024], P('sp', None, 'tp'), may hold values from -0.125 to 0.125
- w_down: bfloat16 [64, 1024, 2048], P('sp', 'tp'), may hold values from -0.1875 to 0.1875
- w_out: bfloat16 [2048, 2048], P('tp'), may hold values from -0.125 to 0.125
- norm_gain: bfloat16 [2048], P('tp'), may hold values from 0.099609375 to 1.8984375
- scan_in: bfloat16 [8192, 2048], P('sp', 'tp'), may hold values from -6 to 6
- gate_in: bfloat16 [8192, 2048], P('sp', 'tp'), may hold values from -9 to 9
- b_proj: bfloat16 [8192, 1024], P('sp', 'tp'), may hold values from -1.796875 to 1.796875
- c_proj: bfloat16 [8192, 1024], P('sp', 'tp'), may hold values from -1.796875 to 1.796875
- log_decay: float32 [8192, 32], P('sp', 'tp'), may hold values from -3 to 0
- entry_state: float32 [64, 32, 64, 128], P('sp', 'tp'), may hold values from -24 to 24
Outputs:
- grad_w_gate: bfloat16 [64, 2048, 1024], P('sp', None, 'tp')
- grad_w_up: bfloat16 [64, 2048, 1024], P('sp', None, 'tp')
- grad_w_down: bfloat16 [64, 1024, 2048], P('sp', 'tp')
- grad_out_proj: float32 [2048, 2048], P('sp', 'tp')
- grad_scan_in: bfloat16 [8192, 2048], P('sp', 'tp')
- grad_gate_in: bfloat16 [8192, 2048], P('sp', 'tp')
- grad_b_proj: bfloat16 [8192, 1024], P('sp', 'tp')
- grad_c_proj: bfloat16 [8192, 1024], P('sp', 'tp')
- grad_log_decay: float32 [8192, 32], P('sp', 'tp')
The draws below stay inside these ranges and needn't reach their ends.
Inputs may be any that keep to these rules, and one draw needn't show every extreme that they name: `expert_choice`: in the 128 rows of one device no expert is named more than 8 times, a bound that some blocks reach; the 2 entries of a row differ.
All inputs are finite; a program needn't handle non-finite values.
Results may differ from the reference program's by a relative error of at most 0.012.
Values may be sent and summed in bfloat16 or wider, within the bound.
No kernel may reach another device: no remote copies, remote signals or barrier semaphores. Data moves between devices by JAX's collectives and lax.ppermute only.
A program may use at most 192 MiB of HBM per device.

```python
import math
from functools import partial
import jax
import jax.numpy as jnp
import numpy as np
from jax import lax

D = 2048
MIXER_HEADS = 32
HEAD_DIM = 64
GROUPS = 8
STATE = 128
FF = 1024
TOPK = 2
TOK_DEV = 128
SEQUENCE_TOKENS = 8192
EXPERTS = 64
INNER = 2048
CAP = 8
EXPERT_ROWS = 512
N_SP = 64
N_TP = 2


def draw_log_decay(key, part):
    random_keys_split = jax.random.split(key, 7)
    fast_share = 0.5
    is_fast = jax.random.uniform(random_keys_split[0], (MIXER_HEADS,)) < fast_share
    fast_rate = jax.random.uniform(random_keys_split[1], (MIXER_HEADS,), minval=1.0 / 100.0, maxval=1.0 / 30.0)
    slow_rate = jax.random.uniform(random_keys_split[2], (MIXER_HEADS,), minval=0.05, maxval=0.3) * math.log(10.0) / SEQUENCE_TOKENS
    base_rate = jnp.where(is_fast, fast_rate, slow_rate)
    block_count = SEQUENCE_TOKENS // TOK_DEV
    block_factor = jnp.exp(jax.random.uniform(random_keys_split[3], (block_count, 1, MIXER_HEADS), minval=math.log(0.5), maxval=math.log(2.0)))
    token_factor = jnp.exp(jax.random.uniform(random_keys_split[4], (block_count, TOK_DEV, MIXER_HEADS), minval=math.log(0.5), maxval=math.log(2.0)))
    decay_rate_table = (base_rate[None, None, :] * block_factor * token_factor).reshape(SEQUENCE_TOKENS, MIXER_HEADS)
    spike_positions = jax.random.randint(random_keys_split[5], (3, MIXER_HEADS), 0, SEQUENCE_TOKENS)
    spike_length = jnp.log(jax.random.uniform(random_keys_split[6], (3, MIXER_HEADS), minval=0.5, maxval=0.8))
    token_locations = jnp.arange(SEQUENCE_TOKENS)[:, None]
    spike_events = jnp.zeros((SEQUENCE_TOKENS, MIXER_HEADS), jnp.float32)
    for event_count in range(3):
        spike_events = spike_events + jnp.where(token_locations == spike_positions[event_count][None, :], spike_length[event_count][None, :], 0.0)
    return (spike_events - decay_rate_table).astype(jnp.float32)


def raised(drawn, rng, source, target, parts, factor):
    owner, partner = [(jnp.arange(drawn.shape[dim]) // (drawn.shape[dim] // parts)).reshape([-1 if axis == dim else 1 for axis in range(drawn.ndim)]) for dim in (source, target)]
    chosen = jax.random.permutation(rng, parts)[partner]
    strong = (owner == chosen) | (owner == (partner + parts // 2) % parts)
    return jnp.where(strong, factor * drawn, drawn)


def steps_of(key, extent, shards, low, top_value):
    loudness, own = 1.0, jax.random.fold_in(key, 6)
    for dim, blocks in shards:
        draws = jnp.exp(jax.random.uniform(jax.random.fold_in(own, dim), (blocks,), jnp.float32, low / len(shards), top_value / len(shards)))
        loudness = loudness * jnp.repeat(draws, extent[dim] // blocks).reshape([-1 if axis == dim else 1 for axis in range(len(extent))])
    return loudness


def shared_out(own_key, own, number, rows, count, top, most, lean):
    ranking = jax.random.permutation(own_key, count)
    crowded, usual = load_shares(count, rows * top, most, lean, True), load_shares(count, rows * top, most, lean, False)
    places = jnp.arange(count)

    def named(sizes, offset_by):
        used = int((sizes > 0).sum())
        fixed = max(1, used // 4)
        shifted = fixed + (places - fixed + offset_by * (used - fixed)) % max(1, count - fixed)
        return jnp.zeros((count,), jnp.int32).at[ranking[jnp.where(places < fixed, places, shifted)]].set(jnp.asarray(sizes, jnp.int32))

    sizes = jnp.where(number % 4 == 0, named(crowded, number // 4), named(usual, number - number // 4 - 1))
    mixed = jax.random.permutation(jax.random.fold_in(own, 3), count)
    giver, sink = mixed[0:count // 2 * 2:2], mixed[1:count // 2 * 2:2]
    room = jnp.minimum(sizes[giver] - 1, most - sizes[sink]) // 2
    room = jnp.where((giver == ranking[0]) | (sink == ranking[0]) | (sizes[sink] == 0), 0, jnp.maximum(room, 0))
    shifted = jax.random.randint(jax.random.fold_in(own, 4), (count // 2,), 0, 1 << 20) % (room + 1)
    sizes = sizes.at[giver].add(-shifted).at[sink].add(shifted)
    items = jnp.searchsorted(jnp.cumsum(sizes), jnp.arange(rows * top), side="right").astype(jnp.int32)
    listing = items.reshape(top, rows).T
    listing = listing[jax.random.permutation(jax.random.fold_in(own, 1), rows)]
    offset_by = jax.random.randint(jax.random.fold_in(own, 2), (rows, 1), 0, top)
    return jnp.take_along_axis(listing, (jnp.arange(top)[None, :] + offset_by) % top, axis=1)


def load_shares(number_of, total, most, skew, full):
    portions = [(1 << 20) // math.isqrt(grade ** skew) + 1 for grade in range(1, number_of + 1)]
    largest = most if full else min(most, max(-(-total // number_of), total * portions[0] // sum(portions)))
    least = 1 if total - largest >= number_of - 1 else 0
    given, surplus = [largest] + [least] * (number_of - 1), total - largest - least * (number_of - 1)
    while surplus > 0:
        candidates = [i for i in range(1, number_of) if given[i] < largest] or [i for i in range(1, number_of) if given[i] < most]
        whole, remaining = sum([portions[i] for i in candidates]), surplus
        for i in candidates:
            extra = min(most - given[i], max(1, remaining * portions[i] // whole), surplus)
            given[i] = given[i] + extra
            surplus = surplus - extra
    return np.array(given)


def normal_values(stream_key, dims, deviation, reach, cuts=(), kind=jnp.bfloat16):
    drawn = deviation * jax.random.normal(stream_key, dims, jnp.float32)
    if cuts:
        drawn = drawn * steps_of(stream_key, dims, cuts, -0.22, 0.18)
    return jnp.clip(drawn, -reach, reach).astype(kind)


def bell_draw_with(own_key, extent, spread, bound, cuts, heavy, kind=jnp.bfloat16):
    values = spread * jax.random.normal(own_key, extent, jnp.float32)
    if cuts:
        values = values * steps_of(own_key, extent, cuts, -0.22, 0.18)
    return jnp.clip(raised(values, jax.random.fold_in(own_key, 3), *heavy), -bound, bound).astype(kind)


def setup_inputs(seed: int = 0) -> dict:
    streams_of = jax.random.split(jax.random.key(seed), 18)
    mixer_output = normal_values(streams_of[0], (SEQUENCE_TOKENS, D), 1.0, 6.0, ((0, 64),))
    layer_cotangent = bell_draw_with(streams_of[1], (SEQUENCE_TOKENS, D), 1.0, 16.0, ((0, 64),), (0, 1, 64, 4.0))
    expert_choice_keys = jax.random.split(jax.random.fold_in(streams_of[2], 1), SEQUENCE_TOKENS // TOK_DEV)
    expert_choice_turns = jax.random.permutation(jax.random.fold_in(streams_of[2], 3), SEQUENCE_TOKENS // TOK_DEV)
    expert_choice = jax.vmap(lambda own, number: shared_out(jax.random.fold_in(streams_of[2], 2), own, number, TOK_DEV, EXPERTS, TOPK, CAP, 1))(expert_choice_keys, expert_choice_turns).reshape((SEQUENCE_TOKENS, TOPK))
    route_weight = jnp.clip(0.1 + 0.79999997 * jax.random.uniform(streams_of[3], (SEQUENCE_TOKENS, TOPK), jnp.float32) ** steps_of(streams_of[3], (SEQUENCE_TOKENS, TOPK), ((0, 64),), -0.2, 0.2), 0.1, 0.9)
    gate_pre = normal_values(streams_of[4], (EXPERTS, EXPERT_ROWS, FF), 3.0, 15.0, ((0, 64), (2, 2)))
    up_pre = normal_values(streams_of[5], (EXPERTS, EXPERT_ROWS, FF), 3.0, 15.0, ((0, 64), (2, 2)))
    w_gate = normal_values(streams_of[6], (EXPERTS, D, FF), D ** -0.5, 0.125, ((0, 64), (2, 2)))
    w_up = normal_values(streams_of[7], (EXPERTS, D, FF), D ** -0.5, 0.125, ((0, 64), (2, 2)))
    w_down = normal_values(streams_of[8], (EXPERTS, FF, D), FF ** -0.5, 0.1875, ((0, 64), (1, 2)))
    w_out = normal_values(streams_of[9], (INNER, D), INNER ** -0.5, 0.125, ((0, 2),))
    norm_gain = jnp.clip(1.0 + 0.18 * jax.random.normal(streams_of[10], (INNER,), jnp.float32), 0.099609375, 1.8984375).astype(jnp.bfloat16)
    scan_in = normal_values(streams_of[11], (SEQUENCE_TOKENS, INNER), 1.0, 6.0, ((0, 64), (1, 2)))
    gate_in = normal_values(streams_of[12], (SEQUENCE_TOKENS, INNER), 1.5, 9.0, ((0, 64), (1, 2)))
    b_proj = normal_values(streams_of[13], (SEQUENCE_TOKENS, GROUPS * STATE), 0.3, 1.796875, ((0, 64), (1, 2)))
    c_proj = normal_values(streams_of[14], (SEQUENCE_TOKENS, GROUPS * STATE), 0.3, 1.796875, ((0, 64), (1, 2)))
    log_decay = draw_log_decay(jax.random.fold_in(streams_of[17], 71), 0)
    entry_state = normal_values(streams_of[16], (N_SP, MIXER_HEADS, HEAD_DIM, STATE), 4.0, 24.0, ((0, 64), (1, 2)), jnp.float32)
    return {"mixer_output": mixer_output, "layer_cotangent": layer_cotangent, "expert_choice": expert_choice, "route_weight": route_weight, "gate_pre": gate_pre, "up_pre": up_pre, "w_gate": w_gate, "w_up": w_up, "w_down": w_down, "w_out": w_out, "norm_gain": norm_gain, "scan_in": scan_in, "gate_in": gate_in, "b_proj": b_proj, "c_proj": c_proj, "log_decay": log_decay, "entry_state": entry_state}


rms_epsilon = 1e-05
clamp_limit = 7.0
swish_alpha = 1.702

def slot_ranks(expert_ids, expert_count):
    targets = expert_ids.reshape(-1)
    one_hot = (targets[:, None] == jnp.arange(expert_count, dtype=jnp.int32)[None, :]).astype(jnp.int32)
    earlier = jnp.cumsum(one_hot, axis=0) - one_hot
    return (targets, lax.optimization_barrier(jnp.sum(earlier * one_hot, axis=1)).astype(jnp.int32))

def fill_slots(rows, targets, ranked):
    buffer = jnp.zeros((N_SP, CAP, rows.shape[1]), rows.dtype)
    return buffer.at[targets, ranked].set(rows)

def pick_rows(buffer, targets, ranked):
    return buffer[targets, ranked]

def expert_ref(inputs):
    hidden_rows, grad_rows, gate_value, up_value, gate_weight, up_weight, down_weight = inputs
    act_grad = jnp.dot(grad_rows, down_weight.T, preferred_element_type=jnp.float32)
    gate_full = gate_value.astype(jnp.float32)
    up_full = up_value.astype(jnp.float32)
    gate_clip = jnp.minimum(gate_full, clamp_limit)
    up_clip = jnp.clip(up_full, -clamp_limit, clamp_limit)
    sigmoid_gate = jax.nn.sigmoid(swish_alpha * gate_clip)
    swish_gate = gate_clip * sigmoid_gate
    active = ((up_clip + 1.0) * swish_gate).astype(jnp.bfloat16)
    up_grad = jnp.where((up_full > -clamp_limit) & (up_full < clamp_limit), act_grad * swish_gate, 0.0).astype(jnp.bfloat16)
    slope = sigmoid_gate + swish_alpha * gate_clip * sigmoid_gate * (1.0 - sigmoid_gate)
    gate_grad = jnp.where(gate_full < clamp_limit, act_grad * (up_clip + 1.0) * slope, 0.0).astype(jnp.bfloat16)
    down_wgrad = jnp.dot(active.T, grad_rows, preferred_element_type=jnp.float32).astype(jnp.bfloat16)
    gate_wgrad = jnp.dot(hidden_rows.T, gate_grad, preferred_element_type=jnp.float32).astype(jnp.bfloat16)
    up_wgrad = jnp.dot(hidden_rows.T, up_grad, preferred_element_type=jnp.float32).astype(jnp.bfloat16)
    row_count = gate_grad.shape[0]
    part_width = FF // N_TP
    gate_split = gate_grad.reshape(row_count, N_TP, part_width).astype(jnp.float32)
    up_split = up_grad.reshape(row_count, N_TP, part_width).astype(jnp.float32)
    gate_parts = gate_weight.reshape(D, N_TP, part_width).astype(jnp.float32)
    up_parts = up_weight.reshape(D, N_TP, part_width).astype(jnp.float32)
    partial_rows = jnp.einsum('rjf,djf->jrd', gate_split, gate_parts) + jnp.einsum('rjf,djf->jrd', up_split, up_parts)
    rounded = lax.optimization_barrier(partial_rows.astype(jnp.bfloat16))
    back_rows = lax.optimization_barrier(jnp.sum(rounded.astype(jnp.float32), axis=0)).astype(jnp.bfloat16)
    return (gate_wgrad, up_wgrad, down_wgrad, back_rows)

def block_step(carry, inputs, w_out, norm_gain):
    later_state, later_grad = carry
    scan_block, gate_block, b_block, c_block, decay_block, state_block, hidden_block = inputs
    length = scan_block.shape[0]
    per_group = MIXER_HEADS // GROUPS
    scan_heads = scan_block.reshape(length, MIXER_HEADS, HEAD_DIM).astype(jnp.float32)
    b_groups = b_block.reshape(length, GROUPS, STATE).astype(jnp.float32)
    c_groups = c_block.reshape(length, GROUPS, STATE).astype(jnp.float32)
    cumulative = jnp.cumsum(decay_block, axis=0)
    growth = jnp.exp(cumulative)
    tail_decay = jnp.exp(cumulative[-1][None, :] - cumulative)
    token_locations = jnp.arange(length)
    causal = token_locations[:, None] >= token_locations[None, :]
    log_gaps = cumulative.T[:, :, None] - cumulative.T[:, None, :]
    decay_mat = jnp.exp(jnp.where(causal[None], log_gaps, -jnp.inf))
    inner_prod = jnp.einsum('tgn,sgn->gts', c_groups, b_groups)
    mix_weights = (jnp.repeat(inner_prod, per_group, axis=0) * decay_mat).astype(jnp.bfloat16).astype(jnp.float32)
    state_groups = state_block.reshape(GROUPS, per_group, HEAD_DIM, STATE)
    y_inner = jnp.einsum('hts,shp->thp', mix_weights, scan_heads)
    y_carry = jnp.einsum('tgn,grpn->tgrp', c_groups, state_groups, precision=lax.Precision.HIGHEST).reshape(length, MIXER_HEADS, HEAD_DIM)
    scan_out = y_inner + y_carry * growth[:, :, None]
    gate_float = gate_block.astype(jnp.float32)
    gate_sig = jax.nn.sigmoid(gate_float)
    gate_silu = gate_float * gate_sig
    gated = scan_out.reshape(length, -1) * gate_silu
    grouped = gated.reshape(length, GROUPS, -1)
    inv_rms = lax.rsqrt(lax.optimization_barrier(jnp.mean(grouped * grouped, axis=-1, keepdims=True)) + rms_epsilon)
    unit = grouped * inv_rms
    gain_groups = norm_gain.astype(jnp.float32).reshape(GROUPS, -1)
    mixed = (unit * gain_groups).reshape(length, -1).astype(jnp.bfloat16)
    grad_mixed = jnp.dot(hidden_block, w_out.T, preferred_element_type=jnp.float32)
    grad_unit = grad_mixed.reshape(length, GROUPS, -1) * gain_groups
    grad_grouped = inv_rms * (grad_unit - unit * lax.optimization_barrier(jnp.mean(grad_unit * unit, axis=-1, keepdims=True)))
    grad_gated = grad_grouped.reshape(length, -1)
    grad_gate = (grad_gated * scan_out.reshape(length, -1) * gate_sig * (1.0 + gate_float * (1.0 - gate_sig))).astype(jnp.bfloat16)
    grad_y = (grad_gated * gate_silu).reshape(length, MIXER_HEADS, HEAD_DIM)
    grad_y_b = grad_y.astype(jnp.bfloat16).astype(jnp.float32)
    grad_x_inner = jnp.einsum('hts,thp->shp', mix_weights, grad_y_b)
    grad_weights = (jnp.einsum('thp,shp->hts', grad_y_b, scan_heads) * decay_mat).reshape(GROUPS, per_group, length, length).sum(axis=1)
    grad_weights = grad_weights.astype(jnp.bfloat16).astype(jnp.float32)
    grad_c_inner = jnp.einsum('gts,sgn->tgn', grad_weights, b_groups)
    grad_b_inner = jnp.einsum('gts,tgn->sgn', grad_weights, c_groups)
    grown_grads = (grad_y * growth[:, :, None]).reshape(length, GROUPS, per_group, HEAD_DIM)
    grad_c_carry = jnp.einsum('tgrp,grpn->tgn', grown_grads, state_groups, precision=lax.Precision.HIGHEST)
    block_state = jnp.einsum('tgrp,tgn->grpn', grown_grads, c_groups, precision=lax.Precision.HIGHEST).reshape(MIXER_HEADS, HEAD_DIM, STATE)
    later_groups = later_state.reshape(GROUPS, per_group, HEAD_DIM, STATE)
    grad_x_carry = jnp.einsum('sgn,grpn->sgrp', b_groups, later_groups, precision=lax.Precision.HIGHEST).reshape(length, MIXER_HEADS, HEAD_DIM)
    grad_x = grad_x_inner + grad_x_carry * tail_decay[:, :, None]
    x_tail = (scan_heads * tail_decay[:, :, None]).reshape(length, GROUPS, per_group, HEAD_DIM)
    grad_b_carry = jnp.einsum('sgrp,grpn->sgn', x_tail, later_groups, precision=lax.Precision.HIGHEST)
    grad_a = lax.optimization_barrier(jnp.sum(grad_y * scan_out, axis=2)) - lax.optimization_barrier(jnp.sum(scan_heads * grad_x, axis=2))
    grad_decay = jnp.flip(jnp.cumsum(jnp.flip(grad_a, 0), axis=0), 0) + later_grad[None, :]
    new_state = block_state + jnp.exp(cumulative[-1])[:, None, None] * later_state
    new_grad = later_grad + lax.optimization_barrier(jnp.sum(grad_a, axis=0))
    outputs = (grad_x.reshape(length, -1).astype(jnp.bfloat16), grad_gate, (grad_b_inner + grad_b_carry).reshape(length, -1).astype(jnp.bfloat16), (grad_c_inner + grad_c_carry).reshape(length, -1).astype(jnp.bfloat16), grad_decay, mixed)
    return ((new_state, new_grad), outputs)

def reference(mixer_output, layer_cotangent, expert_choice, route_weight, gate_pre, up_pre, w_gate, w_up, w_down, w_out, norm_gain, scan_in, gate_in, b_proj, c_proj, log_decay, entry_state):
    id_blocks = expert_choice.reshape(N_SP, TOK_DEV, TOPK)
    targets, ranked = jax.vmap(partial(slot_ranks, expert_count=N_SP))(id_blocks)
    token_of = jnp.arange(SEQUENCE_TOKENS * TOPK, dtype=jnp.int32) // TOPK
    hidden_rows = mixer_output[token_of].reshape(N_SP, TOK_DEV * TOPK, D)
    grad_rows = (route_weight.reshape(-1)[:, None] * layer_cotangent[token_of].astype(jnp.float32)).astype(jnp.bfloat16)
    grad_rows = grad_rows.reshape(N_SP, TOK_DEV * TOPK, D)
    send_hidden = jax.vmap(fill_slots)(hidden_rows, targets, ranked)
    send_grads = jax.vmap(fill_slots)(grad_rows, targets, ranked)
    recv_hidden = jnp.transpose(send_hidden, (1, 0, 2, 3)).reshape(N_SP, N_SP * CAP, D)
    recv_grads = jnp.transpose(send_grads, (1, 0, 2, 3)).reshape(N_SP, N_SP * CAP, D)
    gate_wgrad, up_wgrad, down_wgrad, back_rows = lax.map(expert_ref, (recv_hidden, recv_grads, gate_pre, up_pre, w_gate, w_up, w_down))
    returned = jnp.transpose(back_rows.reshape(N_SP, N_SP, CAP, D), (1, 0, 2, 3))
    picked = jax.vmap(pick_rows)(returned, targets, ranked)
    moe_terms = picked.astype(jnp.float32).reshape(SEQUENCE_TOKENS, TOPK, D).sum(axis=1)
    grad_hidden = (layer_cotangent.astype(jnp.float32) + moe_terms).astype(jnp.bfloat16)

    def blocks_of(array):
        return array.reshape((N_SP, TOK_DEV) + array.shape[1:])
    initial = (jnp.zeros((MIXER_HEADS, HEAD_DIM, STATE), jnp.float32), jnp.zeros((MIXER_HEADS,), jnp.float32))
    stepper = partial(block_step, w_out=w_out, norm_gain=norm_gain)
    block_inputs = (blocks_of(scan_in), blocks_of(gate_in), blocks_of(b_proj), blocks_of(c_proj), blocks_of(log_decay), entry_state, blocks_of(grad_hidden))
    results = lax.scan(stepper, initial, block_inputs, reverse=True)[1]
    grad_scan, grad_gate, grad_b, grad_c, grad_decay, mixed = [item.reshape((SEQUENCE_TOKENS,) + item.shape[2:]) for item in results]
    grad_out_proj = jnp.dot(grad_hidden.T, mixed, preferred_element_type=jnp.float32)
    return (gate_wgrad, up_wgrad, down_wgrad, grad_out_proj, grad_scan, grad_gate, grad_b, grad_c, grad_decay)
```

```python
import jax
import jax.numpy as jnp
from jax import lax
from jax.sharding import Mesh
from jax.sharding import PartitionSpec as P

HEAD_DIM = 64
STATE = 128
SP = ("sp_0", "sp_1", "sp_2")


rms_epsilon = 1e-05
clamp_limit = 7.0
swish_alpha = 1.702

bf16 = jnp.bfloat16
f32 = jnp.float32


def dot(a, b, dims):
    return lax.dot_general(a, b, (dims, ((), ())), preferred_element_type=f32)


def both_halves(x):
    sent = jnp.broadcast_to(x[None], (2, *x.shape))
    return lax.all_to_all(sent, "tp", 0, 0, tiled=True)


def three_parts(x):
    high = lax.reduce_precision(x, 8, 7)
    rest = x - high
    middle = lax.reduce_precision(rest, 8, 7)
    return high.astype(bf16), middle.astype(bf16), (rest - middle).astype(bf16)


def routing(expert_choice, experts, capacity):
    tokens = expert_choice.shape[0]
    hot = expert_choice[:, :, None] == jnp.arange(experts, dtype=jnp.int32)
    hot = hot.astype(f32)
    named = hot.sum(axis=1).astype(bf16)
    at = jnp.arange(tokens)
    before = (at[:, None] > at[None, :]).astype(bf16)
    earlier = dot(before, named, ((1,), (0,)))
    rank = (earlier[:, None, :] * hot).sum(axis=2).astype(jnp.int32)
    slot = expert_choice * capacity + rank
    return (slot[:, :, None] == jnp.arange(experts * capacity, dtype=jnp.int32)).astype(bf16)


def expert_side(hidden_rows, grad_rows, gate_value, up_value, gate_weight, up_weight, down_weight):
    act_grad = dot(grad_rows, down_weight, ((1,), (1,)))
    gate_full = gate_value.astype(f32)
    up_full = up_value.astype(f32)
    gate_clip = jnp.minimum(gate_full, clamp_limit)
    up_clip = jnp.clip(up_full, -clamp_limit, clamp_limit)
    sigmoid_gate = jax.nn.sigmoid(swish_alpha * gate_clip)
    swish_gate = gate_clip * sigmoid_gate
    active = ((up_clip + 1.0) * swish_gate).astype(bf16)
    up_grad = jnp.where(
        (up_full > -clamp_limit) & (up_full < clamp_limit), act_grad * swish_gate, 0.0
    ).astype(bf16)
    slope = sigmoid_gate + swish_alpha * gate_clip * sigmoid_gate * (1.0 - sigmoid_gate)
    gate_grad = jnp.where(gate_full < clamp_limit, act_grad * (up_clip + 1.0) * slope, 0.0).astype(
        bf16
    )
    down_wgrad = dot(active, grad_rows, ((0,), (0,))).astype(bf16)
    gate_wgrad = dot(hidden_rows, gate_grad, ((0,), (0,))).astype(bf16)
    up_wgrad = dot(hidden_rows, up_grad, ((0,), (0,))).astype(bf16)
    partial_rows = dot(gate_grad, gate_weight, ((1,), (1,)))
    partial_rows = partial_rows + dot(up_grad, up_weight, ((1,), (1,)))
    return (gate_wgrad, up_wgrad, down_wgrad, partial_rows)


def scan_piece(came):
    blocks = came.shape[0]
    values = came[:, :16].reshape(blocks, -1)
    local = came[:, 16:32].reshape(blocks, -1).astype(f32)
    sums = came[:, 35:38, 0].astype(f32).sum(axis=1)
    at = jnp.arange(blocks)
    after = at[None, :] > at[:, None]
    gaps = jnp.zeros((blocks, blocks), f32)
    for k in range(3):
        part = jnp.where(after, came[:, 32 + k, 0][None, :], 0).astype(bf16)
        gaps = gaps + dot(part, after.astype(bf16), ((1,), (0,)))
    weights = jnp.where(after, jnp.exp(gaps), 0.0)
    high = lax.reduce_precision(weights, 8, 7)
    low = weights - high
    later = dot(high.astype(bf16), values, ((1,), (0,))) + dot(
        low.astype(bf16), values, ((1,), (0,))
    )
    own = sums - jnp.sum(later * local, axis=1)
    carried = jnp.sum(jnp.where(after, own[None, :], 0.0), axis=1)
    return later.astype(bf16).reshape(blocks, 16, STATE), carried


def spread(parts, blocks):
    rows = jnp.stack(parts, axis=1)
    rows = jnp.pad(rows, ((0, 0), (0, 8 - len(parts))))
    return jnp.broadcast_to(rows[:, :, None], (blocks, 8, STATE)).astype(bf16)


def body(
    mixer_output,
    layer_cotangent,
    expert_choice,
    route_weight,
    gate_pre,
    up_pre,
    w_gate,
    w_up,
    w_down,
    w_out,
    norm_gain,
    scan_in,
    gate_in,
    b_proj,
    c_proj,
    log_decay,
    entry_state,
):
    experts = lax.axis_size(SP)
    tokens, width = mixer_output.shape
    capacity = gate_pre.shape[1] // experts
    half = width // 2
    start = lax.axis_index("tp") * half

    places = routing(expert_choice, experts, capacity)
    hidden_half = lax.dynamic_slice_in_dim(mixer_output, start, half, 1)
    cotangent_half = lax.dynamic_slice_in_dim(layer_cotangent, start, half, 1)
    weighted = (route_weight[:, :, None] * cotangent_half.astype(f32)[:, None, :]).astype(bf16)
    either = places[:, 0] + places[:, 1]
    send_grads = (
        dot(places[:, 0], weighted[:, 0], ((0,), (0,)))
        + dot(places[:, 1], weighted[:, 1], ((0,), (0,)))
    ).astype(bf16)
    send_hidden = dot(either, hidden_half, ((0,), (0,))).astype(bf16)
    send_grads = send_grads.reshape(experts, capacity, half)
    send_hidden = send_hidden.reshape(experts, capacity, half)
    came_grads = lax.all_to_all(send_grads, SP, 0, 0, tiled=True)
    came_hidden = lax.all_to_all(send_hidden, SP, 0, 0, tiled=True)

    def whole(x):
        x = both_halves(x.reshape(-1, half))
        return jnp.concatenate([x[0], x[1]], axis=1)

    gate_wgrad, up_wgrad, down_wgrad, partial_rows = expert_side(
        whole(came_hidden),
        whole(came_grads),
        gate_pre[0],
        up_pre[0],
        w_gate[0],
        w_up[0],
        w_down[0],
    )
    partial_rows = partial_rows.astype(bf16)
    split_rows = jnp.stack([partial_rows[:, :half], partial_rows[:, half:]])
    split_rows = lax.all_to_all(split_rows, "tp", 0, 0, tiled=True)
    summed = (split_rows[0].astype(f32) + split_rows[1].astype(f32)).astype(bf16)
    returned = lax.all_to_all(summed.reshape(experts, capacity, half), SP, 0, 0, tiled=True)
    moe_terms = dot(either, returned.reshape(-1, half), ((1,), (0,)))
    grad_half = (cotangent_half.astype(f32) + moe_terms).astype(bf16)
    grad_halves = both_halves(grad_half)
    grad_hidden = jnp.concatenate([grad_halves[0], grad_halves[1]], axis=1)

    head_count = log_decay.shape[1]
    group_count = b_proj.shape[1] // STATE
    per_group = head_count // group_count
    scan_heads = scan_in.reshape(tokens, head_count, HEAD_DIM)
    b_groups = b_proj.reshape(tokens, group_count, STATE)
    c_groups = c_proj.reshape(tokens, group_count, STATE)
    x_float = scan_heads.astype(f32)
    b_float = b_groups.astype(f32)
    c_float = c_groups.astype(f32)
    cumulative = jnp.cumsum(log_decay, axis=0)
    growth = jnp.exp(cumulative)
    tail_decay = jnp.exp(cumulative[-1][None, :] - cumulative)
    locations = jnp.arange(tokens)
    causal = locations[:, None] >= locations[None, :]
    log_gaps = cumulative.T[:, :, None] - cumulative.T[:, None, :]
    decay_mat = jnp.exp(jnp.where(causal[None], log_gaps, -jnp.inf))
    inner_prod = jnp.einsum("tgn,sgn->gts", c_groups, b_groups, preferred_element_type=f32)
    mix_weights = (jnp.repeat(inner_prod, per_group, axis=0) * decay_mat).astype(bf16)
    state_groups = entry_state.reshape(group_count, per_group, HEAD_DIM, STATE)
    y_inner = jnp.einsum("hts,shp->thp", mix_weights, scan_heads, preferred_element_type=f32)
    y_carry = jnp.einsum("tgn,grpn->tgrp", c_float, state_groups).reshape(
        tokens, head_count, HEAD_DIM
    )
    scan_out = y_inner + y_carry * growth[:, :, None]
    gate_float = gate_in.astype(f32)
    gate_sig = jax.nn.sigmoid(gate_float)
    gate_silu = gate_float * gate_sig
    gated = scan_out.reshape(tokens, -1) * gate_silu
    grouped = gated.reshape(tokens, group_count, -1)
    inv_rms = lax.rsqrt(jnp.mean(grouped * grouped, axis=-1, keepdims=True) + rms_epsilon)
    unit = grouped * inv_rms
    gain_groups = norm_gain.astype(f32).reshape(group_count, -1)
    mixed = (unit * gain_groups).reshape(tokens, -1).astype(bf16)
    x_tail = (x_float * tail_decay[:, :, None]).reshape(tokens, group_count, per_group, HEAD_DIM)
    local_state = jnp.einsum("sgrp,sgn->grpn", x_tail, b_float)

    line = lax.axis_size("sp_0")
    mixed_line = lax.all_to_all(
        jnp.broadcast_to(mixed[None], (line, *mixed.shape)), "sp_0", 0, 0, tiled=True
    )
    grads_line = lax.all_to_all(
        grad_hidden.reshape(tokens, line, -1).transpose(1, 0, 2), "sp_0", 0, 0, tiled=True
    )
    product = dot(
        grads_line.reshape(line * tokens, -1), mixed_line.reshape(line * tokens, -1), ((0,), (0,))
    ).astype(bf16)
    product = product.reshape(experts // line, -1, product.shape[1])
    grad_out_proj = (
        lax.all_to_all(product, ("sp_1", "sp_2"), 0, 0, tiled=True).astype(f32).sum(axis=0)
    )

    grad_mixed = jnp.einsum("td,id->ti", grad_hidden, w_out, preferred_element_type=f32)
    grad_unit = grad_mixed.reshape(tokens, group_count, -1) * gain_groups
    grad_grouped = inv_rms * (grad_unit - unit * jnp.mean(grad_unit * unit, axis=-1, keepdims=True))
    grad_gated = grad_grouped.reshape(tokens, -1)
    grad_gate_in = (
        grad_gated
        * scan_out.reshape(tokens, -1)
        * gate_sig
        * (1.0 + gate_float * (1.0 - gate_sig))
    ).astype(bf16)
    grad_y = (grad_gated * gate_silu).reshape(tokens, head_count, HEAD_DIM)
    grad_y_b = grad_y.astype(bf16)
    grad_x_inner = jnp.einsum("hts,thp->shp", mix_weights, grad_y_b, preferred_element_type=f32)
    grad_weights = (
        jnp.einsum("thp,shp->hts", grad_y_b, scan_heads, preferred_element_type=f32) * decay_mat
    )
    grad_weights = (
        grad_weights.reshape(group_count, per_group, tokens, tokens).sum(axis=1).astype(bf16)
    )
    grad_c_inner = jnp.einsum("gts,sgn->tgn", grad_weights, b_groups, preferred_element_type=f32)
    grad_b_inner = jnp.einsum("gts,tgn->sgn", grad_weights, c_groups, preferred_element_type=f32)
    grown_grads = (grad_y * growth[:, :, None]).reshape(tokens, group_count, per_group, HEAD_DIM)
    grad_c_carry = jnp.einsum("tgrp,grpn->tgn", grown_grads, state_groups)
    block_state = jnp.einsum("tgrp,tgn->grpn", grown_grads, c_float)
    y_dots = jnp.sum(grad_y * scan_out, axis=2)
    local_grad = jnp.sum(y_dots - jnp.sum(x_float * grad_x_inner, axis=2), axis=0)

    pieces = experts // head_count
    first = (jnp.arange(experts) % pieces == 0).astype(f32)
    scalars = [jnp.repeat(part, pieces) for part in three_parts(cumulative[-1])] + list(
        three_parts(jnp.repeat(local_grad, pieces) * first)
    )
    sent = jnp.concatenate(
        [
            block_state.astype(bf16).reshape(experts, -1, STATE),
            local_state.astype(bf16).reshape(experts, -1, STATE),
            spread(scalars, experts),
        ],
        axis=1,
    )
    later, carried = scan_piece(lax.all_to_all(sent, SP, 0, 0, tiled=True))
    back = jnp.concatenate([later, spread(list(three_parts(carried)), experts)], axis=1)
    back = lax.all_to_all(back, SP, 0, 0, tiled=True)
    later_groups = back[:, :16].reshape(group_count, per_group, HEAD_DIM, STATE).astype(f32)
    later_grad = back[:, 16:19, 0].astype(f32).sum(axis=1).reshape(head_count, pieces).sum(axis=1)

    grad_x_carry = jnp.einsum("sgn,grpn->sgrp", b_float, later_groups).reshape(
        tokens, head_count, HEAD_DIM
    )
    grad_x = grad_x_inner + grad_x_carry * tail_decay[:, :, None]
    grad_b_carry = jnp.einsum("sgrp,grpn->sgn", x_tail, later_groups)
    grad_a = y_dots - jnp.sum(x_float * grad_x, axis=2)
    grad_log_decay = jnp.flip(jnp.cumsum(jnp.flip(grad_a, 0), axis=0), 0) + later_grad[None, :]
    grad_scan_in = grad_x.reshape(tokens, -1).astype(bf16)
    grad_b_proj = (grad_b_inner + grad_b_carry).reshape(tokens, -1).astype(bf16)
    grad_c_proj = (grad_c_inner + grad_c_carry).reshape(tokens, -1).astype(bf16)
    return (
        gate_wgrad[None],
        up_wgrad[None],
        down_wgrad[None],
        grad_out_proj,
        grad_scan_in,
        grad_gate_in,
        grad_b_proj,
        grad_c_proj,
        grad_log_decay,
    )


def solution(mesh):
    split = Mesh(mesh.devices.reshape(4, 4, 4, mesh.shape["tp"]), ("sp_0", "sp_1", "sp_2", "tp"))
    return jax.shard_map(
        body,
        mesh=split,
        in_specs=(
            P(SP, None),
            P(SP, None),
            P(SP, None),
            P(SP, None),
            P(SP, None, "tp"),
            P(SP, None, "tp"),
            P(SP, None, "tp"),
            P(SP, None, "tp"),
            P(SP, "tp", None),
            P("tp", None),
            P("tp"),
            P(SP, "tp"),
            P(SP, "tp"),
            P(SP, "tp"),
            P(SP, "tp"),
            P(SP, "tp"),
            P(SP, "tp", None, None),
        ),
        out_specs=(
            P(SP, None, "tp"),
            P(SP, None, "tp"),
            P(SP, "tp", None),
            P(SP, "tp"),
            P(SP, "tp"),
            P(SP, "tp"),
            P(SP, "tp"),
            P(SP, "tp"),
            P(SP, "tp"),
        ),
        check_vma=False,
    )
```

```python
import jax
import jax.numpy as jnp
from jax import lax
from jax.sharding import Mesh
from jax.experimental import pallas as pl
from jax.experimental.pallas import tpu as pltpu
from jax.sharding import PartitionSpec as P

HEAD_DIM = 64
STATE = 128
SP = ("sp_0", "sp_1", "sp_2")


rms_epsilon = 1e-05
clamp_limit = 7.0
swish_alpha = 1.702

bf16 = jnp.bfloat16
f32 = jnp.float32


def dot(a, b, dims):
    return lax.dot_general(a, b, (dims, ((), ())), preferred_element_type=f32)


def swapped(x):
    return lax.ppermute(x, "tp", [(0, 1), (1, 0)])


def from_line(parts, axis):
    size = lax.axis_size(axis)
    return [parts[0]] + [
        lax.ppermute(parts[k], axis, [(i, (i + k) % size) for i in range(size)])
        for k in range(1, size)
    ]


def three_parts(x):
    high = lax.reduce_precision(x, 8, 7)
    rest = x - high
    middle = lax.reduce_precision(rest, 8, 7)
    return high.astype(bf16), middle.astype(bf16), (rest - middle).astype(bf16)


def routing(expert_choice, experts, capacity):
    tokens = expert_choice.shape[0]
    hot = expert_choice[:, :, None] == jnp.arange(experts, dtype=jnp.int32)
    hot = hot.astype(f32)
    named = hot.sum(axis=1).astype(bf16)
    at = jnp.arange(tokens)
    before = (at[:, None] > at[None, :]).astype(bf16)
    earlier = dot(before, named, ((1,), (0,)))
    rank = (earlier[:, None, :] * hot).sum(axis=2).astype(jnp.int32)
    slot = expert_choice * capacity + rank
    return (slot[:, :, None] == jnp.arange(experts * capacity, dtype=jnp.int32)).astype(bf16)


def expert_rows_kernel(
    side, mine, other, gate_value, up_value, down_own, down_far, gate_own, gate_far, up_own, up_far,
    active, gate_grad, up_grad, rows_own, rows_far,
):
    act_grad = dot(mine[...], down_own[...], ((1,), (1,)))
    act_grad = act_grad + dot(other[...], down_far[...], ((1,), (1,)))
    gate_full = gate_value[...].astype(f32)
    up_full = up_value[...].astype(f32)
    gate_clip = jnp.minimum(gate_full, clamp_limit)
    up_clip = jnp.clip(up_full, -clamp_limit, clamp_limit)
    sigmoid_gate = jax.nn.sigmoid(swish_alpha * gate_clip)
    swish_gate = gate_clip * sigmoid_gate
    active[...] = ((up_clip + 1.0) * swish_gate).astype(bf16)
    inside = (up_full > -clamp_limit) & (up_full < clamp_limit)
    up_side = jnp.where(inside, act_grad * swish_gate, 0.0).astype(bf16)
    slope = sigmoid_gate + swish_alpha * gate_clip * sigmoid_gate * (1.0 - sigmoid_gate)
    gate_side = jnp.where(
        gate_full < clamp_limit, act_grad * (up_clip + 1.0) * slope, 0.0
    ).astype(bf16)
    up_grad[...] = up_side
    gate_grad[...] = gate_side
    far = dot(gate_side, gate_far[...], ((1,), (1,))) + dot(up_side, up_far[...], ((1,), (1,)))
    rows_far[...] = far.astype(bf16)
    own = dot(gate_side, gate_own[...], ((1,), (1,))) + dot(up_side, up_own[...], ((1,), (1,)))
    rows_own[...] = own.astype(bf16)


def whole_block(*shape):
    return pl.BlockSpec(shape, lambda i, side: (0,) * len(shape))


def expert_rows(side, mine, other, gate_value, up_value, w_down, w_gate, w_up):
    rows, half = mine.shape
    hidden = gate_value.shape[1]
    row_block = whole_block(rows, half)
    act_block = whole_block(rows, hidden)
    down = [
        pl.BlockSpec((hidden, half), lambda i, side: (0, side[0])),
        pl.BlockSpec((hidden, half), lambda i, side: (0, 1 - side[0])),
    ]
    tall = [
        pl.BlockSpec((half, hidden), lambda i, side: (side[0], 0)),
        pl.BlockSpec((half, hidden), lambda i, side: (1 - side[0], 0)),
    ]
    act = jax.ShapeDtypeStruct((rows, hidden), bf16)
    out = jax.ShapeDtypeStruct((rows, half), bf16)
    return pl.pallas_call(
        expert_rows_kernel,
        grid_spec=pltpu.PrefetchScalarGridSpec(
            num_scalar_prefetch=1,
            grid=(1,),
            in_specs=[row_block, row_block, act_block, act_block] + down + tall + tall,
            out_specs=[act_block] * 3 + [row_block] * 2,
        ),
        out_shape=[act] * 3 + [out] * 2,
        name="expert_rows",
    )(side, mine, other, gate_value, up_value, w_down, w_down, w_gate, w_gate, w_up, w_up)


def down_kernel(side, active, mine, other, out):
    @pl.when(pl.program_id(0) == 0)
    def _():
        out[...] = dot(active[...], mine[...], ((0,), (0,))).astype(bf16)

    @pl.when(pl.program_id(0) == 1)
    def _():
        out[...] = dot(active[...], other[...], ((0,), (0,))).astype(bf16)


def tall_kernel(side, gate_grad, up_grad, mine, other, gate_out, up_out):
    def write(rows):
        gate_out[...] = dot(rows, gate_grad[...], ((0,), (0,))).astype(bf16)
        up_out[...] = dot(rows, up_grad[...], ((0,), (0,))).astype(bf16)

    @pl.when(pl.program_id(0) == 0)
    def _():
        write(mine[...])

    @pl.when(pl.program_id(0) == 1)
    def _():
        write(other[...])


def half_of(i, side):
    return lax.rem(i + side[0], 2)


def down_weights(side, active, mine, other):
    rows, half = mine.shape
    hidden = active.shape[1]
    return pl.pallas_call(
        down_kernel,
        grid_spec=pltpu.PrefetchScalarGridSpec(
            num_scalar_prefetch=1,
            grid=(2,),
            in_specs=[whole_block(rows, hidden)] + [whole_block(rows, half)] * 2,
            out_specs=pl.BlockSpec((hidden, half), lambda i, side: (0, half_of(i, side))),
        ),
        out_shape=jax.ShapeDtypeStruct((hidden, 2 * half), bf16),
        name="down_weights",
    )(side, active, mine, other)


def tall_weights(side, gate_grad, up_grad, mine, other):
    rows, half = mine.shape
    hidden = gate_grad.shape[1]
    return pl.pallas_call(
        tall_kernel,
        grid_spec=pltpu.PrefetchScalarGridSpec(
            num_scalar_prefetch=1,
            grid=(2,),
            in_specs=[whole_block(rows, hidden)] * 2 + [whole_block(rows, half)] * 2,
            out_specs=[pl.BlockSpec((half, hidden), lambda i, side: (half_of(i, side), 0))] * 2,
        ),
        out_shape=[jax.ShapeDtypeStruct((2 * half, hidden), bf16)] * 2,
        name="tall_weights",
    )(side, gate_grad, up_grad, mine, other)


def scan_piece(came):
    blocks = came.shape[0]
    values = came[:, :16].reshape(blocks, -1)
    local = came[:, 16:32].reshape(blocks, -1).astype(f32)
    sums = came[:, 35:38, 0].astype(f32).sum(axis=1)
    at = jnp.arange(blocks)
    after = at[None, :] > at[:, None]
    gaps = jnp.zeros((blocks, blocks), f32)
    for k in range(3):
        part = jnp.where(after, came[:, 32 + k, 0][None, :], 0).astype(bf16)
        gaps = gaps + dot(part, after.astype(bf16), ((1,), (0,)))
    weights = jnp.where(after, jnp.exp(gaps), 0.0)
    high = lax.reduce_precision(weights, 8, 7)
    low = weights - high
    later = dot(high.astype(bf16), values, ((1,), (0,))) + dot(
        low.astype(bf16), values, ((1,), (0,))
    )
    own = sums - jnp.sum(later * local, axis=1)
    carried = jnp.sum(jnp.where(after, own[None, :], 0.0), axis=1)
    return later.astype(bf16).reshape(blocks, 16, STATE), carried


def spread(parts, blocks):
    rows = jnp.stack(parts, axis=1)
    rows = jnp.pad(rows, ((0, 0), (0, 8 - len(parts))))
    return jnp.broadcast_to(rows[:, :, None], (blocks, 8, STATE)).astype(bf16)


def body(
    mixer_output,
    layer_cotangent,
    expert_choice,
    route_weight,
    gate_pre,
    up_pre,
    w_gate,
    w_up,
    w_down,
    w_out,
    norm_gain,
    scan_in,
    gate_in,
    b_proj,
    c_proj,
    log_decay,
    entry_state,
):
    experts = lax.axis_size(SP)
    tokens, width = mixer_output.shape
    capacity = gate_pre.shape[1] // experts
    half = width // 2
    start = lax.axis_index("tp") * half

    places = routing(expert_choice, experts, capacity)
    hidden_half = lax.dynamic_slice_in_dim(mixer_output, start, half, 1)
    cotangent_half = lax.dynamic_slice_in_dim(layer_cotangent, start, half, 1)
    weighted = (route_weight[:, :, None] * cotangent_half.astype(f32)[:, None, :]).astype(bf16)
    either = places[:, 0] + places[:, 1]
    send_grads = (
        dot(places[:, 0], weighted[:, 0], ((0,), (0,)))
        + dot(places[:, 1], weighted[:, 1], ((0,), (0,)))
    ).astype(bf16)
    send_hidden = dot(either, hidden_half, ((0,), (0,))).astype(bf16)
    send_grads = send_grads.reshape(experts, capacity, half)
    send_hidden = send_hidden.reshape(experts, capacity, half)
    came_grads = lax.all_to_all(send_grads, SP, 0, 0, tiled=True)
    send_hidden, came_grads = lax.optimization_barrier((send_hidden, came_grads))
    came_hidden = lax.all_to_all(send_hidden, SP, 0, 0, tiled=True)
    grads_own = came_grads.reshape(-1, half)
    grads_far = swapped(grads_own)
    side = lax.axis_index("tp")[None]
    active, gate_grad, up_grad, rows_own, rows_far = expert_rows(
        side, grads_own, grads_far, gate_pre[0], up_pre[0], w_down[0], w_gate[0], w_up[0]
    )
    summed = (rows_own.astype(f32) + swapped(rows_far).astype(f32)).astype(bf16)
    summed, came_hidden = lax.optimization_barrier((summed, came_hidden))
    returned = lax.all_to_all(summed.reshape(experts, capacity, half), SP, 0, 0, tiled=True)
    hidden_own = came_hidden.reshape(-1, half)
    hidden_far = swapped(hidden_own)
    down_wgrad = down_weights(side, active, grads_own, grads_far)
    gate_wgrad, up_wgrad = tall_weights(side, gate_grad, up_grad, hidden_own, hidden_far)
    moe_terms = dot(either, returned.reshape(-1, half), ((1,), (0,)))
    grad_own = (cotangent_half.astype(f32) + moe_terms).astype(bf16)
    grad_far = swapped(grad_own)
    grad_hidden = jnp.where(
        side == 0,
        jnp.concatenate([grad_own, grad_far], axis=1),
        jnp.concatenate([grad_far, grad_own], axis=1),
    )

    head_count = log_decay.shape[1]
    group_count = b_proj.shape[1] // STATE
    per_group = head_count // group_count
    scan_heads = scan_in.reshape(tokens, head_count, HEAD_DIM)
    b_groups = b_proj.reshape(tokens, group_count, STATE)
    c_groups = c_proj.reshape(tokens, group_count, STATE)
    x_float = scan_heads.astype(f32)
    b_float = b_groups.astype(f32)
    c_float = c_groups.astype(f32)
    cumulative = jnp.cumsum(log_decay, axis=0)
    growth = jnp.exp(cumulative)
    tail_decay = jnp.exp(cumulative[-1][None, :] - cumulative)
    locations = jnp.arange(tokens)
    causal = locations[:, None] >= locations[None, :]
    log_gaps = cumulative.T[:, :, None] - cumulative.T[:, None, :]
    decay_mat = jnp.exp(jnp.where(causal[None], log_gaps, -jnp.inf))
    inner_prod = jnp.einsum("tgn,sgn->gts", c_groups, b_groups, preferred_element_type=f32)
    mix_weights = (jnp.repeat(inner_prod, per_group, axis=0) * decay_mat).astype(bf16)
    state_groups = entry_state.reshape(group_count, per_group, HEAD_DIM, STATE)
    y_inner = jnp.einsum("hts,shp->thp", mix_weights, scan_heads, preferred_element_type=f32)
    y_carry = jnp.einsum("tgn,grpn->tgrp", c_float, state_groups).reshape(
        tokens, head_count, HEAD_DIM
    )
    scan_out = y_inner + y_carry * growth[:, :, None]
    gate_float = gate_in.astype(f32)
    gate_sig = jax.nn.sigmoid(gate_float)
    gate_silu = gate_float * gate_sig
    gated = scan_out.reshape(tokens, -1) * gate_silu
    grouped = gated.reshape(tokens, group_count, -1)
    inv_rms = lax.rsqrt(jnp.mean(grouped * grouped, axis=-1, keepdims=True) + rms_epsilon)
    unit = grouped * inv_rms
    gain_groups = norm_gain.astype(f32).reshape(group_count, -1)
    mixed = (unit * gain_groups).reshape(tokens, -1).astype(bf16)
    x_tail = (x_float * tail_decay[:, :, None]).reshape(tokens, group_count, per_group, HEAD_DIM)
    local_state = jnp.einsum("sgrp,sgn->grpn", x_tail, b_float)

    line = lax.axis_size("sp_0")
    spot = lax.axis_index("sp_0")
    span = width // line
    mixed_line = from_line([mixed] * line, "sp_0")
    grads_line = from_line(
        [
            lax.dynamic_slice_in_dim(grad_hidden, lax.rem(spot + k, line) * span, span, 1)
            for k in range(line)
        ],
        "sp_0",
    )
    product = dot(
        jnp.concatenate(grads_line, axis=0), jnp.concatenate(mixed_line, axis=0), ((0,), (0,))
    ).astype(bf16)
    product = product.reshape(experts // line, -1, product.shape[1])
    grad_out_proj = (
        lax.all_to_all(product, ("sp_1", "sp_2"), 0, 0, tiled=True).astype(f32).sum(axis=0)
    )

    grad_mixed = jnp.einsum("td,id->ti", grad_hidden, w_out, preferred_element_type=f32)
    grad_unit = grad_mixed.reshape(tokens, group_count, -1) * gain_groups
    grad_grouped = inv_rms * (grad_unit - unit * jnp.mean(grad_unit * unit, axis=-1, keepdims=True))
    grad_gated = grad_grouped.reshape(tokens, -1)
    grad_gate_in = (
        grad_gated
        * scan_out.reshape(tokens, -1)
        * gate_sig
        * (1.0 + gate_float * (1.0 - gate_sig))
    ).astype(bf16)
    grad_y = (grad_gated * gate_silu).reshape(tokens, head_count, HEAD_DIM)
    grad_y_b = grad_y.astype(bf16)
    grad_x_inner = jnp.einsum("hts,thp->shp", mix_weights, grad_y_b, preferred_element_type=f32)
    grad_weights = (
        jnp.einsum("thp,shp->hts", grad_y_b, scan_heads, preferred_element_type=f32) * decay_mat
    )
    grad_weights = (
        grad_weights.reshape(group_count, per_group, tokens, tokens).sum(axis=1).astype(bf16)
    )
    grad_c_inner = jnp.einsum("gts,sgn->tgn", grad_weights, b_groups, preferred_element_type=f32)
    grad_b_inner = jnp.einsum("gts,tgn->sgn", grad_weights, c_groups, preferred_element_type=f32)
    grown_grads = (grad_y * growth[:, :, None]).reshape(tokens, group_count, per_group, HEAD_DIM)
    grad_c_carry = jnp.einsum("tgrp,grpn->tgn", grown_grads, state_groups)
    block_state = jnp.einsum("tgrp,tgn->grpn", grown_grads, c_float)
    y_dots = jnp.sum(grad_y * scan_out, axis=2)
    local_grad = jnp.sum(y_dots - jnp.sum(x_float * grad_x_inner, axis=2), axis=0)

    pieces = experts // head_count
    first = (jnp.arange(experts) % pieces == 0).astype(f32)
    scalars = [jnp.repeat(part, pieces) for part in three_parts(cumulative[-1])] + list(
        three_parts(jnp.repeat(local_grad, pieces) * first)
    )
    sent = jnp.concatenate(
        [
            block_state.astype(bf16).reshape(experts, -1, STATE),
            local_state.astype(bf16).reshape(experts, -1, STATE),
            spread(scalars, experts),
        ],
        axis=1,
    )
    later, carried = scan_piece(lax.all_to_all(sent, SP, 0, 0, tiled=True))
    back = jnp.concatenate([later, spread(list(three_parts(carried)), experts)], axis=1)
    back = lax.all_to_all(back, SP, 0, 0, tiled=True)
    later_groups = back[:, :16].reshape(group_count, per_group, HEAD_DIM, STATE).astype(f32)
    later_grad = back[:, 16:19, 0].astype(f32).sum(axis=1).reshape(head_count, pieces).sum(axis=1)

    grad_x_carry = jnp.einsum("sgn,grpn->sgrp", b_float, later_groups).reshape(
        tokens, head_count, HEAD_DIM
    )
    grad_x = grad_x_inner + grad_x_carry * tail_decay[:, :, None]
    grad_b_carry = jnp.einsum("sgrp,grpn->sgn", x_tail, later_groups)
    grad_a = y_dots - jnp.sum(x_float * grad_x, axis=2)
    grad_log_decay = jnp.flip(jnp.cumsum(jnp.flip(grad_a, 0), axis=0), 0) + later_grad[None, :]
    grad_scan_in = grad_x.reshape(tokens, -1).astype(bf16)
    grad_b_proj = (grad_b_inner + grad_b_carry).reshape(tokens, -1).astype(bf16)
    grad_c_proj = (grad_c_inner + grad_c_carry).reshape(tokens, -1).astype(bf16)
    return (
        gate_wgrad[None],
        up_wgrad[None],
        down_wgrad[None],
        grad_out_proj,
        grad_scan_in,
        grad_gate_in,
        grad_b_proj,
        grad_c_proj,
        grad_log_decay,
    )


def solution(mesh):
    split = Mesh(mesh.devices.reshape(4, 4, 4, mesh.shape["tp"]), ("sp_0", "sp_1", "sp_2", "tp"))
    return jax.shard_map(
        body,
        mesh=split,
        in_specs=(
            P(SP, None),
            P(SP, None),
            P(SP, None),
            P(SP, None),
            P(SP, None, "tp"),
            P(SP, None, "tp"),
            P(SP, None, "tp"),
            P(SP, None, "tp"),
            P(SP, "tp", None),
            P("tp", None),
            P("tp"),
            P(SP, "tp"),
            P(SP, "tp"),
            P(SP, "tp"),
            P(SP, "tp"),
            P(SP, "tp"),
            P(SP, "tp", None, None),
        ),
        out_specs=(
            P(SP, None, "tp"),
            P(SP, None, "tp"),
            P(SP, "tp", None),
            P(SP, "tp"),
            P(SP, "tp"),
            P(SP, "tp"),
            P(SP, "tp"),
            P(SP, "tp"),
            P(SP, "tp"),
        ),
        check_vma=False,
    )
```

```python
import jax
import jax.numpy as jnp
from jax import lax
from jax.sharding import Mesh
from jax.experimental import pallas as pl
from jax.experimental.pallas import tpu as pltpu
from jax.sharding import PartitionSpec as P

HEAD_DIM = 64
STATE = 128
SP = ("sp_0", "sp_1", "sp_2")


rms_epsilon = 1e-05
clamp_limit = 7.0
swish_alpha = 1.702

bf16 = jnp.bfloat16
f32 = jnp.float32


def dot(a, b, dims):
    return lax.dot_general(a, b, (dims, ((), ())), preferred_element_type=f32)


def swapped(x):
    return lax.ppermute(x, "tp", [(0, 1), (1, 0)])


def from_line(parts, axis):
    size = lax.axis_size(axis)
    return [parts[0]] + [
        lax.ppermute(parts[k], axis, [(i, (i + k) % size) for i in range(size)])
        for k in range(1, size)
    ]


def pieces_for(x, axis, dim):
    size, spot = lax.axis_size(axis), lax.axis_index(axis)
    span = x.shape[dim] // size
    return [
        lax.dynamic_slice_in_dim(x, lax.rem(spot + k, size) * span, span, dim) for k in range(size)
    ]


def three_parts(x):
    high = lax.reduce_precision(x, 8, 7)
    rest = x - high
    middle = lax.reduce_precision(rest, 8, 7)
    return high.astype(bf16), middle.astype(bf16), (rest - middle).astype(bf16)


def expert_rows_kernel(
    side, mine, other, gate_value, up_value, down_own, down_far, gate_own, gate_far, up_own, up_far,
    active, gate_grad, up_grad, rows_own, rows_far,
):
    act_grad = dot(mine[...], down_own[...], ((1,), (1,)))
    act_grad = act_grad + dot(other[...], down_far[...], ((1,), (1,)))
    gate_full = gate_value[...].astype(f32)
    up_full = up_value[...].astype(f32)
    gate_clip = jnp.minimum(gate_full, clamp_limit)
    up_clip = jnp.clip(up_full, -clamp_limit, clamp_limit)
    sigmoid_gate = jax.nn.sigmoid(swish_alpha * gate_clip)
    swish_gate = gate_clip * sigmoid_gate
    active[...] = ((up_clip + 1.0) * swish_gate).astype(bf16)
    inside = (up_full > -clamp_limit) & (up_full < clamp_limit)
    up_side = jnp.where(inside, act_grad * swish_gate, 0.0).astype(bf16)
    slope = sigmoid_gate + swish_alpha * gate_clip * sigmoid_gate * (1.0 - sigmoid_gate)
    gate_side = jnp.where(
        gate_full < clamp_limit, act_grad * (up_clip + 1.0) * slope, 0.0
    ).astype(bf16)
    up_grad[...] = up_side
    gate_grad[...] = gate_side
    far = dot(gate_side, gate_far[...], ((1,), (1,))) + dot(up_side, up_far[...], ((1,), (1,)))
    rows_far[...] = far.astype(bf16)
    own = dot(gate_side, gate_own[...], ((1,), (1,))) + dot(up_side, up_own[...], ((1,), (1,)))
    rows_own[...] = own.astype(bf16)


def whole_block(*shape):
    return pl.BlockSpec(shape, lambda i, side: (0,) * len(shape))


def expert_rows(side, mine, other, gate_value, up_value, w_down, w_gate, w_up):
    rows, half = mine.shape
    hidden = gate_value.shape[1]
    row_block = whole_block(rows, half)
    act_block = whole_block(rows, hidden)
    down = [
        pl.BlockSpec((hidden, half), lambda i, side: (0, side[0])),
        pl.BlockSpec((hidden, half), lambda i, side: (0, 1 - side[0])),
    ]
    tall = [
        pl.BlockSpec((half, hidden), lambda i, side: (side[0], 0)),
        pl.BlockSpec((half, hidden), lambda i, side: (1 - side[0], 0)),
    ]
    act = jax.ShapeDtypeStruct((rows, hidden), bf16)
    out = jax.ShapeDtypeStruct((rows, half), bf16)
    return pl.pallas_call(
        expert_rows_kernel,
        grid_spec=pltpu.PrefetchScalarGridSpec(
            num_scalar_prefetch=1,
            grid=(1,),
            in_specs=[row_block, row_block, act_block, act_block] + down + tall + tall,
            out_specs=[act_block] * 3 + [row_block] * 2,
        ),
        out_shape=[act] * 3 + [out] * 2,
        name="expert_rows",
    )(side, mine, other, gate_value, up_value, w_down, w_down, w_gate, w_gate, w_up, w_up)


def down_kernel(side, active, mine, other, out):
    @pl.when(pl.program_id(0) == 0)
    def _():
        out[...] = dot(active[...], mine[...], ((0,), (0,))).astype(bf16)

    @pl.when(pl.program_id(0) == 1)
    def _():
        out[...] = dot(active[...], other[...], ((0,), (0,))).astype(bf16)


def tall_kernel(side, gate_grad, up_grad, mine, other, gate_out, up_out):
    def write(rows):
        gate_out[...] = dot(rows, gate_grad[...], ((0,), (0,))).astype(bf16)
        up_out[...] = dot(rows, up_grad[...], ((0,), (0,))).astype(bf16)

    @pl.when(pl.program_id(0) == 0)
    def _():
        write(mine[...])

    @pl.when(pl.program_id(0) == 1)
    def _():
        write(other[...])


def half_of(i, side):
    return lax.rem(i + side[0], 2)


def down_weights(side, active, mine, other):
    rows, half = mine.shape
    hidden = active.shape[1]
    return pl.pallas_call(
        down_kernel,
        grid_spec=pltpu.PrefetchScalarGridSpec(
            num_scalar_prefetch=1,
            grid=(2,),
            in_specs=[whole_block(rows, hidden)] + [whole_block(rows, half)] * 2,
            out_specs=pl.BlockSpec((hidden, half), lambda i, side: (0, half_of(i, side))),
        ),
        out_shape=jax.ShapeDtypeStruct((hidden, 2 * half), bf16),
        name="down_weights",
    )(side, active, mine, other)


def tall_weights(side, gate_grad, up_grad, mine, other):
    rows, half = mine.shape
    hidden = gate_grad.shape[1]
    return pl.pallas_call(
        tall_kernel,
        grid_spec=pltpu.PrefetchScalarGridSpec(
            num_scalar_prefetch=1,
            grid=(2,),
            in_specs=[whole_block(rows, hidden)] * 2 + [whole_block(rows, half)] * 2,
            out_specs=[pl.BlockSpec((half, hidden), lambda i, side: (half_of(i, side), 0))] * 2,
        ),
        out_shape=[jax.ShapeDtypeStruct((2 * half, hidden), bf16)] * 2,
        name="tall_weights",
    )(side, gate_grad, up_grad, mine, other)


def scan_piece(came):
    blocks = came.shape[0]
    values = came[:, :16].reshape(blocks, -1)
    local = came[:, 16:32].reshape(blocks, -1).astype(f32)
    pieces = 4
    lead = lax.rem(lax.axis_index(SP), pieces) == 0
    sums = jnp.where(lead, came[:, 35:38, 0].astype(f32).sum(axis=1), 0.0)
    at = jnp.arange(blocks)
    after = at[None, :] > at[:, None]
    gaps = jnp.zeros((blocks, blocks), f32)
    for k in range(3):
        part = jnp.where(after, came[:, 32 + k, 0][None, :], 0).astype(bf16)
        gaps = gaps + dot(part, after.astype(bf16), ((1,), (0,)))
    weights = jnp.where(after, jnp.exp(gaps), 0.0)
    high = lax.reduce_precision(weights, 8, 7)
    low = weights - high
    later = dot(high.astype(bf16), values, ((1,), (0,))) + dot(
        low.astype(bf16), values, ((1,), (0,))
    )
    own = sums - jnp.sum(later * local, axis=1)
    carried = jnp.sum(jnp.where(after, own[None, :], 0.0), axis=1)
    return later.astype(bf16).reshape(blocks, 16, STATE), carried


def spread(parts, blocks):
    rows = jnp.stack(parts, axis=1)
    rows = jnp.pad(rows, ((0, 0), (0, 8 - len(parts))))
    return jnp.broadcast_to(rows[:, :, None], (blocks, 8, STATE)).astype(bf16)


def exact_dot(a, b, dims):
    return lax.dot_general(
        a, b, (dims, ((), ())), preferred_element_type=f32, precision=lax.Precision.HIGHEST
    )


def grid_of(rows, columns, axis):
    return lax.broadcasted_iota(jnp.int32, (rows, columns), axis)


def route_kernel(side, choice, weight, cotangent, grads, places):
    tokens = choice.shape[1]
    slots = places.shape[0]
    experts = slots // 8
    expert_at = grid_of(experts, tokens, 0)
    hot = [(expert_at == choice[k : k + 1, :]).astype(f32) for k in range(2)]
    before = (grid_of(tokens, tokens, 0) < grid_of(tokens, tokens, 1)).astype(bf16)
    earlier = dot((hot[0] + hot[1]).astype(bf16), before, ((1,), (0,)))
    same = (grid_of(tokens, tokens, 0) == grid_of(tokens, tokens, 1)).astype(f32)
    weights = exact_dot(same, weight[...], ((1,), (1,)))
    cotangents = cotangent[...].astype(f32)
    slot_at = grid_of(slots, tokens, 0)
    either = jnp.zeros((slots, tokens), f32)
    sent = jnp.zeros((slots, cotangent.shape[1]), f32)
    for k in range(2):
        rank = jnp.sum(earlier * hot[k], axis=0, keepdims=True).astype(jnp.int32)
        taken = (slot_at == choice[k : k + 1, :] * 8 + rank).astype(f32)
        either = either + taken
        rows = (weights[:, k : k + 1] * cotangents).astype(bf16)
        sent = sent + dot(taken.astype(bf16), rows, ((1,), (0,)))
    grads[...] = sent.astype(bf16)
    places[...] = either.astype(bf16)


def route(side, choice, weight, cotangent, slots):
    tokens, width = cotangent.shape
    half = width // 2
    return pl.pallas_call(
        route_kernel,
        grid_spec=pltpu.PrefetchScalarGridSpec(
            num_scalar_prefetch=1,
            grid=(1,),
            in_specs=[
                whole_block(*choice.shape),
                whole_block(*weight.shape),
                pl.BlockSpec((tokens, half), lambda i, side: (0, side[0])),
            ],
            out_specs=[whole_block(slots, half), whole_block(slots, tokens)],
        ),
        out_shape=[
            jax.ShapeDtypeStruct((slots, half), bf16),
            jax.ShapeDtypeStruct((slots, tokens), bf16),
        ],
        name="route",
    )(side, choice, weight, cotangent)


GROUP = 256
PER_GROUP = GROUP // HEAD_DIM


def per_head(rows, first):
    return jnp.concatenate(
        [
            jnp.broadcast_to(rows[first + r : first + r + 1, :], (HEAD_DIM, rows.shape[1]))
            for r in range(PER_GROUP)
        ],
        axis=0,
    )


def head_sums(x):
    return [
        jnp.sum(x[r * HEAD_DIM : (r + 1) * HEAD_DIM, :], axis=0, keepdims=True)
        for r in range(PER_GROUP)
    ]


def forward_kernel(
    scan_in, gate_in, b_proj, c_proj, log_decay, entry, gain,
    mixed, gated_out, silu_out, slope_out, mix_out, decay_out, x_out, tail_out, local_out,
    rows_out, inverse_out,
):
    tokens = scan_in.shape[0]
    groups = scan_in.shape[1] // GROUP
    down, across = grid_of(tokens, tokens, 0), grid_of(tokens, tokens, 1)
    decays = log_decay[...]
    cum_rows = exact_dot(decays, (down <= across).astype(f32), ((1,), (0,)))
    cum_columns = exact_dot((across <= down).astype(f32), decays, ((1,), (1,)))
    total = cum_rows[:, tokens - 1 :]
    growth = jnp.exp(cum_rows)
    tail = jnp.exp(total - cum_rows)
    rows_out[0] = growth
    rows_out[1] = tail
    rows_out[2] = jnp.broadcast_to(total, growth.shape)
    causal = down >= across
    for g in range(groups):
        span = slice(g * GROUP, (g + 1) * GROUP)
        states = slice(g * STATE, (g + 1) * STATE)
        first = g * PER_GROUP
        b_group, c_group = b_proj[:, states], c_proj[:, states]
        inner = dot(c_group, b_group, ((1,), (1,)))
        x = jnp.transpose(scan_in[:, span].astype(f32))
        x_b = x.astype(bf16)
        carried = dot(entry[span, :].astype(bf16), c_group, ((1,), (1,)))
        within = []
        for r in range(PER_GROUP):
            h = first + r
            gaps = cum_columns[:, h : h + 1] - cum_rows[h : h + 1, :]
            decay = jnp.where(causal, jnp.exp(jnp.where(causal, gaps, 0.0)), 0.0)
            decay_out[h] = decay
            mix = (inner * decay).astype(bf16)
            mix_out[h] = mix
            within.append(dot(x_b[r * HEAD_DIM : (r + 1) * HEAD_DIM, :], mix, ((1,), (1,))))
        scan_out = jnp.concatenate(within, axis=0) + carried * per_head(growth, first)
        gate = jnp.transpose(gate_in[:, span].astype(f32))
        sig = jax.nn.sigmoid(gate)
        silu = gate * sig
        gated = scan_out * silu
        inverse = lax.rsqrt(jnp.mean(gated * gated, axis=0, keepdims=True) + rms_epsilon)
        mixed[span, :] = (gated * inverse * gain[span, :]).astype(bf16)
        gated_out[span, :] = gated
        silu_out[span, :] = silu
        slope_out[span, :] = scan_out * sig * (1.0 + gate * (1.0 - sig))
        inverse_out[g : g + 1, :] = inverse
        x_out[span, :] = x_b
        x_tail = (x * per_head(tail, first)).astype(bf16)
        tail_out[span, :] = x_tail
        local_out[span, :] = dot(x_tail, b_group, ((1,), (0,))).astype(bf16)


def whole_call(kernel, out_shape, *args):
    return pl.pallas_call(kernel, out_shape=[jax.ShapeDtypeStruct(*x) for x in out_shape])(*args)


def forward(scan_in, gate_in, b_proj, c_proj, log_decay, entry, gain):
    tokens, inner = scan_in.shape
    heads = log_decay.shape[0]
    return whole_call(
        forward_kernel,
        [
            ((inner, tokens), bf16),
            ((inner, tokens), f32),
            ((inner, tokens), f32),
            ((inner, tokens), f32),
            ((heads, tokens, tokens), bf16),
            ((heads, tokens, tokens), f32),
            ((inner, tokens), bf16),
            ((inner, tokens), bf16),
            ((inner, STATE), bf16),
            ((3, heads, tokens), f32),
            ((inner // GROUP, tokens), f32),
        ],
        scan_in, gate_in, b_proj, c_proj, log_decay, entry, gain,
    )


def spread_parts(x, heads, pieces):
    high = x.astype(bf16)
    rest = x - high.astype(f32)
    middle = rest.astype(bf16)
    low = (rest - middle.astype(f32)).astype(bf16)
    return [
        jnp.broadcast_to(part.astype(f32)[:, None, :], (heads, pieces, STATE)).reshape(
            heads * pieces, 1, STATE
        )
        for part in (high, middle, low)
    ]


def backward_kernel(
    side, grad_own, grad_far, out_own, out_far, gain, gated_in, silu_in, slope_in, mix_in, decay_in,
    x_in, b_proj, c_proj, entry, local_in, rows_in, inverse_in,
    message, gate_grad, x_grad, b_grad, c_grad, y_dots,
):
    groups = gain.shape[0] // GROUP
    pieces = GROUP // 16
    tokens = grad_own.shape[0]
    for g in range(groups):
        span = slice(g * GROUP, (g + 1) * GROUP)
        states = slice(g * STATE, (g + 1) * STATE)
        first = g * PER_GROUP
        grad_mixed = dot(out_own[span, :], grad_own[...], ((1,), (1,)))
        grad_mixed = grad_mixed + dot(out_far[span, :], grad_far[...], ((1,), (1,)))
        inverse = inverse_in[g : g + 1, :]
        gated = gated_in[span, :]
        unit = gated * inverse
        grad_unit = grad_mixed * gain[span, :]
        mean = jnp.mean(grad_unit * unit, axis=0, keepdims=True)
        grad_gated = inverse * (grad_unit - unit * mean)
        gate_grad[:, span] = jnp.transpose(grad_gated * slope_in[span, :]).astype(bf16)
        grad_y = grad_gated * silu_in[span, :]
        grad_y_b = grad_y.astype(bf16)
        grown = (grad_y * per_head(rows_in[0], first)).astype(bf16)
        b_group, c_group = b_proj[:, states], c_proj[:, states]
        block_state = dot(grown, c_group, ((1,), (0,))).astype(bf16)
        message[g * pieces : (g + 1) * pieces, 0:16, :] = block_state.reshape(pieces, 16, STATE)
        message[g * pieces : (g + 1) * pieces, 16:32, :] = local_in[span, :].reshape(
            pieces, 16, STATE
        )
        x = x_in[span, :]
        weights = jnp.zeros((tokens, tokens), f32)
        inside = []
        for r in range(PER_GROUP):
            h = first + r
            head = slice(r * HEAD_DIM, (r + 1) * HEAD_DIM)
            inside.append(dot(grad_y_b[head, :], mix_in[h], ((1,), (0,))))
            weights = weights + decay_in[h] * dot(grad_y_b[head, :], x[head, :], ((0,), (0,)))
        inside = jnp.concatenate(inside, axis=0)
        x_grad[span, :] = inside
        weights = weights.astype(bf16)
        c_grad[:, states] = (
            dot(weights, b_group, ((1,), (0,)))
            + dot(grown, entry[span, :].astype(bf16), ((0,), (0,)))
        ).astype(bf16)
        b_grad[:, states] = dot(weights, c_group, ((0,), (0,)))
        dots = jnp.concatenate(head_sums(grad_gated * gated), axis=0)
        y_dots[first : first + PER_GROUP, :] = dots
        own = dots - jnp.concatenate(head_sums(x.astype(f32) * inside), axis=0)
        own = jnp.broadcast_to(jnp.sum(own, axis=1, keepdims=True), (PER_GROUP, STATE))
        total = rows_in[2][first : first + PER_GROUP, :]
        per = pieces // PER_GROUP
        zero = jnp.zeros((pieces, 2, STATE), f32)
        extra = jnp.concatenate(
            spread_parts(total, PER_GROUP, per) + spread_parts(own, PER_GROUP, per) + [zero],
            axis=1,
        )
        message[g * pieces : (g + 1) * pieces, 32:40, :] = extra.astype(bf16)


def backward(side, grad_own, grad_far, w_out, gain, saved, b_proj, c_proj, entry):
    gated, silu, slope, mix, decay, x, local, rows, inverse = saved
    tokens, half = grad_own.shape
    inner = gain.shape[0]
    heads = decay.shape[0]
    wide = [gain, gated, silu, slope, mix, decay, x, b_proj, c_proj, entry, local, rows, inverse]
    outs = [
        ((inner // 16, 40, STATE), bf16),
        ((tokens, inner), bf16),
        ((inner, tokens), f32),
        ((tokens, b_proj.shape[1]), f32),
        ((tokens, b_proj.shape[1]), bf16),
        ((heads, tokens), f32),
    ]
    return pl.pallas_call(
        backward_kernel,
        grid_spec=pltpu.PrefetchScalarGridSpec(
            num_scalar_prefetch=1,
            grid=(1,),
            in_specs=[whole_block(tokens, half)] * 2
            + [
                pl.BlockSpec((inner, half), lambda i, side: (0, side[0])),
                pl.BlockSpec((inner, half), lambda i, side: (0, 1 - side[0])),
            ]
            + [whole_block(*x.shape) for x in wide],
            out_specs=[whole_block(*shape) for shape, _ in outs],
        ),
        out_shape=[jax.ShapeDtypeStruct(*x) for x in outs],
        name="backward",
    )(side, grad_own, grad_far, w_out, w_out, *wide)


def final_kernel(back, b_proj, x_in, tail_in, rows_in, x_inside, y_dots, b_inside, x_grad, b_grad, decay_grad):
    groups = x_in.shape[0] // GROUP
    pieces = GROUP // 16
    tokens = x_in.shape[1]
    heads = y_dots.shape[0]
    dots = []
    for g in range(groups):
        span = slice(g * GROUP, (g + 1) * GROUP)
        states = slice(g * STATE, (g + 1) * STATE)
        first = g * PER_GROUP
        later = back[g * pieces : (g + 1) * pieces, 0:16, :].reshape(GROUP, STATE)
        carried = dot(later, b_proj[:, states], ((1,), (1,)))
        grad = x_inside[span, :] + carried * per_head(rows_in[1], first)
        x_grad[:, span] = jnp.transpose(grad).astype(bf16)
        b_grad[:, states] = (
            b_inside[:, states] + dot(tail_in[span, :], later, ((0,), (0,)))
        ).astype(bf16)
        dots = dots + head_sums(x_in[span, :].astype(f32) * grad)
    own = y_dots[...] - jnp.concatenate(dots, axis=0)
    after = (grid_of(tokens, tokens, 0) >= grid_of(tokens, tokens, 1)).astype(f32)
    extra = jnp.sum(back[:, 16:24, :].astype(f32), axis=1)
    extra = jnp.sum(extra.reshape(heads, extra.shape[0] // heads, STATE), axis=1)
    decay_grad[...] = exact_dot(own, after, ((1,), (0,))) + extra


def final(back, b_proj, x, x_tail, rows, x_inside, y_dots, b_inside):
    inner, tokens = x.shape
    return whole_call(
        final_kernel,
        [
            ((tokens, inner), bf16),
            (b_proj.shape, bf16),
            (y_dots.shape, f32),
        ],
        back, b_proj, x, x_tail, rows, x_inside, y_dots, b_inside,
    )


def body(
    mixer_output,
    layer_cotangent,
    expert_choice,
    route_weight,
    gate_pre,
    up_pre,
    w_gate,
    w_up,
    w_down,
    w_out,
    norm_gain,
    scan_in,
    gate_in,
    b_proj,
    c_proj,
    log_decay,
    entry_state,
):
    experts = lax.axis_size(SP)
    _, width = mixer_output.shape
    capacity = gate_pre.shape[1] // experts
    half = width // 2
    start = lax.axis_index("tp") * half

    side = lax.axis_index("tp")[None]
    send_grads, either = route(
        side, expert_choice.T, route_weight.T, layer_cotangent, experts * capacity
    )
    hidden_half = lax.dynamic_slice_in_dim(mixer_output, start, half, 1)
    cotangent_half = lax.dynamic_slice_in_dim(layer_cotangent, start, half, 1)
    send_hidden = dot(either, hidden_half, ((1,), (0,))).astype(bf16)
    send_grads = send_grads.reshape(experts, capacity, half)
    send_hidden = send_hidden.reshape(experts, capacity, half)
    came_grads = lax.all_to_all(send_grads, SP, 0, 0, tiled=True)
    send_hidden, came_grads = lax.optimization_barrier((send_hidden, came_grads))
    came_hidden = lax.all_to_all(send_hidden, SP, 0, 0, tiled=True)
    grads_own = came_grads.reshape(-1, half)
    grads_far = swapped(grads_own)
    active, gate_grad, up_grad, rows_own, rows_far = expert_rows(
        side, grads_own, grads_far, gate_pre[0], up_pre[0], w_down[0], w_gate[0], w_up[0]
    )
    summed = (rows_own.astype(f32) + swapped(rows_far).astype(f32)).astype(bf16)
    summed, came_hidden = lax.optimization_barrier((summed, came_hidden))
    returned = lax.all_to_all(summed.reshape(experts, capacity, half), SP, 0, 0, tiled=True)
    hidden_own = came_hidden.reshape(-1, half)
    hidden_far = swapped(hidden_own)
    down_wgrad = down_weights(side, active, grads_own, grads_far)
    gate_wgrad, up_wgrad = tall_weights(side, gate_grad, up_grad, hidden_own, hidden_far)
    moe_terms = dot(either, returned.reshape(-1, half), ((0,), (0,)))
    grad_own = (cotangent_half.astype(f32) + moe_terms).astype(bf16)
    grad_far = swapped(grad_own)
    grad_hidden = jnp.where(
        side == 0,
        jnp.concatenate([grad_own, grad_far], axis=1),
        jnp.concatenate([grad_far, grad_own], axis=1),
    )

    inner = scan_in.shape[1]
    gain = norm_gain.astype(f32)[:, None]
    entry = entry_state.reshape(inner, STATE)
    mixed, *saved, x_tail, local, rows, inverse = forward(
        scan_in, gate_in, b_proj, c_proj, log_decay.T, entry, gain
    )
    gated, silu, slope, mix, decay, x = saved
    message, grad_gate_in, x_inside, b_inside, grad_c_proj, y_dots = backward(
        side, grad_own, grad_far, w_out, gain,
        (gated, silu, slope, mix, decay, x, local, rows, inverse), b_proj, c_proj, entry,
    )
    came_states = lax.all_to_all(message, SP, 0, 0, tiled=True)
    later, carried = scan_piece(came_states)
    back = jnp.concatenate([later, spread(list(three_parts(carried)), experts)], axis=1)
    back = lax.all_to_all(back, SP, 0, 0, tiled=True)
    grad_scan_in, grad_b_proj, decay_grad = final(
        back, b_proj, x, x_tail, rows, x_inside, y_dots, b_inside
    )
    grad_log_decay = decay_grad.T

    line = lax.axis_size("sp_0")
    mixed_line = from_line([mixed] * line, "sp_0")
    grads_line = from_line(pieces_for(grad_hidden, "sp_0", 1), "sp_0")
    grad_out_proj = dot(
        jnp.concatenate(grads_line, axis=0), jnp.concatenate(mixed_line, axis=1), ((0,), (1,))
    )
    for axis in ("sp_1", "sp_2"):
        parts = from_line(pieces_for(grad_out_proj.astype(bf16), axis, 0), axis)
        grad_out_proj = sum(part.astype(f32) for part in parts)

    return (
        gate_wgrad[None],
        up_wgrad[None],
        down_wgrad[None],
        grad_out_proj,
        grad_scan_in,
        grad_gate_in,
        grad_b_proj,
        grad_c_proj,
        grad_log_decay,
    )


def solution(mesh):
    split = Mesh(mesh.devices.reshape(4, 4, 4, mesh.shape["tp"]), ("sp_0", "sp_1", "sp_2", "tp"))
    return jax.shard_map(
        body,
        mesh=split,
        in_specs=(
            P(SP, None),
            P(SP, None),
            P(SP, None),
            P(SP, None),
            P(SP, None, "tp"),
            P(SP, None, "tp"),
            P(SP, None, "tp"),
            P(SP, None, "tp"),
            P(SP, "tp", None),
            P("tp", None),
            P("tp"),
            P(SP, "tp"),
            P(SP, "tp"),
            P(SP, "tp"),
            P(SP, "tp"),
            P(SP, "tp"),
            P(SP, "tp", None, None),
        ),
        out_specs=(
            P(SP, None, "tp"),
            P(SP, None, "tp"),
            P(SP, "tp", None),
            P(SP, "tp"),
            P(SP, "tp"),
            P(SP, "tp"),
            P(SP, "tp"),
            P(SP, "tp"),
            P(SP, "tp"),
        ),
        check_vma=False,
    )
```

```python
import jax
import jax.numpy as jnp
from jax import lax
from jax.sharding import Mesh
from jax.experimental import pallas as pl
from jax.experimental.pallas import tpu as pltpu
from jax.sharding import PartitionSpec as P

HEAD_DIM = 64
STATE = 128
SP = ("sp_0", "sp_1", "sp_2")


rms_epsilon = 1e-05
clamp_limit = 7.0
swish_alpha = 1.702

bf16 = jnp.bfloat16
f32 = jnp.float32


def dot(a, b, dims):
    return lax.dot_general(a, b, (dims, ((), ())), preferred_element_type=f32)


def swapped(x):
    return lax.ppermute(x, "tp", [(0, 1), (1, 0)])


def from_line(parts, axis):
    size = lax.axis_size(axis)
    return [parts[0]] + [
        lax.ppermute(parts[k], axis, [(i, (i + k) % size) for i in range(size)])
        for k in range(1, size)
    ]


def pieces_for(x, axis, dim):
    size, spot = lax.axis_size(axis), lax.axis_index(axis)
    span = x.shape[dim] // size
    return [
        lax.dynamic_slice_in_dim(x, lax.rem(spot + k, size) * span, span, dim) for k in range(size)
    ]


def three_parts(x):
    high = lax.reduce_precision(x, 8, 7)
    rest = x - high
    middle = lax.reduce_precision(rest, 8, 7)
    return high.astype(bf16), middle.astype(bf16), (rest - middle).astype(bf16)


def expert_rows_kernel(
    side, mine, other, gate_value, up_value, down_own, down_far, gate_own, gate_far, up_own, up_far,
    active, gate_grad, up_grad, rows_own, rows_far,
):
    act_grad = dot(mine[...], down_own[...], ((1,), (1,)))
    act_grad = act_grad + dot(other[...], down_far[...], ((1,), (1,)))
    gate_full = gate_value[...].astype(f32)
    up_full = up_value[...].astype(f32)
    gate_clip = jnp.minimum(gate_full, clamp_limit)
    up_clip = jnp.clip(up_full, -clamp_limit, clamp_limit)
    sigmoid_gate = jax.nn.sigmoid(swish_alpha * gate_clip)
    swish_gate = gate_clip * sigmoid_gate
    active[...] = ((up_clip + 1.0) * swish_gate).astype(bf16)
    inside = (up_full > -clamp_limit) & (up_full < clamp_limit)
    up_side = jnp.where(inside, act_grad * swish_gate, 0.0).astype(bf16)
    slope = sigmoid_gate + swish_alpha * gate_clip * sigmoid_gate * (1.0 - sigmoid_gate)
    gate_side = jnp.where(
        gate_full < clamp_limit, act_grad * (up_clip + 1.0) * slope, 0.0
    ).astype(bf16)
    up_grad[...] = up_side
    gate_grad[...] = gate_side
    far = dot(gate_side, gate_far[...], ((1,), (1,))) + dot(up_side, up_far[...], ((1,), (1,)))
    rows_far[...] = far.astype(bf16)
    own = dot(gate_side, gate_own[...], ((1,), (1,))) + dot(up_side, up_own[...], ((1,), (1,)))
    rows_own[...] = own.astype(bf16)


def whole_block(*shape):
    return pl.BlockSpec(shape, lambda i, side: (0,) * len(shape))


def expert_rows(side, mine, other, gate_value, up_value, w_down, w_gate, w_up):
    rows, half = mine.shape
    hidden = gate_value.shape[1]
    row_block = whole_block(rows, half)
    act_block = whole_block(rows, hidden)
    down = [
        pl.BlockSpec((hidden, half), lambda i, side: (0, side[0])),
        pl.BlockSpec((hidden, half), lambda i, side: (0, 1 - side[0])),
    ]
    tall = [
        pl.BlockSpec((half, hidden), lambda i, side: (side[0], 0)),
        pl.BlockSpec((half, hidden), lambda i, side: (1 - side[0], 0)),
    ]
    act = jax.ShapeDtypeStruct((rows, hidden), bf16)
    out = jax.ShapeDtypeStruct((rows, half), bf16)
    return pl.pallas_call(
        expert_rows_kernel,
        grid_spec=pltpu.PrefetchScalarGridSpec(
            num_scalar_prefetch=1,
            grid=(1,),
            in_specs=[row_block, row_block, act_block, act_block] + down + tall + tall,
            out_specs=[act_block] * 3 + [row_block] * 2,
        ),
        out_shape=[act] * 3 + [out] * 2,
        name="expert_rows",
    )(side, mine, other, gate_value, up_value, w_down, w_down, w_gate, w_gate, w_up, w_up)


def down_kernel(side, active, mine, other, out):
    @pl.when(pl.program_id(0) == 0)
    def _():
        out[...] = dot(active[...], mine[...], ((0,), (0,))).astype(bf16)

    @pl.when(pl.program_id(0) == 1)
    def _():
        out[...] = dot(active[...], other[...], ((0,), (0,))).astype(bf16)


def tall_kernel(side, gate_grad, up_grad, mine, other, gate_out, up_out):
    def write(rows):
        gate_out[...] = dot(rows, gate_grad[...], ((0,), (0,))).astype(bf16)
        up_out[...] = dot(rows, up_grad[...], ((0,), (0,))).astype(bf16)

    @pl.when(pl.program_id(0) == 0)
    def _():
        write(mine[...])

    @pl.when(pl.program_id(0) == 1)
    def _():
        write(other[...])


def half_of(i, side):
    return lax.rem(i + side[0], 2)


def down_weights(side, active, mine, other):
    rows, half = mine.shape
    hidden = active.shape[1]
    return pl.pallas_call(
        down_kernel,
        grid_spec=pltpu.PrefetchScalarGridSpec(
            num_scalar_prefetch=1,
            grid=(2,),
            in_specs=[whole_block(rows, hidden)] + [whole_block(rows, half)] * 2,
            out_specs=pl.BlockSpec((hidden, half), lambda i, side: (0, half_of(i, side))),
        ),
        out_shape=jax.ShapeDtypeStruct((hidden, 2 * half), bf16),
        name="down_weights",
    )(side, active, mine, other)


def tall_weights(side, gate_grad, up_grad, mine, other):
    rows, half = mine.shape
    hidden = gate_grad.shape[1]
    return pl.pallas_call(
        tall_kernel,
        grid_spec=pltpu.PrefetchScalarGridSpec(
            num_scalar_prefetch=1,
            grid=(2,),
            in_specs=[whole_block(rows, hidden)] * 2 + [whole_block(rows, half)] * 2,
            out_specs=[pl.BlockSpec((half, hidden), lambda i, side: (half_of(i, side), 0))] * 2,
        ),
        out_shape=[jax.ShapeDtypeStruct((2 * half, hidden), bf16)] * 2,
        name="tall_weights",
    )(side, gate_grad, up_grad, mine, other)


def scan_piece(came):
    blocks = came.shape[0]
    values = came[:, :16].reshape(blocks, -1)
    local = came[:, 16:32].reshape(blocks, -1).astype(f32)
    pieces = 4
    lead = lax.rem(lax.axis_index(SP), pieces) == 0
    sums = jnp.where(lead, came[:, 35:38, 0].astype(f32).sum(axis=1), 0.0)
    at = jnp.arange(blocks)
    after = at[None, :] > at[:, None]
    gaps = jnp.zeros((blocks, blocks), f32)
    for k in range(3):
        part = jnp.where(after, came[:, 32 + k, 0][None, :], 0).astype(bf16)
        gaps = gaps + dot(part, after.astype(bf16), ((1,), (0,)))
    weights = jnp.where(after, jnp.exp(gaps), 0.0)
    high = lax.reduce_precision(weights, 8, 7)
    low = weights - high
    later = dot(high.astype(bf16), values, ((1,), (0,))) + dot(
        low.astype(bf16), values, ((1,), (0,))
    )
    own = sums - jnp.sum(later * local, axis=1)
    carried = jnp.sum(jnp.where(after, own[None, :], 0.0), axis=1)
    return later.astype(bf16).reshape(blocks, 16, STATE), carried


def spread(parts, blocks):
    rows = jnp.stack(parts, axis=1)
    rows = jnp.pad(rows, ((0, 0), (0, 8 - len(parts))))
    return jnp.broadcast_to(rows[:, :, None], (blocks, 8, STATE)).astype(bf16)


def exact_dot(a, b, dims):
    return lax.dot_general(
        a, b, (dims, ((), ())), preferred_element_type=f32, precision=lax.Precision.HIGHEST
    )


def grid_of(rows, columns, axis):
    return lax.broadcasted_iota(jnp.int32, (rows, columns), axis)


def route_kernel(side, choice, weight, cotangent, grads, places):
    tokens = choice.shape[1]
    slots = places.shape[0]
    experts = slots // 8
    expert_at = grid_of(experts, tokens, 0)
    hot = [(expert_at == choice[k : k + 1, :]).astype(f32) for k in range(2)]
    before = (grid_of(tokens, tokens, 0) < grid_of(tokens, tokens, 1)).astype(bf16)
    earlier = dot((hot[0] + hot[1]).astype(bf16), before, ((1,), (0,)))
    same = (grid_of(tokens, tokens, 0) == grid_of(tokens, tokens, 1)).astype(f32)
    weights = exact_dot(same, weight[...], ((1,), (1,)))
    cotangents = cotangent[...].astype(f32)
    slot_at = grid_of(slots, tokens, 0)
    either = jnp.zeros((slots, tokens), f32)
    sent = jnp.zeros((slots, cotangent.shape[1]), f32)
    for k in range(2):
        rank = jnp.sum(earlier * hot[k], axis=0, keepdims=True).astype(jnp.int32)
        taken = (slot_at == choice[k : k + 1, :] * 8 + rank).astype(f32)
        either = either + taken
        rows = (weights[:, k : k + 1] * cotangents).astype(bf16)
        sent = sent + dot(taken.astype(bf16), rows, ((1,), (0,)))
    grads[...] = sent.astype(bf16)
    places[...] = either.astype(bf16)


def route(side, choice, weight, cotangent, slots):
    tokens, width = cotangent.shape
    half = width // 2
    return pl.pallas_call(
        route_kernel,
        grid_spec=pltpu.PrefetchScalarGridSpec(
            num_scalar_prefetch=1,
            grid=(1,),
            in_specs=[
                whole_block(*choice.shape),
                whole_block(*weight.shape),
                pl.BlockSpec((tokens, half), lambda i, side: (0, side[0])),
            ],
            out_specs=[whole_block(slots, half), whole_block(slots, tokens)],
        ),
        out_shape=[
            jax.ShapeDtypeStruct((slots, half), bf16),
            jax.ShapeDtypeStruct((slots, tokens), bf16),
        ],
        name="route",
    )(side, choice, weight, cotangent)


GROUP = 256
PER_GROUP = GROUP // HEAD_DIM


def per_head(rows, first):
    return jnp.concatenate(
        [
            jnp.broadcast_to(rows[first + r : first + r + 1, :], (HEAD_DIM, rows.shape[1]))
            for r in range(PER_GROUP)
        ],
        axis=0,
    )


def head_sums(x):
    return [
        jnp.sum(x[r * HEAD_DIM : (r + 1) * HEAD_DIM, :], axis=0, keepdims=True)
        for r in range(PER_GROUP)
    ]


def forward_kernel(
    scan_in, gate_in, b_proj, c_proj, log_decay, entry, gain,
    mixed, gated_out, silu_out, slope_out, mix_out, decay_out, x_out, tail_out, local_out,
    rows_out, inverse_out, carry_out,
):
    tokens = scan_in.shape[0]
    groups = scan_in.shape[1] // GROUP
    down, across = grid_of(tokens, tokens, 0), grid_of(tokens, tokens, 1)
    decays = log_decay[...]
    cum_rows = exact_dot(decays, (down <= across).astype(f32), ((1,), (0,)))
    cum_columns = exact_dot((across <= down).astype(f32), decays, ((1,), (1,)))
    total = cum_rows[:, tokens - 1 :]
    growth = jnp.exp(cum_rows)
    tail = jnp.exp(total - cum_rows)
    totals = jnp.broadcast_to(total, growth.shape)
    causal = down >= across
    for g in range(groups):
        span = slice(g * GROUP, (g + 1) * GROUP)
        states = slice(g * STATE, (g + 1) * STATE)
        first = g * PER_GROUP
        b_group, c_group = b_proj[:, states], c_proj[:, states]
        inner = dot(c_group, b_group, ((1,), (1,)))
        x = jnp.transpose(scan_in[:, span].astype(f32))
        x_b = x.astype(bf16)
        carried = dot(entry[span, :].astype(bf16), c_group, ((1,), (1,)))
        within = []
        for r in range(PER_GROUP):
            h = first + r
            gaps = cum_columns[:, h : h + 1] - cum_rows[h : h + 1, :]
            decay = jnp.where(causal, jnp.exp(jnp.where(causal, gaps, 0.0)), 0.0)
            decay_out[h] = decay
            mix = (inner * decay).astype(bf16)
            mix_out[h] = mix
            within.append(dot(x_b[r * HEAD_DIM : (r + 1) * HEAD_DIM, :], mix, ((1,), (1,))))
        carried = carried * per_head(growth, first)
        scan_out = jnp.concatenate(within, axis=0) + carried
        gate = jnp.transpose(gate_in[:, span].astype(f32))
        sig = jax.nn.sigmoid(gate)
        silu = gate * sig
        gated = scan_out * silu
        inverse = lax.rsqrt(jnp.mean(gated * gated, axis=0, keepdims=True) + rms_epsilon)
        mixed[span, :] = (gated * inverse * gain[span, :]).astype(bf16)
        gated_out[span, :] = gated
        silu_out[span, :] = silu
        slope_out[span, :] = scan_out * sig * (1.0 + gate * (1.0 - sig))
        carry_out[span, :] = carried * silu
        inverse_out[g] = inverse
        for k, part in enumerate((growth, tail, totals)):
            rows_out[k, g] = part[first : first + PER_GROUP, :]
        x_out[span, :] = x_b
        x_tail = (x * per_head(tail, first)).astype(bf16)
        tail_out[span, :] = x_tail
        local_out[span, :] = dot(x_tail, b_group, ((1,), (0,))).astype(bf16)


def whole_call(kernel, out_shape, *args):
    return pl.pallas_call(kernel, out_shape=[jax.ShapeDtypeStruct(*x) for x in out_shape])(*args)


def forward(scan_in, gate_in, b_proj, c_proj, log_decay, entry, gain):
    tokens, inner = scan_in.shape
    heads = log_decay.shape[0]
    return whole_call(
        forward_kernel,
        [
            ((inner, tokens), bf16),
            ((inner, tokens), f32),
            ((inner, tokens), f32),
            ((inner, tokens), f32),
            ((heads, tokens, tokens), bf16),
            ((heads, tokens, tokens), f32),
            ((inner, tokens), bf16),
            ((inner, tokens), bf16),
            ((inner, STATE), bf16),
            ((3, inner // GROUP, PER_GROUP, tokens), f32),
            ((inner // GROUP, 1, tokens), f32),
            ((inner, tokens), f32),
        ],
        scan_in, gate_in, b_proj, c_proj, log_decay, entry, gain,
    )


def spread_parts(x, heads, pieces):
    high = x.astype(bf16)
    rest = x - high.astype(f32)
    middle = rest.astype(bf16)
    low = (rest - middle.astype(f32)).astype(bf16)
    return [
        jnp.broadcast_to(part.astype(f32)[:, None, :], (heads, pieces, STATE)).reshape(
            heads * pieces, 1, STATE
        )
        for part in (high, middle, low)
    ]


def message_kernel(
    side, grad_own, grad_far, out_own, out_far, gain, gated_in, silu_in, carry_in, c_proj, local_in,
    rows_in, inverse_in,
    message, grad_out,
):
    pieces = GROUP // 16
    grad_mixed = dot(out_own[...], grad_own[...], ((1,), (1,)))
    grad_mixed = grad_mixed + dot(out_far[...], grad_far[...], ((1,), (1,)))
    inverse = inverse_in[0]
    unit = gated_in[...] * inverse
    grad_unit = grad_mixed * gain[...]
    mean = jnp.mean(grad_unit * unit, axis=0, keepdims=True)
    grad_gated = inverse * (grad_unit - unit * mean)
    grad_out[...] = grad_gated
    grown = (grad_gated * silu_in[...] * per_head(rows_in[0, 0], 0)).astype(bf16)
    block_state = dot(grown, c_proj[...], ((1,), (0,))).astype(bf16)
    message[:, 0:16, :] = block_state.reshape(pieces, 16, STATE)
    message[:, 16:32, :] = local_in[...].reshape(pieces, 16, STATE)
    own = jnp.concatenate(head_sums(grad_gated * carry_in[...]), axis=0)
    own = jnp.broadcast_to(jnp.sum(own, axis=1, keepdims=True), (PER_GROUP, STATE))
    per = pieces // PER_GROUP
    zero = jnp.zeros((pieces, 2, STATE), f32)
    extra = jnp.concatenate(
        spread_parts(rows_in[2, 0], PER_GROUP, per) + spread_parts(own, PER_GROUP, per) + [zero],
        axis=1,
    )
    message[:, 32:40, :] = extra.astype(bf16)


def state_message(side, grad_own, grad_far, w_out, gain, gated, silu, carry, c_proj, local, rows, inverse):
    tokens, half = grad_own.shape
    inner = gain.shape[0]
    pieces = GROUP // 16
    channels = pl.BlockSpec((GROUP, tokens), lambda i, side: (i, 0))
    return pl.pallas_call(
        message_kernel,
        grid_spec=pltpu.PrefetchScalarGridSpec(
            num_scalar_prefetch=1,
            grid=(inner // GROUP,),
            in_specs=[
                whole_block(tokens, half),
                whole_block(tokens, half),
                pl.BlockSpec((GROUP, half), lambda i, side: (i, side[0])),
                pl.BlockSpec((GROUP, half), lambda i, side: (i, 1 - side[0])),
                pl.BlockSpec((GROUP, 1), lambda i, side: (i, 0)),
                channels,
                channels,
                channels,
                pl.BlockSpec((tokens, STATE), lambda i, side: (0, i)),
                pl.BlockSpec((GROUP, STATE), lambda i, side: (i, 0)),
                pl.BlockSpec((3, 1, PER_GROUP, tokens), lambda i, side: (0, i, 0, 0)),
                pl.BlockSpec((1, 1, tokens), lambda i, side: (i, 0, 0)),
            ],
            out_specs=[
                pl.BlockSpec((pieces, 40, STATE), lambda i, side: (i, 0, 0)),
                channels,
            ],
        ),
        out_shape=[
            jax.ShapeDtypeStruct((inner // 16, 40, STATE), bf16),
            jax.ShapeDtypeStruct((inner, tokens), f32),
        ],
        name="message",
    )(side, grad_own, grad_far, w_out, w_out, gain, gated, silu, carry, c_proj, local, rows, inverse)


def inside_kernel(
    grad_in, gated_in, silu_in, slope_in, mix_in, decay_in, x_in, b_proj, c_proj, entry, rows_in,
    gate_grad, x_grad, b_grad, c_grad, y_dots,
):
    tokens = x_in.shape[1]
    for g in range(x_in.shape[0] // GROUP):
        span = slice(g * GROUP, (g + 1) * GROUP)
        states = slice(g * STATE, (g + 1) * STATE)
        first = g * PER_GROUP
        grad_gated = grad_in[span, :]
        gate_grad[:, span] = jnp.transpose(grad_gated * slope_in[span, :]).astype(bf16)
        grad_y = grad_gated * silu_in[span, :]
        grad_y_b = grad_y.astype(bf16)
        grown = (grad_y * per_head(rows_in[0, g], 0)).astype(bf16)
        b_group, c_group = b_proj[:, states], c_proj[:, states]
        x = x_in[span, :]
        weights = jnp.zeros((tokens, tokens), f32)
        inside = []
        for r in range(PER_GROUP):
            h = first + r
            head = slice(r * HEAD_DIM, (r + 1) * HEAD_DIM)
            inside.append(dot(grad_y_b[head, :], mix_in[h], ((1,), (0,))))
            weights = weights + decay_in[h] * dot(grad_y_b[head, :], x[head, :], ((0,), (0,)))
        x_grad[span, :] = jnp.concatenate(inside, axis=0)
        weights = weights.astype(bf16)
        c_grad[:, states] = (
            dot(weights, b_group, ((1,), (0,)))
            + dot(grown, entry[span, :].astype(bf16), ((0,), (0,)))
        ).astype(bf16)
        b_grad[:, states] = dot(weights, c_group, ((0,), (0,)))
        y_dots[first : first + PER_GROUP, :] = jnp.concatenate(
            head_sums(grad_gated * gated_in[span, :]), axis=0
        )


def inside_grads(grad, gated, silu, slope, mix, decay, x, b_proj, c_proj, entry, rows):
    inner, tokens = grad.shape
    return whole_call(
        inside_kernel,
        [
            ((tokens, inner), bf16),
            ((inner, tokens), f32),
            (b_proj.shape, f32),
            (b_proj.shape, bf16),
            ((decay.shape[0], tokens), f32),
        ],
        grad, gated, silu, slope, mix, decay, x, b_proj, c_proj, entry, rows,
    )


def final_kernel(back, b_proj, x_in, tail_in, rows_in, x_inside, y_dots, b_inside, x_grad, b_grad, decay_grad):
    groups = x_in.shape[0] // GROUP
    pieces = GROUP // 16
    tokens = x_in.shape[1]
    heads = y_dots.shape[0]
    dots = []
    for g in range(groups):
        span = slice(g * GROUP, (g + 1) * GROUP)
        states = slice(g * STATE, (g + 1) * STATE)
        later = back[g * pieces : (g + 1) * pieces, 0:16, :].reshape(GROUP, STATE)
        carried = dot(later, b_proj[:, states], ((1,), (1,)))
        grad = x_inside[span, :] + carried * per_head(rows_in[1, g], 0)
        x_grad[:, span] = jnp.transpose(grad).astype(bf16)
        b_grad[:, states] = (
            b_inside[:, states] + dot(tail_in[span, :], later, ((0,), (0,)))
        ).astype(bf16)
        dots = dots + head_sums(x_in[span, :].astype(f32) * grad)
    own = y_dots[...] - jnp.concatenate(dots, axis=0)
    after = (grid_of(tokens, tokens, 0) >= grid_of(tokens, tokens, 1)).astype(f32)
    extra = jnp.sum(back[:, 16:24, :].astype(f32), axis=1)
    extra = jnp.sum(extra.reshape(heads, extra.shape[0] // heads, STATE), axis=1)
    decay_grad[...] = exact_dot(own, after, ((1,), (0,))) + extra


def final(back, b_proj, x, x_tail, rows, x_inside, y_dots, b_inside):
    inner, tokens = x.shape
    return whole_call(
        final_kernel,
        [
            ((tokens, inner), bf16),
            (b_proj.shape, bf16),
            (y_dots.shape, f32),
        ],
        back, b_proj, x, x_tail, rows, x_inside, y_dots, b_inside,
    )


def body(
    mixer_output,
    layer_cotangent,
    expert_choice,
    route_weight,
    gate_pre,
    up_pre,
    w_gate,
    w_up,
    w_down,
    w_out,
    norm_gain,
    scan_in,
    gate_in,
    b_proj,
    c_proj,
    log_decay,
    entry_state,
):
    experts = lax.axis_size(SP)
    _, width = mixer_output.shape
    capacity = gate_pre.shape[1] // experts
    half = width // 2
    start = lax.axis_index("tp") * half

    side = lax.axis_index("tp")[None]
    send_grads, either = route(
        side, expert_choice.T, route_weight.T, layer_cotangent, experts * capacity
    )
    hidden_half = lax.dynamic_slice_in_dim(mixer_output, start, half, 1)
    cotangent_half = lax.dynamic_slice_in_dim(layer_cotangent, start, half, 1)
    send_hidden = dot(either, hidden_half, ((1,), (0,))).astype(bf16)
    send_grads = send_grads.reshape(experts, capacity, half)
    send_hidden = send_hidden.reshape(experts, capacity, half)
    came_grads = lax.all_to_all(send_grads, SP, 0, 0, tiled=True)
    send_hidden, came_grads = lax.optimization_barrier((send_hidden, came_grads))
    came_hidden = lax.all_to_all(send_hidden, SP, 0, 0, tiled=True)
    grads_own = came_grads.reshape(-1, half)
    grads_far = swapped(grads_own)
    active, gate_grad, up_grad, rows_own, rows_far = expert_rows(
        side, grads_own, grads_far, gate_pre[0], up_pre[0], w_down[0], w_gate[0], w_up[0]
    )
    summed = (rows_own.astype(f32) + swapped(rows_far).astype(f32)).astype(bf16)
    summed, came_hidden = lax.optimization_barrier((summed, came_hidden))
    returned = lax.all_to_all(summed.reshape(experts, capacity, half), SP, 0, 0, tiled=True)
    hidden_own = came_hidden.reshape(-1, half)
    hidden_far = swapped(hidden_own)
    down_wgrad = down_weights(side, active, grads_own, grads_far)
    gate_wgrad, up_wgrad = tall_weights(side, gate_grad, up_grad, hidden_own, hidden_far)
    moe_terms = dot(either, returned.reshape(-1, half), ((0,), (0,)))
    grad_own = (cotangent_half.astype(f32) + moe_terms).astype(bf16)
    grad_far = swapped(grad_own)
    grad_hidden = jnp.where(
        side == 0,
        jnp.concatenate([grad_own, grad_far], axis=1),
        jnp.concatenate([grad_far, grad_own], axis=1),
    )

    inner = scan_in.shape[1]
    gain = norm_gain.astype(f32)[:, None]
    entry = entry_state.reshape(inner, STATE)
    mixed, *saved, x_tail, local, rows, inverse, carry = forward(
        scan_in, gate_in, b_proj, c_proj, log_decay.T, entry, gain
    )
    gated, silu, slope, mix, decay, x = saved
    message, grad_gated = state_message(
        side, grad_own, grad_far, w_out, gain, gated, silu, carry, c_proj, local, rows, inverse
    )
    grad_hidden, message = lax.optimization_barrier((grad_hidden, message))
    came_states = lax.all_to_all(message, SP, 0, 0, tiled=True)
    later, carried = scan_piece(came_states)
    back = jnp.concatenate([later, spread(list(three_parts(carried)), experts)], axis=1)
    grad_gated, ready = lax.optimization_barrier((grad_gated, back))
    grad_gate_in, x_inside, b_inside, grad_c_proj, y_dots = inside_grads(
        grad_gated, gated, silu, slope, mix, decay, x, b_proj, c_proj, entry, rows
    )
    back = lax.all_to_all(back, SP, 0, 0, tiled=True)
    grad_scan_in, grad_b_proj, decay_grad = final(
        back, b_proj, x, x_tail, rows, x_inside, y_dots, b_inside
    )
    grad_log_decay = decay_grad.T

    line = lax.axis_size("sp_0")
    mixed, gate_wgrad = lax.optimization_barrier((mixed, gate_wgrad))
    mixed_line = from_line([mixed] * line, "sp_0")
    grads_line = from_line(pieces_for(grad_hidden, "sp_0", 1), "sp_0")
    product = dot(
        jnp.concatenate(grads_line, axis=0), jnp.concatenate(mixed_line, axis=1), ((0,), (1,))
    ).astype(bf16)
    parts = from_line(pieces_for(product, "sp_1", 0), "sp_1")
    parts, ready = lax.optimization_barrier((parts, ready))
    product = sum(part.astype(f32) for part in parts).astype(bf16)
    parts = from_line(pieces_for(product, "sp_2", 0), "sp_2")
    grad_out_proj = sum(part.astype(f32) for part in parts)

    return (
        gate_wgrad[None],
        up_wgrad[None],
        down_wgrad[None],
        grad_out_proj,
        grad_scan_in,
        grad_gate_in,
        grad_b_proj,
        grad_c_proj,
        grad_log_decay,
    )


def solution(mesh):
    split = Mesh(mesh.devices.reshape(4, 4, 4, mesh.shape["tp"]), ("sp_0", "sp_1", "sp_2", "tp"))
    return jax.shard_map(
        body,
        mesh=split,
        in_specs=(
            P(SP, None),
            P(SP, None),
            P(SP, None),
            P(SP, None),
            P(SP, None, "tp"),
            P(SP, None, "tp"),
            P(SP, None, "tp"),
            P(SP, None, "tp"),
            P(SP, "tp", None),
            P("tp", None),
            P("tp"),
            P(SP, "tp"),
            P(SP, "tp"),
            P(SP, "tp"),
            P(SP, "tp"),
            P(SP, "tp"),
            P(SP, "tp", None, None),
        ),
        out_specs=(
            P(SP, None, "tp"),
            P(SP, None, "tp"),
            P(SP, "tp", None),
            P(SP, "tp"),
            P(SP, "tp"),
            P(SP, "tp"),
            P(SP, "tp"),
            P(SP, "tp"),
            P(SP, "tp"),
        ),
        check_vma=False,
    )
```

```python
import jax
import jax.numpy as jnp
from jax import lax
from jax.sharding import Mesh
from jax.experimental import pallas as pl
from jax.experimental.pallas import tpu as pltpu
from jax.sharding import PartitionSpec as P

HEAD_DIM = 64
STATE = 128
SP = ("sp_0", "sp_1", "sp_2")


rms_epsilon = 1e-05
clamp_limit = 7.0
swish_alpha = 1.702

bf16 = jnp.bfloat16
f32 = jnp.float32


def dot(a, b, dims):
    return lax.dot_general(a, b, (dims, ((), ())), preferred_element_type=f32)


def swapped(x):
    return lax.ppermute(x, "tp", [(0, 1), (1, 0)])


def from_line(parts, axis):
    size = lax.axis_size(axis)
    return [parts[0]] + [
        lax.ppermute(parts[k], axis, [(i, (i + k) % size) for i in range(size)])
        for k in range(1, size)
    ]


def pieces_for(x, axis, dim):
    size, spot = lax.axis_size(axis), lax.axis_index(axis)
    span = x.shape[dim] // size
    return [
        lax.dynamic_slice_in_dim(x, lax.rem(spot + k, size) * span, span, dim) for k in range(size)
    ]


def three_parts(x):
    high = lax.reduce_precision(x, 8, 7)
    rest = x - high
    middle = lax.reduce_precision(rest, 8, 7)
    return high.astype(bf16), middle.astype(bf16), (rest - middle).astype(bf16)


def expert_rows_kernel(
    side, mine, other, gate_value, up_value, down_own, down_far, gate_own, gate_far, up_own, up_far,
    active, gate_grad, up_grad, rows_own, rows_far,
):
    act_grad = dot(mine[...], down_own[...], ((1,), (1,)))
    act_grad = act_grad + dot(other[...], down_far[...], ((1,), (1,)))
    gate_full = gate_value[...].astype(f32)
    up_full = up_value[...].astype(f32)
    gate_clip = jnp.minimum(gate_full, clamp_limit)
    up_clip = jnp.clip(up_full, -clamp_limit, clamp_limit)
    sigmoid_gate = jax.nn.sigmoid(swish_alpha * gate_clip)
    swish_gate = gate_clip * sigmoid_gate
    active[...] = ((up_clip + 1.0) * swish_gate).astype(bf16)
    inside = (up_full > -clamp_limit) & (up_full < clamp_limit)
    up_side = jnp.where(inside, act_grad * swish_gate, 0.0).astype(bf16)
    slope = sigmoid_gate + swish_alpha * gate_clip * sigmoid_gate * (1.0 - sigmoid_gate)
    gate_side = jnp.where(
        gate_full < clamp_limit, act_grad * (up_clip + 1.0) * slope, 0.0
    ).astype(bf16)
    up_grad[...] = up_side
    gate_grad[...] = gate_side
    far = dot(gate_side, gate_far[...], ((1,), (1,))) + dot(up_side, up_far[...], ((1,), (1,)))
    rows_far[...] = far.astype(bf16)
    own = dot(gate_side, gate_own[...], ((1,), (1,))) + dot(up_side, up_own[...], ((1,), (1,)))
    rows_own[...] = own.astype(bf16)


def whole_block(*shape):
    return pl.BlockSpec(shape, lambda i, side: (0,) * len(shape))


def expert_rows(side, mine, other, gate_value, up_value, w_down, w_gate, w_up):
    rows, half = mine.shape
    hidden = gate_value.shape[1]
    row_block = whole_block(rows, half)
    act_block = whole_block(rows, hidden)
    down = [
        pl.BlockSpec((hidden, half), lambda i, side: (0, side[0])),
        pl.BlockSpec((hidden, half), lambda i, side: (0, 1 - side[0])),
    ]
    tall = [
        pl.BlockSpec((half, hidden), lambda i, side: (side[0], 0)),
        pl.BlockSpec((half, hidden), lambda i, side: (1 - side[0], 0)),
    ]
    act = jax.ShapeDtypeStruct((rows, hidden), bf16)
    out = jax.ShapeDtypeStruct((rows, half), bf16)
    return pl.pallas_call(
        expert_rows_kernel,
        grid_spec=pltpu.PrefetchScalarGridSpec(
            num_scalar_prefetch=1,
            grid=(1,),
            in_specs=[row_block, row_block, act_block, act_block] + down + tall + tall,
            out_specs=[act_block] * 3 + [row_block] * 2,
        ),
        out_shape=[act] * 3 + [out] * 2,
        name="expert_rows",
    )(side, mine, other, gate_value, up_value, w_down, w_down, w_gate, w_gate, w_up, w_up)


def down_kernel(side, active, mine, other, out):
    @pl.when(pl.program_id(0) == 0)
    def _():
        out[...] = dot(active[...], mine[...], ((0,), (0,))).astype(bf16)

    @pl.when(pl.program_id(0) == 1)
    def _():
        out[...] = dot(active[...], other[...], ((0,), (0,))).astype(bf16)


def tall_kernel(side, gate_grad, up_grad, mine, other, gate_out, up_out):
    def write(rows):
        gate_out[...] = dot(rows, gate_grad[...], ((0,), (0,))).astype(bf16)
        up_out[...] = dot(rows, up_grad[...], ((0,), (0,))).astype(bf16)

    @pl.when(pl.program_id(0) == 0)
    def _():
        write(mine[...])

    @pl.when(pl.program_id(0) == 1)
    def _():
        write(other[...])


def half_of(i, side):
    return lax.rem(i + side[0], 2)


def down_weights(side, active, mine, other):
    rows, half = mine.shape
    hidden = active.shape[1]
    return pl.pallas_call(
        down_kernel,
        grid_spec=pltpu.PrefetchScalarGridSpec(
            num_scalar_prefetch=1,
            grid=(2,),
            in_specs=[whole_block(rows, hidden)] + [whole_block(rows, half)] * 2,
            out_specs=pl.BlockSpec((hidden, half), lambda i, side: (0, half_of(i, side))),
        ),
        out_shape=jax.ShapeDtypeStruct((hidden, 2 * half), bf16),
        name="down_weights",
    )(side, active, mine, other)


def tall_weights(side, gate_grad, up_grad, mine, other):
    rows, half = mine.shape
    hidden = gate_grad.shape[1]
    return pl.pallas_call(
        tall_kernel,
        grid_spec=pltpu.PrefetchScalarGridSpec(
            num_scalar_prefetch=1,
            grid=(2,),
            in_specs=[whole_block(rows, hidden)] * 2 + [whole_block(rows, half)] * 2,
            out_specs=[pl.BlockSpec((half, hidden), lambda i, side: (half_of(i, side), 0))] * 2,
        ),
        out_shape=[jax.ShapeDtypeStruct((2 * half, hidden), bf16)] * 2,
        name="tall_weights",
    )(side, gate_grad, up_grad, mine, other)


def scan_piece(came):
    blocks = came.shape[0]
    values = came[:, :16].reshape(blocks, -1)
    local = came[:, 16:32].reshape(blocks, -1).astype(f32)
    pieces = 4
    lead = lax.rem(lax.axis_index(SP), pieces) == 0
    sums = jnp.where(lead, came[:, 35:38, 0].astype(f32).sum(axis=1), 0.0)
    at = jnp.arange(blocks)
    after = at[None, :] > at[:, None]
    gaps = jnp.zeros((blocks, blocks), f32)
    for k in range(3):
        part = jnp.where(after, came[:, 32 + k, 0][None, :], 0).astype(bf16)
        gaps = gaps + dot(part, after.astype(bf16), ((1,), (0,)))
    weights = jnp.where(after, jnp.exp(gaps), 0.0)
    high = lax.reduce_precision(weights, 8, 7)
    low = weights - high
    later = dot(high.astype(bf16), values, ((1,), (0,))) + dot(
        low.astype(bf16), values, ((1,), (0,))
    )
    own = sums - jnp.sum(later * local, axis=1)
    carried = jnp.sum(jnp.where(after, own[None, :], 0.0), axis=1)
    return later.astype(bf16).reshape(blocks, 16, STATE), carried


def spread(parts, blocks):
    rows = jnp.stack(parts, axis=1)
    rows = jnp.pad(rows, ((0, 0), (0, 8 - len(parts))))
    return jnp.broadcast_to(rows[:, :, None], (blocks, 8, STATE)).astype(bf16)


def exact_dot(a, b, dims):
    return lax.dot_general(
        a, b, (dims, ((), ())), preferred_element_type=f32, precision=lax.Precision.HIGHEST
    )


def grid_of(rows, columns, axis):
    return lax.broadcasted_iota(jnp.int32, (rows, columns), axis)


def route_kernel(side, choice, weight, cotangent, grads, places):
    tokens = choice.shape[1]
    slots = places.shape[0]
    experts = slots // 8
    expert_at = grid_of(experts, tokens, 0)
    hot = [(expert_at == choice[k : k + 1, :]).astype(f32) for k in range(2)]
    before = (grid_of(tokens, tokens, 0) < grid_of(tokens, tokens, 1)).astype(bf16)
    earlier = dot((hot[0] + hot[1]).astype(bf16), before, ((1,), (0,)))
    same = (grid_of(tokens, tokens, 0) == grid_of(tokens, tokens, 1)).astype(f32)
    weights = exact_dot(same, weight[...], ((1,), (1,)))
    cotangents = cotangent[...].astype(f32)
    slot_at = grid_of(slots, tokens, 0)
    either = jnp.zeros((slots, tokens), f32)
    sent = jnp.zeros((slots, cotangent.shape[1]), f32)
    for k in range(2):
        rank = jnp.sum(earlier * hot[k], axis=0, keepdims=True).astype(jnp.int32)
        taken = (slot_at == choice[k : k + 1, :] * 8 + rank).astype(f32)
        either = either + taken
        rows = (weights[:, k : k + 1] * cotangents).astype(bf16)
        sent = sent + dot(taken.astype(bf16), rows, ((1,), (0,)))
    grads[...] = sent.astype(bf16)
    places[...] = either.astype(bf16)


def route(side, choice, weight, cotangent, slots):
    tokens, width = cotangent.shape
    half = width // 2
    return pl.pallas_call(
        route_kernel,
        grid_spec=pltpu.PrefetchScalarGridSpec(
            num_scalar_prefetch=1,
            grid=(1,),
            in_specs=[
                whole_block(*choice.shape),
                whole_block(*weight.shape),
                pl.BlockSpec((tokens, half), lambda i, side: (0, side[0])),
            ],
            out_specs=[whole_block(slots, half), whole_block(slots, tokens)],
        ),
        out_shape=[
            jax.ShapeDtypeStruct((slots, half), bf16),
            jax.ShapeDtypeStruct((slots, tokens), bf16),
        ],
        name="route",
    )(side, choice, weight, cotangent)


GROUP = 256
PER_GROUP = GROUP // HEAD_DIM


def per_head(rows, first):
    return jnp.concatenate(
        [
            jnp.broadcast_to(rows[first + r : first + r + 1, :], (HEAD_DIM, rows.shape[1]))
            for r in range(PER_GROUP)
        ],
        axis=0,
    )


def head_sums(x):
    return [
        jnp.sum(x[r * HEAD_DIM : (r + 1) * HEAD_DIM, :], axis=0, keepdims=True)
        for r in range(PER_GROUP)
    ]


def forward_kernel(
    scan_in, gate_in, b_proj, c_proj, log_decay, entry, gain, cotangent,
    mixed, gated_out, silu_out, slope_out, mix_out, decay_out, x_out, tail_out, local_out,
    rows_out, inverse_out, carry_out, cotangent_out,
):
    tokens = scan_in.shape[0]
    groups = scan_in.shape[1] // GROUP
    down, across = grid_of(tokens, tokens, 0), grid_of(tokens, tokens, 1)
    decays = log_decay[...]
    cum_rows = exact_dot(decays, (down <= across).astype(f32), ((1,), (0,)))
    cum_columns = exact_dot((across <= down).astype(f32), decays, ((1,), (1,)))
    total = cum_rows[:, tokens - 1 :]
    growth = jnp.exp(cum_rows)
    tail = jnp.exp(total - cum_rows)
    totals = jnp.broadcast_to(total, growth.shape)
    causal = down >= across
    for g in range(groups):
        span = slice(g * GROUP, (g + 1) * GROUP)
        states = slice(g * STATE, (g + 1) * STATE)
        first = g * PER_GROUP
        b_group, c_group = b_proj[:, states], c_proj[:, states]
        inner = dot(c_group, b_group, ((1,), (1,)))
        x = jnp.transpose(scan_in[:, span].astype(f32))
        x_b = x.astype(bf16)
        carried = dot(entry[span, :].astype(bf16), c_group, ((1,), (1,)))
        within = []
        for r in range(PER_GROUP):
            h = first + r
            gaps = cum_columns[:, h : h + 1] - cum_rows[h : h + 1, :]
            decay = jnp.where(causal, jnp.exp(jnp.where(causal, gaps, 0.0)), 0.0)
            decay_out[h] = decay
            mix = (inner * decay).astype(bf16)
            mix_out[h] = mix
            within.append(dot(x_b[r * HEAD_DIM : (r + 1) * HEAD_DIM, :], mix, ((1,), (1,))))
        carried = carried * per_head(growth, first)
        scan_out = jnp.concatenate(within, axis=0) + carried
        gate = jnp.transpose(gate_in[:, span].astype(f32))
        sig = jax.nn.sigmoid(gate)
        silu = gate * sig
        gated = scan_out * silu
        inverse = lax.rsqrt(jnp.mean(gated * gated, axis=0, keepdims=True) + rms_epsilon)
        mixed[span, :] = (gated * inverse * gain[span, :]).astype(bf16)
        gated_out[span, :] = gated
        silu_out[span, :] = silu
        slope_out[span, :] = scan_out * sig * (1.0 + gate * (1.0 - sig))
        carry_out[span, :] = carried * silu
        cotangent_out[span, :] = jnp.transpose(cotangent[:, span].astype(f32)).astype(bf16)
        inverse_out[g] = inverse
        for k, part in enumerate((growth, tail, totals)):
            rows_out[k, g] = part[first : first + PER_GROUP, :]
        x_out[span, :] = x_b
        x_tail = (x * per_head(tail, first)).astype(bf16)
        tail_out[span, :] = x_tail
        local_out[span, :] = dot(x_tail, b_group, ((1,), (0,))).astype(bf16)


def whole_call(kernel, out_shape, *args):
    return pl.pallas_call(kernel, out_shape=[jax.ShapeDtypeStruct(*x) for x in out_shape])(*args)


def forward(scan_in, gate_in, b_proj, c_proj, log_decay, entry, gain, cotangent):
    tokens, inner = scan_in.shape
    heads = log_decay.shape[0]
    return whole_call(
        forward_kernel,
        [
            ((inner, tokens), bf16),
            ((inner, tokens), f32),
            ((inner, tokens), f32),
            ((inner, tokens), f32),
            ((heads, tokens, tokens), bf16),
            ((heads, tokens, tokens), f32),
            ((inner, tokens), bf16),
            ((inner, tokens), bf16),
            ((inner, STATE), bf16),
            ((3, inner // GROUP, PER_GROUP, tokens), f32),
            ((inner // GROUP, 1, tokens), f32),
            ((inner, tokens), f32),
            ((cotangent.shape[1], tokens), bf16),
        ],
        scan_in, gate_in, b_proj, c_proj, log_decay, entry, gain, cotangent,
    )


def spread_parts(x, heads, pieces):
    high = x.astype(bf16)
    rest = x - high.astype(f32)
    middle = rest.astype(bf16)
    low = (rest - middle.astype(f32)).astype(bf16)
    return [
        jnp.broadcast_to(part.astype(f32)[:, None, :], (heads, pieces, STATE)).reshape(
            heads * pieces, 1, STATE
        )
        for part in (high, middle, low)
    ]


def message_kernel(
    side, grad_own, grad_far, out_own, out_far, gain, gated_in, silu_in, carry_in, c_proj, local_in,
    rows_in, inverse_in,
    message, grad_out,
):
    pieces = GROUP // 16
    grad_mixed = dot(out_own[...], grad_own[...], ((1,), (0,)))
    grad_mixed = grad_mixed + dot(out_far[...], grad_far[...], ((1,), (0,)))
    inverse = inverse_in[0]
    unit = gated_in[...] * inverse
    grad_unit = grad_mixed * gain[...]
    mean = jnp.mean(grad_unit * unit, axis=0, keepdims=True)
    grad_gated = inverse * (grad_unit - unit * mean)
    grad_out[...] = grad_gated
    grown = (grad_gated * silu_in[...] * per_head(rows_in[0, 0], 0)).astype(bf16)
    block_state = dot(grown, c_proj[...], ((1,), (0,))).astype(bf16)
    message[:, 0:16, :] = block_state.reshape(pieces, 16, STATE)
    message[:, 16:32, :] = local_in[...].reshape(pieces, 16, STATE)
    own = jnp.concatenate(head_sums(grad_gated * carry_in[...]), axis=0)
    own = jnp.broadcast_to(jnp.sum(own, axis=1, keepdims=True), (PER_GROUP, STATE))
    per = pieces // PER_GROUP
    zero = jnp.zeros((pieces, 2, STATE), f32)
    extra = jnp.concatenate(
        spread_parts(rows_in[2, 0], PER_GROUP, per) + spread_parts(own, PER_GROUP, per) + [zero],
        axis=1,
    )
    message[:, 32:40, :] = extra.astype(bf16)


def state_message(side, grad_own, grad_far, w_out, gain, gated, silu, carry, c_proj, local, rows, inverse):
    half, tokens = grad_own.shape
    inner = gain.shape[0]
    pieces = GROUP // 16
    channels = pl.BlockSpec((GROUP, tokens), lambda i, side: (i, 0))
    return pl.pallas_call(
        message_kernel,
        grid_spec=pltpu.PrefetchScalarGridSpec(
            num_scalar_prefetch=1,
            grid=(inner // GROUP,),
            in_specs=[
                whole_block(half, tokens),
                whole_block(half, tokens),
                pl.BlockSpec((GROUP, half), lambda i, side: (i, side[0])),
                pl.BlockSpec((GROUP, half), lambda i, side: (i, 1 - side[0])),
                pl.BlockSpec((GROUP, 1), lambda i, side: (i, 0)),
                channels,
                channels,
                channels,
                pl.BlockSpec((tokens, STATE), lambda i, side: (0, i)),
                pl.BlockSpec((GROUP, STATE), lambda i, side: (i, 0)),
                pl.BlockSpec((3, 1, PER_GROUP, tokens), lambda i, side: (0, i, 0, 0)),
                pl.BlockSpec((1, 1, tokens), lambda i, side: (i, 0, 0)),
            ],
            out_specs=[
                pl.BlockSpec((pieces, 40, STATE), lambda i, side: (i, 0, 0)),
                channels,
            ],
        ),
        out_shape=[
            jax.ShapeDtypeStruct((inner // 16, 40, STATE), bf16),
            jax.ShapeDtypeStruct((inner, tokens), f32),
        ],
        name="message",
    )(side, grad_own, grad_far, w_out, w_out, gain, gated, silu, carry, c_proj, local, rows, inverse)


def inside_kernel(
    grad_in, gated_in, silu_in, slope_in, mix_in, decay_in, x_in, b_proj, c_proj, entry, rows_in,
    gate_grad, x_grad, b_grad, c_grad, y_dots,
):
    tokens = x_in.shape[1]
    for g in range(x_in.shape[0] // GROUP):
        span = slice(g * GROUP, (g + 1) * GROUP)
        states = slice(g * STATE, (g + 1) * STATE)
        first = g * PER_GROUP
        grad_gated = grad_in[span, :]
        gate_grad[:, span] = jnp.transpose(grad_gated * slope_in[span, :]).astype(bf16)
        grad_y = grad_gated * silu_in[span, :]
        grad_y_b = grad_y.astype(bf16)
        grown = (grad_y * per_head(rows_in[0, g], 0)).astype(bf16)
        b_group, c_group = b_proj[:, states], c_proj[:, states]
        x = x_in[span, :]
        weights = jnp.zeros((tokens, tokens), f32)
        inside = []
        for r in range(PER_GROUP):
            h = first + r
            head = slice(r * HEAD_DIM, (r + 1) * HEAD_DIM)
            inside.append(dot(grad_y_b[head, :], mix_in[h], ((1,), (0,))))
            weights = weights + decay_in[h] * dot(grad_y_b[head, :], x[head, :], ((0,), (0,)))
        x_grad[span, :] = jnp.concatenate(inside, axis=0)
        weights = weights.astype(bf16)
        c_grad[:, states] = (
            dot(weights, b_group, ((1,), (0,)))
            + dot(grown, entry[span, :].astype(bf16), ((0,), (0,)))
        ).astype(bf16)
        b_grad[:, states] = dot(weights, c_group, ((0,), (0,)))
        y_dots[first : first + PER_GROUP, :] = jnp.concatenate(
            head_sums(grad_gated * gated_in[span, :]), axis=0
        )


def inside_grads(grad, gated, silu, slope, mix, decay, x, b_proj, c_proj, entry, rows):
    inner, tokens = grad.shape
    return whole_call(
        inside_kernel,
        [
            ((tokens, inner), bf16),
            ((inner, tokens), f32),
            (b_proj.shape, f32),
            (b_proj.shape, bf16),
            ((decay.shape[0], tokens), f32),
        ],
        grad, gated, silu, slope, mix, decay, x, b_proj, c_proj, entry, rows,
    )


def final_kernel(back, b_proj, x_in, tail_in, rows_in, x_inside, y_dots, b_inside, x_grad, b_grad, decay_grad):
    groups = x_in.shape[0] // GROUP
    pieces = GROUP // 16
    tokens = x_in.shape[1]
    heads = y_dots.shape[0]
    dots = []
    for g in range(groups):
        span = slice(g * GROUP, (g + 1) * GROUP)
        states = slice(g * STATE, (g + 1) * STATE)
        later = back[g * pieces : (g + 1) * pieces, 0:16, :].reshape(GROUP, STATE)
        carried = dot(later, b_proj[:, states], ((1,), (1,)))
        grad = x_inside[span, :] + carried * per_head(rows_in[1, g], 0)
        x_grad[:, span] = jnp.transpose(grad).astype(bf16)
        b_grad[:, states] = (
            b_inside[:, states] + dot(tail_in[span, :], later, ((0,), (0,)))
        ).astype(bf16)
        dots = dots + head_sums(x_in[span, :].astype(f32) * grad)
    own = y_dots[...] - jnp.concatenate(dots, axis=0)
    after = (grid_of(tokens, tokens, 0) >= grid_of(tokens, tokens, 1)).astype(f32)
    extra = jnp.sum(back[:, 16:24, :].astype(f32), axis=1)
    extra = jnp.sum(extra.reshape(heads, extra.shape[0] // heads, STATE), axis=1)
    decay_grad[...] = exact_dot(own, after, ((1,), (0,))) + extra


def final(back, b_proj, x, x_tail, rows, x_inside, y_dots, b_inside):
    inner, tokens = x.shape
    return whole_call(
        final_kernel,
        [
            ((tokens, inner), bf16),
            (b_proj.shape, bf16),
            (y_dots.shape, f32),
        ],
        back, b_proj, x, x_tail, rows, x_inside, y_dots, b_inside,
    )


def body(
    mixer_output,
    layer_cotangent,
    expert_choice,
    route_weight,
    gate_pre,
    up_pre,
    w_gate,
    w_up,
    w_down,
    w_out,
    norm_gain,
    scan_in,
    gate_in,
    b_proj,
    c_proj,
    log_decay,
    entry_state,
):
    experts = lax.axis_size(SP)
    _, width = mixer_output.shape
    capacity = gate_pre.shape[1] // experts
    half = width // 2
    start = lax.axis_index("tp") * half

    side = lax.axis_index("tp")[None]
    send_grads, either = route(
        side, expert_choice.T, route_weight.T, layer_cotangent, experts * capacity
    )
    hidden_half = lax.dynamic_slice_in_dim(mixer_output, start, half, 1)
    cotangent_half = lax.dynamic_slice_in_dim(layer_cotangent, start, half, 1)
    send_hidden = dot(either, hidden_half, ((1,), (0,))).astype(bf16)
    send_grads = send_grads.reshape(experts, capacity, half)
    send_hidden = send_hidden.reshape(experts, capacity, half)
    inner = scan_in.shape[1]
    gain = norm_gain.astype(f32)[:, None]
    entry = entry_state.reshape(inner, STATE)
    mixed, *saved, x_tail, local, rows, inverse, carry, cotangent_rows = forward(
        scan_in, gate_in, b_proj, c_proj, log_decay.T, entry, gain, cotangent_half
    )
    gated, silu, slope, mix, decay, x = saved
    came_grads = lax.all_to_all(send_grads, SP, 0, 0, tiled=True)
    send_hidden, came_grads = lax.optimization_barrier((send_hidden, came_grads))
    came_hidden = lax.all_to_all(send_hidden, SP, 0, 0, tiled=True)
    grads_own = came_grads.reshape(-1, half)
    grads_far = swapped(grads_own)
    active, gate_grad, up_grad, rows_own, rows_far = expert_rows(
        side, grads_own, grads_far, gate_pre[0], up_pre[0], w_down[0], w_gate[0], w_up[0]
    )
    summed = (rows_own.astype(f32) + swapped(rows_far).astype(f32)).astype(bf16)
    summed, came_hidden = lax.optimization_barrier((summed, came_hidden))
    returned = lax.all_to_all(summed.reshape(experts, capacity, half), SP, 0, 0, tiled=True)
    hidden_own = came_hidden.reshape(-1, half)
    hidden_far = swapped(hidden_own)
    down_wgrad = down_weights(side, active, grads_own, grads_far)
    gate_wgrad, up_wgrad = tall_weights(side, gate_grad, up_grad, hidden_own, hidden_far)
    moe_terms = dot(returned.reshape(-1, half), either, ((0,), (0,)))
    grad_own = (cotangent_rows.astype(f32) + moe_terms).astype(bf16)
    grad_far = swapped(grad_own)
    grad_hidden = jnp.where(
        side == 0,
        jnp.concatenate([grad_own, grad_far], axis=0),
        jnp.concatenate([grad_far, grad_own], axis=0),
    )

    message, grad_gated = state_message(
        side, grad_own, grad_far, w_out, gain, gated, silu, carry, c_proj, local, rows, inverse
    )
    came_states = lax.all_to_all(message, SP, 0, 0, tiled=True)
    later, carried = scan_piece(came_states)
    back = jnp.concatenate([later, spread(list(three_parts(carried)), experts)], axis=1)
    grad_gate_in, x_inside, b_inside, grad_c_proj, y_dots = inside_grads(
        grad_gated, gated, silu, slope, mix, decay, x, b_proj, c_proj, entry, rows
    )
    back = lax.all_to_all(back, SP, 0, 0, tiled=True)
    grad_scan_in, grad_b_proj, decay_grad = final(
        back, b_proj, x, x_tail, rows, x_inside, y_dots, b_inside
    )
    grad_log_decay = decay_grad.T

    line = lax.axis_size("sp_0")
    mixed, gate_wgrad = lax.optimization_barrier((mixed, gate_wgrad))
    mixed_line = from_line([mixed] * line, "sp_0")
    grads_line = from_line(pieces_for(grad_hidden, "sp_0", 0), "sp_0")
    product = dot(
        jnp.concatenate(grads_line, axis=1), jnp.concatenate(mixed_line, axis=1), ((1,), (1,))
    ).astype(bf16)
    parts = from_line(pieces_for(product, "sp_1", 0), "sp_1")
    product = sum(part.astype(f32) for part in parts).astype(bf16)
    parts = from_line(pieces_for(product, "sp_2", 0), "sp_2")
    grad_out_proj = sum(part.astype(f32) for part in parts)

    return (
        gate_wgrad[None],
        up_wgrad[None],
        down_wgrad[None],
        grad_out_proj,
        grad_scan_in,
        grad_gate_in,
        grad_b_proj,
        grad_c_proj,
        grad_log_decay,
    )


def solution(mesh):
    split = Mesh(mesh.devices.reshape(4, 4, 4, mesh.shape["tp"]), ("sp_0", "sp_1", "sp_2", "tp"))
    return jax.shard_map(
        body,
        mesh=split,
        in_specs=(
            P(SP, None),
            P(SP, None),
            P(SP, None),
            P(SP, None),
            P(SP, None, "tp"),
            P(SP, None, "tp"),
            P(SP, None, "tp"),
            P(SP, None, "tp"),
            P(SP, "tp", None),
            P("tp", None),
            P("tp"),
            P(SP, "tp"),
            P(SP, "tp"),
            P(SP, "tp"),
            P(SP, "tp"),
            P(SP, "tp"),
            P(SP, "tp", None, None),
        ),
        out_specs=(
            P(SP, None, "tp"),
            P(SP, None, "tp"),
            P(SP, "tp", None),
            P(SP, "tp"),
            P(SP, "tp"),
            P(SP, "tp"),
            P(SP, "tp"),
            P(SP, "tp"),
            P(SP, "tp"),
        ),
        check_vma=False,
    )
```

```python
import jax
import jax.numpy as jnp
from jax import lax
from jax.sharding import Mesh
from jax.experimental import pallas as pl
from jax.experimental.pallas import tpu as pltpu
from jax.sharding import PartitionSpec as P

HEAD_DIM = 64
STATE = 128
SP = ("sp_0", "sp_1", "sp_2")


rms_epsilon = 1e-05
clamp_limit = 7.0
swish_alpha = 1.702

bf16 = jnp.bfloat16
f32 = jnp.float32


def dot(a, b, dims):
    return lax.dot_general(a, b, (dims, ((), ())), preferred_element_type=f32)


def swapped(x):
    return lax.ppermute(x, "tp", [(0, 1), (1, 0)])


def from_line(parts, axis):
    size = lax.axis_size(axis)
    return [parts[0]] + [
        lax.ppermute(parts[k], axis, [(i, (i + k) % size) for i in range(size)])
        for k in range(1, size)
    ]


def pieces_for(x, axis, dim):
    size, spot = lax.axis_size(axis), lax.axis_index(axis)
    span = x.shape[dim] // size
    return [
        lax.dynamic_slice_in_dim(x, lax.rem(spot + k, size) * span, span, dim) for k in range(size)
    ]


def expert_rows_kernel(
    side, mine, other, gate_value, up_value, down_own, down_far, gate_own, gate_far, up_own, up_far,
    active, gate_grad, up_grad, rows_own, rows_far,
):
    act_grad = dot(mine[...], down_own[...], ((1,), (1,)))
    act_grad = act_grad + dot(other[...], down_far[...], ((1,), (1,)))
    gate_full = gate_value[...].astype(f32)
    up_full = up_value[...].astype(f32)
    gate_clip = jnp.minimum(gate_full, clamp_limit)
    up_clip = jnp.clip(up_full, -clamp_limit, clamp_limit)
    sigmoid_gate = jax.nn.sigmoid(swish_alpha * gate_clip)
    swish_gate = gate_clip * sigmoid_gate
    active[...] = ((up_clip + 1.0) * swish_gate).astype(bf16)
    inside = (up_full > -clamp_limit) & (up_full < clamp_limit)
    up_side = jnp.where(inside, act_grad * swish_gate, 0.0).astype(bf16)
    slope = sigmoid_gate + swish_alpha * gate_clip * sigmoid_gate * (1.0 - sigmoid_gate)
    gate_side = jnp.where(
        gate_full < clamp_limit, act_grad * (up_clip + 1.0) * slope, 0.0
    ).astype(bf16)
    up_grad[...] = up_side
    gate_grad[...] = gate_side
    far = dot(gate_side, gate_far[...], ((1,), (1,))) + dot(up_side, up_far[...], ((1,), (1,)))
    rows_far[...] = far.astype(bf16)
    own = dot(gate_side, gate_own[...], ((1,), (1,))) + dot(up_side, up_own[...], ((1,), (1,)))
    rows_own[...] = own.astype(bf16)


def whole_block(*shape):
    return pl.BlockSpec(shape, lambda i, side: (0,) * len(shape))


def expert_rows(side, mine, other, gate_value, up_value, w_down, w_gate, w_up):
    rows, half = mine.shape
    hidden = gate_value.shape[1]
    row_block = whole_block(rows, half)
    act_block = whole_block(rows, hidden)
    down = [
        pl.BlockSpec((hidden, half), lambda i, side: (0, side[0])),
        pl.BlockSpec((hidden, half), lambda i, side: (0, 1 - side[0])),
    ]
    tall = [
        pl.BlockSpec((half, hidden), lambda i, side: (side[0], 0)),
        pl.BlockSpec((half, hidden), lambda i, side: (1 - side[0], 0)),
    ]
    act = jax.ShapeDtypeStruct((rows, hidden), bf16)
    out = jax.ShapeDtypeStruct((rows, half), bf16)
    return pl.pallas_call(
        expert_rows_kernel,
        grid_spec=pltpu.PrefetchScalarGridSpec(
            num_scalar_prefetch=1,
            grid=(1,),
            in_specs=[row_block, row_block, act_block, act_block] + down + tall + tall,
            out_specs=[act_block] * 3 + [row_block] * 2,
        ),
        out_shape=[act] * 3 + [out] * 2,
        name="expert_rows",
    )(side, mine, other, gate_value, up_value, w_down, w_down, w_gate, w_gate, w_up, w_up)


def weights_kernel(
    side, active, gate_grad, up_grad, grads_own, grads_far, hidden_own, hidden_far,
    down_out, gate_out, up_out,
):
    def write(grads, hidden):
        down_out[...] = dot(active[...], grads, ((0,), (0,))).astype(bf16)
        gate_out[...] = dot(hidden, gate_grad[...], ((0,), (0,))).astype(bf16)
        up_out[...] = dot(hidden, up_grad[...], ((0,), (0,))).astype(bf16)

    @pl.when(pl.program_id(0) < 2)
    def _():
        write(grads_own[...], hidden_own[...])

    @pl.when(pl.program_id(0) >= 2)
    def _():
        write(grads_far[...], hidden_far[...])


def expert_weights(side, active, gate_grad, up_grad, grads_own, grads_far, hidden_own, hidden_far):
    rows, half = grads_own.shape
    hidden = active.shape[1]
    own = pl.BlockSpec((rows, half // 2), lambda i, side: (0, jnp.minimum(i, 1)))
    far = pl.BlockSpec((rows, half // 2), lambda i, side: (0, jnp.maximum(i - 2, 0)))

    def place(i, side):
        return lax.rem(i + 2 * side[0], 4)

    tall = pl.BlockSpec((half // 2, hidden), lambda i, side: (place(i, side), 0))
    return pl.pallas_call(
        weights_kernel,
        grid_spec=pltpu.PrefetchScalarGridSpec(
            num_scalar_prefetch=1,
            grid=(4,),
            in_specs=[whole_block(rows, hidden)] * 3 + [own, far, own, far],
            out_specs=[
                pl.BlockSpec((hidden, half // 2), lambda i, side: (0, place(i, side))),
                tall,
                tall,
            ],
        ),
        out_shape=[jax.ShapeDtypeStruct((hidden, 2 * half), bf16)]
        + [jax.ShapeDtypeStruct((2 * half, hidden), bf16)] * 2,
        name="weights",
    )(side, active, gate_grad, up_grad, grads_own, grads_far, hidden_own, hidden_far)


def exact_dot(a, b, dims):
    return lax.dot_general(
        a, b, (dims, ((), ())), preferred_element_type=f32, precision=lax.Precision.HIGHEST
    )


def grid_of(rows, columns, axis):
    return lax.broadcasted_iota(jnp.int32, (rows, columns), axis)


def route_kernel(side, choice, weight, cotangent, grads, places):
    tokens = choice.shape[1]
    slots = places.shape[0]
    experts = slots // 8
    expert_at = grid_of(experts, tokens, 0)
    hot = [(expert_at == choice[k : k + 1, :]).astype(f32) for k in range(2)]
    before = (grid_of(tokens, tokens, 0) < grid_of(tokens, tokens, 1)).astype(bf16)
    earlier = dot((hot[0] + hot[1]).astype(bf16), before, ((1,), (0,)))
    same = (grid_of(tokens, tokens, 0) == grid_of(tokens, tokens, 1)).astype(f32)
    weights = exact_dot(same, weight[...], ((1,), (1,)))
    cotangents = cotangent[...].astype(f32)
    slot_at = grid_of(slots, tokens, 0)
    either = jnp.zeros((slots, tokens), f32)
    sent = jnp.zeros((slots, cotangent.shape[1]), f32)
    for k in range(2):
        rank = jnp.sum(earlier * hot[k], axis=0, keepdims=True).astype(jnp.int32)
        taken = (slot_at == choice[k : k + 1, :] * 8 + rank).astype(f32)
        either = either + taken
        rows = (weights[:, k : k + 1] * cotangents).astype(bf16)
        sent = sent + dot(taken.astype(bf16), rows, ((1,), (0,)))
    grads[...] = sent.astype(bf16)
    places[...] = either.astype(bf16)


def route(side, choice, weight, cotangent, slots):
    tokens, width = cotangent.shape
    half = width // 2
    return pl.pallas_call(
        route_kernel,
        grid_spec=pltpu.PrefetchScalarGridSpec(
            num_scalar_prefetch=1,
            grid=(1,),
            in_specs=[
                whole_block(*choice.shape),
                whole_block(*weight.shape),
                pl.BlockSpec((tokens, half), lambda i, side: (0, side[0])),
            ],
            out_specs=[whole_block(slots, half), whole_block(slots, tokens)],
        ),
        out_shape=[
            jax.ShapeDtypeStruct((slots, half), bf16),
            jax.ShapeDtypeStruct((slots, tokens), bf16),
        ],
        name="route",
    )(side, choice, weight, cotangent)


GROUP = 256
PER_GROUP = GROUP // HEAD_DIM


def per_head(rows, first):
    return jnp.concatenate(
        [
            jnp.broadcast_to(rows[first + r : first + r + 1, :], (HEAD_DIM, rows.shape[1]))
            for r in range(PER_GROUP)
        ],
        axis=0,
    )


def head_sums(x):
    return [
        jnp.sum(x[r * HEAD_DIM : (r + 1) * HEAD_DIM, :], axis=0, keepdims=True)
        for r in range(PER_GROUP)
    ]


def forward_kernel(
    scan_in, gate_in, b_proj, c_proj, log_decay, entry, gain, cotangent,
    mixed, gated_out, silu_out, slope_out, mix_out, decay_out, x_out, tail_out, local_out,
    rows_out, inverse_out, carry_out, cotangent_out,
):
    tokens = scan_in.shape[0]
    groups = scan_in.shape[1] // GROUP
    down, across = grid_of(tokens, tokens, 0), grid_of(tokens, tokens, 1)
    decays = log_decay[...]
    cum_rows = exact_dot(decays, (down <= across).astype(f32), ((1,), (0,)))
    cum_columns = exact_dot((across <= down).astype(f32), decays, ((1,), (1,)))
    total = cum_rows[:, tokens - 1 :]
    growth = jnp.exp(cum_rows)
    tail = jnp.exp(total - cum_rows)
    totals = jnp.broadcast_to(total, growth.shape)
    causal = down >= across
    for g in range(groups):
        span = slice(g * GROUP, (g + 1) * GROUP)
        states = slice(g * STATE, (g + 1) * STATE)
        first = g * PER_GROUP
        b_group, c_group = b_proj[:, states], c_proj[:, states]
        inner = dot(c_group, b_group, ((1,), (1,)))
        x = jnp.transpose(scan_in[:, span].astype(f32))
        x_b = x.astype(bf16)
        carried = dot(entry[span, :].astype(bf16), c_group, ((1,), (1,)))
        within = []
        for r in range(PER_GROUP):
            h = first + r
            gaps = cum_columns[:, h : h + 1] - cum_rows[h : h + 1, :]
            decay = jnp.where(causal, jnp.exp(jnp.where(causal, gaps, 0.0)), 0.0)
            decay_out[h] = decay
            mix = (inner * decay).astype(bf16)
            mix_out[h] = mix
            within.append(dot(x_b[r * HEAD_DIM : (r + 1) * HEAD_DIM, :], mix, ((1,), (1,))))
        carried = carried * per_head(growth, first)
        scan_out = jnp.concatenate(within, axis=0) + carried
        gate = jnp.transpose(gate_in[:, span].astype(f32))
        sig = jax.nn.sigmoid(gate)
        silu = gate * sig
        gated = scan_out * silu
        inverse = lax.rsqrt(jnp.mean(gated * gated, axis=0, keepdims=True) + rms_epsilon)
        mixed[span, :] = (gated * inverse * gain[span, :]).astype(bf16)
        gated_out[span, :] = gated
        silu_out[span, :] = silu
        slope_out[span, :] = scan_out * sig * (1.0 + gate * (1.0 - sig))
        carry_out[span, :] = carried * silu
        cotangent_out[span, :] = jnp.transpose(cotangent[:, span].astype(f32)).astype(bf16)
        inverse_out[g] = inverse
        for k, part in enumerate((growth, tail, totals)):
            rows_out[k, g] = part[first : first + PER_GROUP, :]
        x_out[span, :] = x_b
        x_tail = (x * per_head(tail, first)).astype(bf16)
        tail_out[span, :] = x_tail
        local_out[span, :] = dot(x_tail, b_group, ((1,), (0,))).astype(bf16)


def whole_call(kernel, out_shape, *args):
    return pl.pallas_call(kernel, out_shape=[jax.ShapeDtypeStruct(*x) for x in out_shape])(*args)


def forward(scan_in, gate_in, b_proj, c_proj, log_decay, entry, gain, cotangent):
    tokens, inner = scan_in.shape
    heads = log_decay.shape[0]
    return whole_call(
        forward_kernel,
        [
            ((inner, tokens), bf16),
            ((inner, tokens), f32),
            ((inner, tokens), f32),
            ((inner, tokens), f32),
            ((heads, tokens, tokens), bf16),
            ((heads, tokens, tokens), f32),
            ((inner, tokens), bf16),
            ((inner, tokens), bf16),
            ((inner, STATE), bf16),
            ((3, inner // GROUP, PER_GROUP, tokens), f32),
            ((inner // GROUP, 1, tokens), f32),
            ((inner, tokens), f32),
            ((cotangent.shape[1], tokens), bf16),
        ],
        scan_in, gate_in, b_proj, c_proj, log_decay, entry, gain, cotangent,
    )


def spread_parts(x, heads, pieces):
    high = x.astype(bf16)
    rest = x - high.astype(f32)
    middle = rest.astype(bf16)
    low = (rest - middle.astype(f32)).astype(bf16)
    return [
        jnp.broadcast_to(part.astype(f32)[:, None, :], (heads, pieces, STATE)).reshape(
            heads * pieces, 1, STATE
        )
        for part in (high, middle, low)
    ]


def message_kernel(
    side, grad_own, grad_far, out_own, out_far, gain, gated_in, silu_in, carry_in, c_proj, local_in,
    rows_in, inverse_in,
    message, grad_out,
):
    pieces = GROUP // 16
    grad_mixed = dot(out_own[...], grad_own[...], ((1,), (0,)))
    grad_mixed = grad_mixed + dot(out_far[...], grad_far[...], ((1,), (0,)))
    inverse = inverse_in[0]
    unit = gated_in[...] * inverse
    grad_unit = grad_mixed * gain[...]
    mean = jnp.mean(grad_unit * unit, axis=0, keepdims=True)
    grad_gated = inverse * (grad_unit - unit * mean)
    grad_out[...] = grad_gated
    grown = (grad_gated * silu_in[...] * per_head(rows_in[0, 0], 0)).astype(bf16)
    block_state = dot(grown, c_proj[...], ((1,), (0,))).astype(bf16)
    message[:, 0:16, :] = block_state.reshape(pieces, 16, STATE)
    message[:, 16:32, :] = local_in[...].reshape(pieces, 16, STATE)
    own = jnp.concatenate(head_sums(grad_gated * carry_in[...]), axis=0)
    own = jnp.broadcast_to(jnp.sum(own, axis=1, keepdims=True), (PER_GROUP, STATE))
    per = pieces // PER_GROUP
    zero = jnp.zeros((pieces, 2, STATE), f32)
    extra = jnp.concatenate(
        spread_parts(rows_in[2, 0], PER_GROUP, per) + spread_parts(own, PER_GROUP, per) + [zero],
        axis=1,
    )
    message[:, 32:40, :] = extra.astype(bf16)


def state_message(side, grad_own, grad_far, w_out, gain, gated, silu, carry, c_proj, local, rows, inverse):
    half, tokens = grad_own.shape
    inner = gain.shape[0]
    pieces = GROUP // 16
    channels = pl.BlockSpec((GROUP, tokens), lambda i, side: (i, 0))
    return pl.pallas_call(
        message_kernel,
        grid_spec=pltpu.PrefetchScalarGridSpec(
            num_scalar_prefetch=1,
            grid=(inner // GROUP,),
            in_specs=[
                whole_block(half, tokens),
                whole_block(half, tokens),
                pl.BlockSpec((GROUP, half), lambda i, side: (i, side[0])),
                pl.BlockSpec((GROUP, half), lambda i, side: (i, 1 - side[0])),
                pl.BlockSpec((GROUP, 1), lambda i, side: (i, 0)),
                channels,
                channels,
                channels,
                pl.BlockSpec((tokens, STATE), lambda i, side: (0, i)),
                pl.BlockSpec((GROUP, STATE), lambda i, side: (i, 0)),
                pl.BlockSpec((3, 1, PER_GROUP, tokens), lambda i, side: (0, i, 0, 0)),
                pl.BlockSpec((1, 1, tokens), lambda i, side: (i, 0, 0)),
            ],
            out_specs=[
                pl.BlockSpec((pieces, 40, STATE), lambda i, side: (i, 0, 0)),
                channels,
            ],
        ),
        out_shape=[
            jax.ShapeDtypeStruct((inner // 16, 40, STATE), bf16),
            jax.ShapeDtypeStruct((inner, tokens), f32),
        ],
        name="message",
    )(side, grad_own, grad_far, w_out, w_out, gain, gated, silu, carry, c_proj, local, rows, inverse)


def inside_kernel(
    grad_in, gated_in, silu_in, slope_in, mix_in, decay_in, x_in, b_proj, c_proj, entry, rows_in,
    gate_grad, x_grad, b_grad, c_grad, y_dots,
):
    tokens = x_in.shape[1]
    grad_gated = grad_in[...]
    gate_grad[...] = jnp.transpose(grad_gated * slope_in[...]).astype(bf16)
    grad_y = grad_gated * silu_in[...]
    grad_y_b = grad_y.astype(bf16)
    grown = (grad_y * per_head(rows_in[0, 0], 0)).astype(bf16)
    x = x_in[...]
    weights = jnp.zeros((tokens, tokens), f32)
    inside = []
    for r in range(PER_GROUP):
        head = slice(r * HEAD_DIM, (r + 1) * HEAD_DIM)
        inside.append(dot(grad_y_b[head, :], mix_in[r], ((1,), (0,))))
        weights = weights + decay_in[r] * dot(grad_y_b[head, :], x[head, :], ((0,), (0,)))
    x_grad[...] = jnp.concatenate(inside, axis=0)
    weights = weights.astype(bf16)
    c_grad[...] = (
        dot(weights, b_proj[...], ((1,), (0,)))
        + dot(grown, entry[...].astype(bf16), ((0,), (0,)))
    ).astype(bf16)
    b_grad[...] = dot(weights, c_proj[...], ((0,), (0,)))
    y_dots[0] = jnp.concatenate(head_sums(grad_gated * gated_in[...]), axis=0)


def inside_grads(grad, gated, silu, slope, mix, decay, x, b_proj, c_proj, entry, rows):
    inner, tokens = grad.shape
    channels = pl.BlockSpec((GROUP, tokens), lambda i: (i, 0))
    tokens_by = pl.BlockSpec((tokens, STATE), lambda i: (0, i))
    square = pl.BlockSpec((PER_GROUP, tokens, tokens), lambda i: (i, 0, 0))
    outs = [
        ((tokens, inner), bf16),
        ((inner, tokens), f32),
        (b_proj.shape, f32),
        (b_proj.shape, bf16),
        ((inner // GROUP, PER_GROUP, tokens), f32),
    ]
    return pl.pallas_call(
        inside_kernel,
        grid=(inner // GROUP,),
        in_specs=[channels] * 4
        + [square] * 2
        + [channels, tokens_by, tokens_by, pl.BlockSpec((GROUP, STATE), lambda i: (i, 0))]
        + [pl.BlockSpec((3, 1, PER_GROUP, tokens), lambda i: (0, i, 0, 0))],
        out_specs=[
            pl.BlockSpec((tokens, GROUP), lambda i: (0, i)),
            channels,
            tokens_by,
            tokens_by,
            pl.BlockSpec((1, PER_GROUP, tokens), lambda i: (i, 0, 0)),
        ],
        out_shape=[jax.ShapeDtypeStruct(*x) for x in outs],
        name="inside",
    )(grad, gated, silu, slope, mix, decay, x, b_proj, c_proj, entry, rows)


def owner_kernel(lead, came, back, values, local, later):
    blocks = came.shape[0]
    values[...] = came[:, 0:16, :].astype(f32)
    local[...] = came[:, 16:32, :].astype(f32)
    extra = came[:, 32:40, :].astype(f32)
    first, second = grid_of(blocks, blocks, 0), grid_of(blocks, blocks, 1)
    after = (second > first).astype(bf16)
    gaps = jnp.zeros((blocks, blocks), f32)
    for k in range(3):
        part = jnp.where(first < second, extra[:, k, :blocks], 0.0).astype(bf16)
        gaps = gaps + dot(after, part, ((1,), (0,)))
    weights = jnp.where(second > first, jnp.exp(gaps), 0.0)
    high = weights.astype(bf16)
    low = (weights - high.astype(f32)).astype(bf16)
    total = jnp.zeros((blocks, STATE), f32)
    for r in range(16):
        piece = values[:, r, :].astype(bf16)
        found = dot(high, piece, ((1,), (0,))) + dot(low, piece, ((1,), (0,)))
        later[:, r, :] = found
        total = total + found * local[:, r, :]
    total = jnp.broadcast_to(jnp.sum(total, axis=1, keepdims=True), (blocks, STATE))
    sums = extra[:, 3, :] + extra[:, 4, :] + extra[:, 5, :]
    own = jnp.where(lead[0] == 1, sums, 0.0) - total
    carried = exact_dot(after.astype(f32), own, ((1,), (0,)))
    back[:, 0:16, :] = later[...].astype(bf16)
    zero = jnp.zeros((blocks, 5, STATE), f32)
    back[:, 16:24, :] = jnp.concatenate(spread_parts(carried, blocks, 1) + [zero], axis=1).astype(
        bf16
    )


def owner_scan(lead, came):
    blocks = came.shape[0]
    scratch = pltpu.VMEM((blocks, 16, STATE), f32)
    return pl.pallas_call(
        owner_kernel,
        grid_spec=pltpu.PrefetchScalarGridSpec(
            num_scalar_prefetch=1,
            grid=(1,),
            in_specs=[whole_block(*came.shape)],
            out_specs=whole_block(blocks, 24, STATE),
            scratch_shapes=[scratch] * 3,
        ),
        out_shape=jax.ShapeDtypeStruct((blocks, 24, STATE), bf16),
        name="owner",
    )(lead, came)


def final_kernel(back, b_proj, x_in, tail_in, rows_in, x_inside, y_dots, b_inside, x_grad, b_grad, decay_grad):
    groups = x_in.shape[0] // GROUP
    pieces = GROUP // 16
    tokens = x_in.shape[1]
    heads = groups * PER_GROUP
    dots = []
    for g in range(groups):
        span = slice(g * GROUP, (g + 1) * GROUP)
        states = slice(g * STATE, (g + 1) * STATE)
        later = back[g * pieces : (g + 1) * pieces, 0:16, :].reshape(GROUP, STATE)
        carried = dot(later, b_proj[:, states], ((1,), (1,)))
        grad = x_inside[span, :] + carried * per_head(rows_in[1, g], 0)
        x_grad[:, span] = jnp.transpose(grad).astype(bf16)
        b_grad[:, states] = (
            b_inside[:, states] + dot(tail_in[span, :], later, ((0,), (0,)))
        ).astype(bf16)
        dots = dots + head_sums(x_in[span, :].astype(f32) * grad)
    own = jnp.concatenate([y_dots[g] for g in range(groups)], axis=0)
    own = own - jnp.concatenate(dots, axis=0)
    after = (grid_of(tokens, tokens, 0) >= grid_of(tokens, tokens, 1)).astype(f32)
    extra = jnp.sum(back[:, 16:24, :].astype(f32), axis=1)
    extra = jnp.sum(extra.reshape(heads, extra.shape[0] // heads, STATE), axis=1)
    decay_grad[...] = exact_dot(own, after, ((1,), (0,))) + extra


def final(back, b_proj, x, x_tail, rows, x_inside, y_dots, b_inside):
    inner, tokens = x.shape
    return whole_call(
        final_kernel,
        [
            ((tokens, inner), bf16),
            (b_proj.shape, bf16),
            ((inner // HEAD_DIM, tokens), f32),
        ],
        back, b_proj, x, x_tail, rows, x_inside, y_dots, b_inside,
    )


def body(
    mixer_output,
    layer_cotangent,
    expert_choice,
    route_weight,
    gate_pre,
    up_pre,
    w_gate,
    w_up,
    w_down,
    w_out,
    norm_gain,
    scan_in,
    gate_in,
    b_proj,
    c_proj,
    log_decay,
    entry_state,
):
    experts = lax.axis_size(SP)
    _, width = mixer_output.shape
    capacity = gate_pre.shape[1] // experts
    half = width // 2
    start = lax.axis_index("tp") * half

    side = lax.axis_index("tp")[None]
    send_grads, either = route(
        side, expert_choice.T, route_weight.T, layer_cotangent, experts * capacity
    )
    hidden_half = lax.dynamic_slice_in_dim(mixer_output, start, half, 1)
    cotangent_half = lax.dynamic_slice_in_dim(layer_cotangent, start, half, 1)
    send_hidden = dot(either, hidden_half, ((1,), (0,))).astype(bf16)
    send_grads = send_grads.reshape(experts, capacity, half)
    send_hidden = send_hidden.reshape(experts, capacity, half)
    inner = scan_in.shape[1]
    gain = norm_gain.astype(f32)[:, None]
    entry = entry_state.reshape(inner, STATE)
    mixed, *saved, x_tail, local, rows, inverse, carry, cotangent_rows = forward(
        scan_in, gate_in, b_proj, c_proj, log_decay.T, entry, gain, cotangent_half
    )
    gated, silu, slope, mix, decay, x = saved
    came_grads = lax.all_to_all(send_grads, SP, 0, 0, tiled=True)
    send_hidden, came_grads = lax.optimization_barrier((send_hidden, came_grads))
    came_hidden = lax.all_to_all(send_hidden, SP, 0, 0, tiled=True)
    grads_own = came_grads.reshape(-1, half)
    grads_far = swapped(grads_own)
    active, gate_grad, up_grad, rows_own, rows_far = expert_rows(
        side, grads_own, grads_far, gate_pre[0], up_pre[0], w_down[0], w_gate[0], w_up[0]
    )
    summed = (rows_own.astype(f32) + swapped(rows_far).astype(f32)).astype(bf16)
    summed, came_hidden = lax.optimization_barrier((summed, came_hidden))
    returned = lax.all_to_all(summed.reshape(experts, capacity, half), SP, 0, 0, tiled=True)
    hidden_own = came_hidden.reshape(-1, half)
    hidden_far = swapped(hidden_own)
    down_wgrad, gate_wgrad, up_wgrad = expert_weights(
        side, active, gate_grad, up_grad, grads_own, grads_far, hidden_own, hidden_far
    )
    moe_terms = dot(returned.reshape(-1, half), either, ((0,), (0,)))
    grad_own = (cotangent_rows.astype(f32) + moe_terms).astype(bf16)
    grad_far = swapped(grad_own)
    grad_hidden = jnp.where(
        side == 0,
        jnp.concatenate([grad_own, grad_far], axis=0),
        jnp.concatenate([grad_far, grad_own], axis=0),
    )

    message, grad_gated = state_message(
        side, grad_own, grad_far, w_out, gain, gated, silu, carry, c_proj, local, rows, inverse
    )
    came_states = lax.all_to_all(message, SP, 0, 0, tiled=True)
    lead = lax.rem(lax.axis_index(SP), HEAD_DIM // 16) == 0
    back = owner_scan(lead.astype(jnp.int32)[None], came_states)
    grad_gate_in, x_inside, b_inside, grad_c_proj, y_dots = inside_grads(
        grad_gated, gated, silu, slope, mix, decay, x, b_proj, c_proj, entry, rows
    )
    back = lax.all_to_all(back, SP, 0, 0, tiled=True)
    grad_scan_in, grad_b_proj, decay_grad = final(
        back, b_proj, x, x_tail, rows, x_inside, y_dots, b_inside
    )
    grad_log_decay = decay_grad.T

    line = lax.axis_size("sp_0")
    mixed, gate_wgrad = lax.optimization_barrier((mixed, gate_wgrad))
    mixed_line = from_line([mixed] * line, "sp_0")
    grads_line = from_line(pieces_for(grad_hidden, "sp_0", 0), "sp_0")
    product = dot(
        jnp.concatenate(grads_line, axis=1), jnp.concatenate(mixed_line, axis=1), ((1,), (1,))
    ).astype(bf16)
    parts = from_line(pieces_for(product, "sp_1", 0), "sp_1")
    product = sum(part.astype(f32) for part in parts).astype(bf16)
    parts = from_line(pieces_for(product, "sp_2", 0), "sp_2")
    grad_out_proj = sum(part.astype(f32) for part in parts)

    return (
        gate_wgrad[None],
        up_wgrad[None],
        down_wgrad[None],
        grad_out_proj,
        grad_scan_in,
        grad_gate_in,
        grad_b_proj,
        grad_c_proj,
        grad_log_decay,
    )


def solution(mesh):
    split = Mesh(mesh.devices.reshape(4, 4, 4, mesh.shape["tp"]), ("sp_0", "sp_1", "sp_2", "tp"))
    return jax.shard_map(
        body,
        mesh=split,
        in_specs=(
            P(SP, None),
            P(SP, None),
            P(SP, None),
            P(SP, None),
            P(SP, None, "tp"),
            P(SP, None, "tp"),
            P(SP, None, "tp"),
            P(SP, None, "tp"),
            P(SP, "tp", None),
            P("tp", None),
            P("tp"),
            P(SP, "tp"),
            P(SP, "tp"),
            P(SP, "tp"),
            P(SP, "tp"),
            P(SP, "tp"),
            P(SP, "tp", None, None),
        ),
        out_specs=(
            P(SP, None, "tp"),
            P(SP, None, "tp"),
            P(SP, "tp", None),
            P(SP, "tp"),
            P(SP, "tp"),
            P(SP, "tp"),
            P(SP, "tp"),
            P(SP, "tp"),
            P(SP, "tp"),
        ),
        check_vma=False,
    )
```

```python
import jax
import jax.numpy as jnp
from jax import lax
from jax.sharding import Mesh
from jax.experimental import pallas as pl
from jax.experimental.pallas import tpu as pltpu
from jax.sharding import PartitionSpec as P

HEAD_DIM = 64
STATE = 128
SP = ("sp_0", "sp_1", "sp_2")


rms_epsilon = 1e-05
clamp_limit = 7.0
swish_alpha = 1.702

bf16 = jnp.bfloat16
f32 = jnp.float32


def dot(a, b, dims):
    return lax.dot_general(a, b, (dims, ((), ())), preferred_element_type=f32)


def swapped(x):
    return lax.ppermute(x, "tp", [(0, 1), (1, 0)])


def from_line(parts, axis):
    size = lax.axis_size(axis)
    return [parts[0]] + [
        lax.ppermute(parts[k], axis, [(i, (i + k) % size) for i in range(size)])
        for k in range(1, size)
    ]


def pieces_for(x, axis, dim):
    size, spot = lax.axis_size(axis), lax.axis_index(axis)
    span = x.shape[dim] // size
    return [
        lax.dynamic_slice_in_dim(x, lax.rem(spot + k, size) * span, span, dim) for k in range(size)
    ]


def expert_rows_kernel(
    side, mine, other, gate_value, up_value, down_own, down_far, gate_own, gate_far, up_own, up_far,
    active, gate_grad, up_grad, rows_own, rows_far,
):
    act_grad = dot(mine[...], down_own[...], ((1,), (1,)))
    act_grad = act_grad + dot(other[...], down_far[...], ((1,), (1,)))
    gate_full = gate_value[...].astype(f32)
    up_full = up_value[...].astype(f32)
    gate_clip = jnp.minimum(gate_full, clamp_limit)
    up_clip = jnp.clip(up_full, -clamp_limit, clamp_limit)
    sigmoid_gate = jax.nn.sigmoid(swish_alpha * gate_clip)
    swish_gate = gate_clip * sigmoid_gate
    active[...] = ((up_clip + 1.0) * swish_gate).astype(bf16)
    inside = (up_full > -clamp_limit) & (up_full < clamp_limit)
    up_side = jnp.where(inside, act_grad * swish_gate, 0.0).astype(bf16)
    slope = sigmoid_gate + swish_alpha * gate_clip * sigmoid_gate * (1.0 - sigmoid_gate)
    gate_side = jnp.where(
        gate_full < clamp_limit, act_grad * (up_clip + 1.0) * slope, 0.0
    ).astype(bf16)
    up_grad[...] = up_side
    gate_grad[...] = gate_side
    far = dot(gate_side, gate_far[...], ((1,), (1,))) + dot(up_side, up_far[...], ((1,), (1,)))
    rows_far[...] = far.astype(bf16)
    own = dot(gate_side, gate_own[...], ((1,), (1,))) + dot(up_side, up_own[...], ((1,), (1,)))
    rows_own[...] = own.astype(bf16)


def whole_block(*shape):
    return pl.BlockSpec(shape, lambda i, side: (0,) * len(shape))


def expert_rows(side, mine, other, gate_value, up_value, w_down, w_gate, w_up):
    rows, half = mine.shape
    hidden = gate_value.shape[1]
    row_block = whole_block(rows, half)
    act_block = whole_block(rows, hidden)
    down = [
        pl.BlockSpec((hidden, half), lambda i, side: (0, side[0])),
        pl.BlockSpec((hidden, half), lambda i, side: (0, 1 - side[0])),
    ]
    tall = [
        pl.BlockSpec((half, hidden), lambda i, side: (side[0], 0)),
        pl.BlockSpec((half, hidden), lambda i, side: (1 - side[0], 0)),
    ]
    act = jax.ShapeDtypeStruct((rows, hidden), bf16)
    out = jax.ShapeDtypeStruct((rows, half), bf16)
    return pl.pallas_call(
        expert_rows_kernel,
        grid_spec=pltpu.PrefetchScalarGridSpec(
            num_scalar_prefetch=1,
            grid=(1,),
            in_specs=[row_block, row_block, act_block, act_block] + down + tall + tall,
            out_specs=[act_block] * 3 + [row_block] * 2,
        ),
        out_shape=[act] * 3 + [out] * 2,
        name="expert_rows",
        compiler_params=pltpu.CompilerParams(vmem_limit_bytes=24 << 20),
    )(side, mine, other, gate_value, up_value, w_down, w_down, w_gate, w_gate, w_up, w_up)


def weights_kernel(
    side, active, gate_grad, up_grad, grads_own, grads_far, hidden_own, hidden_far,
    down_out, gate_out, up_out,
):
    def write(grads, hidden):
        down_out[...] = dot(active[...], grads, ((0,), (0,))).astype(bf16)
        gate_out[...] = dot(hidden, gate_grad[...], ((0,), (0,))).astype(bf16)
        up_out[...] = dot(hidden, up_grad[...], ((0,), (0,))).astype(bf16)

    @pl.when(pl.program_id(0) < 2)
    def _():
        write(grads_own[...], hidden_own[...])

    @pl.when(pl.program_id(0) >= 2)
    def _():
        write(grads_far[...], hidden_far[...])


def expert_weights(side, active, gate_grad, up_grad, grads_own, grads_far, hidden_own, hidden_far):
    rows, half = grads_own.shape
    hidden = active.shape[1]
    own = pl.BlockSpec((rows, half // 2), lambda i, side: (0, jnp.minimum(i, 1)))
    far = pl.BlockSpec((rows, half // 2), lambda i, side: (0, jnp.maximum(i - 2, 0)))

    def place(i, side):
        return lax.rem(i + 2 * side[0], 4)

    tall = pl.BlockSpec((half // 2, hidden), lambda i, side: (place(i, side), 0))
    return pl.pallas_call(
        weights_kernel,
        grid_spec=pltpu.PrefetchScalarGridSpec(
            num_scalar_prefetch=1,
            grid=(4,),
            in_specs=[whole_block(rows, hidden)] * 3 + [own, far, own, far],
            out_specs=[
                pl.BlockSpec((hidden, half // 2), lambda i, side: (0, place(i, side))),
                tall,
                tall,
            ],
        ),
        out_shape=[jax.ShapeDtypeStruct((hidden, 2 * half), bf16)]
        + [jax.ShapeDtypeStruct((2 * half, hidden), bf16)] * 2,
        name="weights",
        compiler_params=pltpu.CompilerParams(vmem_limit_bytes=20 << 20),
    )(side, active, gate_grad, up_grad, grads_own, grads_far, hidden_own, hidden_far)


def exact_dot(a, b, dims):
    return lax.dot_general(
        a, b, (dims, ((), ())), preferred_element_type=f32, precision=lax.Precision.HIGHEST
    )


def grid_of(rows, columns, axis):
    return lax.broadcasted_iota(jnp.int32, (rows, columns), axis)


def route_kernel(side, choice, weight, cotangent, grads, places):
    tokens = choice.shape[1]
    slots = places.shape[0]
    experts = slots // 8
    expert_at = grid_of(experts, tokens, 0)
    hot = [(expert_at == choice[k : k + 1, :]).astype(f32) for k in range(2)]
    before = (grid_of(tokens, tokens, 0) < grid_of(tokens, tokens, 1)).astype(bf16)
    earlier = dot((hot[0] + hot[1]).astype(bf16), before, ((1,), (0,)))
    same = (grid_of(tokens, tokens, 0) == grid_of(tokens, tokens, 1)).astype(f32)
    weights = exact_dot(same, weight[...], ((1,), (1,)))
    cotangents = cotangent[...].astype(f32)
    slot_at = grid_of(slots, tokens, 0)
    either = jnp.zeros((slots, tokens), f32)
    sent = jnp.zeros((slots, cotangent.shape[1]), f32)
    for k in range(2):
        rank = jnp.sum(earlier * hot[k], axis=0, keepdims=True).astype(jnp.int32)
        taken = (slot_at == choice[k : k + 1, :] * 8 + rank).astype(f32)
        either = either + taken
        rows = (weights[:, k : k + 1] * cotangents).astype(bf16)
        sent = sent + dot(taken.astype(bf16), rows, ((1,), (0,)))
    grads[...] = sent.astype(bf16)
    places[...] = either.astype(bf16)


def route(side, choice, weight, cotangent, slots):
    tokens, width = cotangent.shape
    half = width // 2
    return pl.pallas_call(
        route_kernel,
        grid_spec=pltpu.PrefetchScalarGridSpec(
            num_scalar_prefetch=1,
            grid=(1,),
            in_specs=[
                whole_block(*choice.shape),
                whole_block(*weight.shape),
                pl.BlockSpec((tokens, half), lambda i, side: (0, side[0])),
            ],
            out_specs=[whole_block(slots, half), whole_block(slots, tokens)],
        ),
        out_shape=[
            jax.ShapeDtypeStruct((slots, half), bf16),
            jax.ShapeDtypeStruct((slots, tokens), bf16),
        ],
        name="route",
        compiler_params=pltpu.CompilerParams(vmem_limit_bytes=10 << 20),
    )(side, choice, weight, cotangent)


GROUP = 256
PER_GROUP = GROUP // HEAD_DIM


def per_head(rows, first):
    return jnp.concatenate(
        [
            jnp.broadcast_to(rows[first + r : first + r + 1, :], (HEAD_DIM, rows.shape[1]))
            for r in range(PER_GROUP)
        ],
        axis=0,
    )


def head_sums(x):
    return [
        jnp.sum(x[r * HEAD_DIM : (r + 1) * HEAD_DIM, :], axis=0, keepdims=True)
        for r in range(PER_GROUP)
    ]


def forward_kernel(
    scan_in, gate_in, b_proj, c_proj, log_decay, entry, gain, cotangent,
    mixed, gated_out, silu_out, slope_out, mix_out, decay_out, x_out, tail_out, local_out,
    rows_out, inverse_out, carry_out, cotangent_out,
):
    tokens = scan_in.shape[0]
    groups = scan_in.shape[1] // GROUP
    down, across = grid_of(tokens, tokens, 0), grid_of(tokens, tokens, 1)
    decays = log_decay[...]
    cum_rows = exact_dot(decays, (down <= across).astype(f32), ((1,), (0,)))
    cum_columns = exact_dot((across <= down).astype(f32), decays, ((1,), (1,)))
    total = cum_rows[:, tokens - 1 :]
    growth = jnp.exp(cum_rows)
    tail = jnp.exp(total - cum_rows)
    totals = jnp.broadcast_to(total, growth.shape)
    causal = down >= across
    for g in range(groups):
        span = slice(g * GROUP, (g + 1) * GROUP)
        states = slice(g * STATE, (g + 1) * STATE)
        first = g * PER_GROUP
        b_group, c_group = b_proj[:, states], c_proj[:, states]
        inner = dot(c_group, b_group, ((1,), (1,)))
        x = jnp.transpose(scan_in[:, span].astype(f32))
        x_b = x.astype(bf16)
        carried = dot(entry[span, :].astype(bf16), c_group, ((1,), (1,)))
        within = []
        for r in range(PER_GROUP):
            h = first + r
            gaps = cum_columns[:, h : h + 1] - cum_rows[h : h + 1, :]
            decay = jnp.where(causal, jnp.exp(jnp.where(causal, gaps, 0.0)), 0.0)
            decay_out[h] = decay
            mix = (inner * decay).astype(bf16)
            mix_out[h] = mix
            within.append(dot(x_b[r * HEAD_DIM : (r + 1) * HEAD_DIM, :], mix, ((1,), (1,))))
        carried = carried * per_head(growth, first)
        scan_out = jnp.concatenate(within, axis=0) + carried
        gate = jnp.transpose(gate_in[:, span].astype(f32))
        sig = jax.nn.sigmoid(gate)
        silu = gate * sig
        gated = scan_out * silu
        inverse = lax.rsqrt(jnp.mean(gated * gated, axis=0, keepdims=True) + rms_epsilon)
        mixed[span, :] = (gated * inverse * gain[span, :]).astype(bf16)
        gated_out[span, :] = gated
        silu_out[span, :] = silu
        slope_out[span, :] = scan_out * sig * (1.0 + gate * (1.0 - sig))
        carry_out[span, :] = carried * silu
        cotangent_out[span, :] = jnp.transpose(cotangent[:, span].astype(f32)).astype(bf16)
        inverse_out[g] = inverse
        for k, part in enumerate((growth, tail, totals)):
            rows_out[k, g] = part[first : first + PER_GROUP, :]
        x_out[span, :] = x_b
        x_tail = (x * per_head(tail, first)).astype(bf16)
        tail_out[span, :] = x_tail
        local_out[span, :] = dot(x_tail, b_group, ((1,), (0,))).astype(bf16)


def whole_call(kernel, limit, out_shape, *args):
    return pl.pallas_call(
        kernel,
        out_shape=[jax.ShapeDtypeStruct(*x) for x in out_shape],
        compiler_params=pltpu.CompilerParams(vmem_limit_bytes=limit << 20),
    )(*args)


def forward(scan_in, gate_in, b_proj, c_proj, log_decay, entry, gain, cotangent):
    tokens, inner = scan_in.shape
    heads = log_decay.shape[0]
    return whole_call(
        forward_kernel,
        12,
        [
            ((inner, tokens), bf16),
            ((inner, tokens), f32),
            ((inner, tokens), f32),
            ((inner, tokens), f32),
            ((heads, tokens, tokens), bf16),
            ((heads, tokens, tokens), f32),
            ((inner, tokens), bf16),
            ((inner, tokens), bf16),
            ((inner, STATE), bf16),
            ((3, inner // GROUP, PER_GROUP, tokens), f32),
            ((inner // GROUP, 1, tokens), f32),
            ((inner, tokens), f32),
            ((cotangent.shape[1], tokens), bf16),
        ],
        scan_in, gate_in, b_proj, c_proj, log_decay, entry, gain, cotangent,
    )


def spread_parts(x, heads, pieces):
    high = x.astype(bf16)
    rest = x - high.astype(f32)
    middle = rest.astype(bf16)
    low = (rest - middle.astype(f32)).astype(bf16)
    return [
        jnp.broadcast_to(part.astype(f32)[:, None, :], (heads, pieces, STATE)).reshape(
            heads * pieces, 1, STATE
        )
        for part in (high, middle, low)
    ]


def message_kernel(
    side, grad_own, grad_far, out_own, out_far, gain, gated_in, silu_in, carry_in, c_proj, local_in,
    rows_in, inverse_in,
    message, grad_out,
):
    pieces = GROUP // 16
    grad_mixed = dot(out_own[...], grad_own[...], ((1,), (0,)))
    grad_mixed = grad_mixed + dot(out_far[...], grad_far[...], ((1,), (0,)))
    inverse = inverse_in[0]
    unit = gated_in[...] * inverse
    grad_unit = grad_mixed * gain[...]
    mean = jnp.mean(grad_unit * unit, axis=0, keepdims=True)
    grad_gated = inverse * (grad_unit - unit * mean)
    grad_out[...] = grad_gated
    grown = (grad_gated * silu_in[...] * per_head(rows_in[0, 0], 0)).astype(bf16)
    block_state = dot(grown, c_proj[...], ((1,), (0,))).astype(bf16)
    message[:, 0:16, :] = block_state.reshape(pieces, 16, STATE)
    message[:, 16:32, :] = local_in[...].reshape(pieces, 16, STATE)
    own = jnp.concatenate(head_sums(grad_gated * carry_in[...]), axis=0)
    own = jnp.broadcast_to(jnp.sum(own, axis=1, keepdims=True), (PER_GROUP, STATE))
    per = pieces // PER_GROUP
    zero = jnp.zeros((pieces, 2, STATE), f32)
    extra = jnp.concatenate(
        spread_parts(rows_in[2, 0], PER_GROUP, per) + spread_parts(own, PER_GROUP, per) + [zero],
        axis=1,
    )
    message[:, 32:40, :] = extra.astype(bf16)


def state_message(side, grad_own, grad_far, w_out, gain, gated, silu, carry, c_proj, local, rows, inverse):
    half, tokens = grad_own.shape
    inner = gain.shape[0]
    pieces = GROUP // 16
    channels = pl.BlockSpec((GROUP, tokens), lambda i, side: (i, 0))
    return pl.pallas_call(
        message_kernel,
        grid_spec=pltpu.PrefetchScalarGridSpec(
            num_scalar_prefetch=1,
            grid=(inner // GROUP,),
            in_specs=[
                whole_block(half, tokens),
                whole_block(half, tokens),
                pl.BlockSpec((GROUP, half), lambda i, side: (i, side[0])),
                pl.BlockSpec((GROUP, half), lambda i, side: (i, 1 - side[0])),
                pl.BlockSpec((GROUP, 1), lambda i, side: (i, 0)),
                channels,
                channels,
                channels,
                pl.BlockSpec((tokens, STATE), lambda i, side: (0, i)),
                pl.BlockSpec((GROUP, STATE), lambda i, side: (i, 0)),
                pl.BlockSpec((3, 1, PER_GROUP, tokens), lambda i, side: (0, i, 0, 0)),
                pl.BlockSpec((1, 1, tokens), lambda i, side: (i, 0, 0)),
            ],
            out_specs=[
                pl.BlockSpec((pieces, 40, STATE), lambda i, side: (i, 0, 0)),
                channels,
            ],
        ),
        out_shape=[
            jax.ShapeDtypeStruct((inner // 16, 40, STATE), bf16),
            jax.ShapeDtypeStruct((inner, tokens), f32),
        ],
        name="message",
        compiler_params=pltpu.CompilerParams(vmem_limit_bytes=8 << 20),
    )(side, grad_own, grad_far, w_out, w_out, gain, gated, silu, carry, c_proj, local, rows, inverse)


def inside_kernel(
    grad_in, gated_in, silu_in, slope_in, mix_in, decay_in, x_in, b_proj, c_proj, entry, rows_in,
    gate_grad, x_grad, b_grad, c_grad, y_dots,
):
    tokens = x_in.shape[1]
    grad_gated = grad_in[...]
    gate_grad[...] = jnp.transpose(grad_gated * slope_in[...]).astype(bf16)
    grad_y = grad_gated * silu_in[...]
    grad_y_b = grad_y.astype(bf16)
    grown = (grad_y * per_head(rows_in[0, 0], 0)).astype(bf16)
    x = x_in[...]
    weights = jnp.zeros((tokens, tokens), f32)
    inside = []
    for r in range(PER_GROUP):
        head = slice(r * HEAD_DIM, (r + 1) * HEAD_DIM)
        inside.append(dot(grad_y_b[head, :], mix_in[r], ((1,), (0,))))
        weights = weights + decay_in[r] * dot(grad_y_b[head, :], x[head, :], ((0,), (0,)))
    x_grad[...] = jnp.concatenate(inside, axis=0)
    weights = weights.astype(bf16)
    c_grad[...] = (
        dot(weights, b_proj[...], ((1,), (0,)))
        + dot(grown, entry[...].astype(bf16), ((0,), (0,)))
    ).astype(bf16)
    b_grad[...] = dot(weights, c_proj[...], ((0,), (0,)))
    y_dots[0] = jnp.concatenate(head_sums(grad_gated * gated_in[...]), axis=0)


def inside_grads(grad, gated, silu, slope, mix, decay, x, b_proj, c_proj, entry, rows):
    inner, tokens = grad.shape
    channels = pl.BlockSpec((GROUP, tokens), lambda i: (i, 0))
    tokens_by = pl.BlockSpec((tokens, STATE), lambda i: (0, i))
    square = pl.BlockSpec((PER_GROUP, tokens, tokens), lambda i: (i, 0, 0))
    outs = [
        ((tokens, inner), bf16),
        ((inner, tokens), f32),
        (b_proj.shape, f32),
        (b_proj.shape, bf16),
        ((inner // GROUP, PER_GROUP, tokens), f32),
    ]
    return pl.pallas_call(
        inside_kernel,
        grid=(inner // GROUP,),
        in_specs=[channels] * 4
        + [square] * 2
        + [channels, tokens_by, tokens_by, pl.BlockSpec((GROUP, STATE), lambda i: (i, 0))]
        + [pl.BlockSpec((3, 1, PER_GROUP, tokens), lambda i: (0, i, 0, 0))],
        out_specs=[
            pl.BlockSpec((tokens, GROUP), lambda i: (0, i)),
            channels,
            tokens_by,
            tokens_by,
            pl.BlockSpec((1, PER_GROUP, tokens), lambda i: (i, 0, 0)),
        ],
        out_shape=[jax.ShapeDtypeStruct(*x) for x in outs],
        name="inside",
        compiler_params=pltpu.CompilerParams(vmem_limit_bytes=8 << 20),
    )(grad, gated, silu, slope, mix, decay, x, b_proj, c_proj, entry, rows)


def owner_kernel(lead, came, back, values, local, later):
    blocks = came.shape[0]
    values[...] = came[:, 0:16, :].astype(f32)
    local[...] = came[:, 16:32, :].astype(f32)
    extra = came[:, 32:40, :].astype(f32)
    first, second = grid_of(blocks, blocks, 0), grid_of(blocks, blocks, 1)
    after = (second > first).astype(bf16)
    gaps = jnp.zeros((blocks, blocks), f32)
    for k in range(3):
        part = jnp.where(first < second, extra[:, k, :blocks], 0.0).astype(bf16)
        gaps = gaps + dot(after, part, ((1,), (0,)))
    weights = jnp.where(second > first, jnp.exp(gaps), 0.0)
    high = weights.astype(bf16)
    low = (weights - high.astype(f32)).astype(bf16)
    total = jnp.zeros((blocks, STATE), f32)
    for r in range(16):
        piece = values[:, r, :].astype(bf16)
        found = dot(high, piece, ((1,), (0,))) + dot(low, piece, ((1,), (0,)))
        later[:, r, :] = found
        total = total + found * local[:, r, :]
    total = jnp.broadcast_to(jnp.sum(total, axis=1, keepdims=True), (blocks, STATE))
    sums = extra[:, 3, :] + extra[:, 4, :] + extra[:, 5, :]
    own = jnp.where(lead[0] == 1, sums, 0.0) - total
    carried = exact_dot(after.astype(f32), own, ((1,), (0,)))
    back[:, 0:16, :] = later[...].astype(bf16)
    zero = jnp.zeros((blocks, 5, STATE), f32)
    back[:, 16:24, :] = jnp.concatenate(spread_parts(carried, blocks, 1) + [zero], axis=1).astype(
        bf16
    )


def owner_scan(lead, came):
    blocks = came.shape[0]
    scratch = pltpu.VMEM((blocks, 16, STATE), f32)
    return pl.pallas_call(
        owner_kernel,
        grid_spec=pltpu.PrefetchScalarGridSpec(
            num_scalar_prefetch=1,
            grid=(1,),
            in_specs=[whole_block(*came.shape)],
            out_specs=whole_block(blocks, 24, STATE),
            scratch_shapes=[scratch] * 3,
        ),
        out_shape=jax.ShapeDtypeStruct((blocks, 24, STATE), bf16),
        name="owner",
        compiler_params=pltpu.CompilerParams(vmem_limit_bytes=6 << 20),
    )(lead, came)


def final_kernel(back, b_proj, x_in, tail_in, rows_in, x_inside, y_dots, b_inside, x_grad, b_grad, decay_grad):
    groups = x_in.shape[0] // GROUP
    pieces = GROUP // 16
    tokens = x_in.shape[1]
    heads = groups * PER_GROUP
    dots = []
    for g in range(groups):
        span = slice(g * GROUP, (g + 1) * GROUP)
        states = slice(g * STATE, (g + 1) * STATE)
        later = back[g * pieces : (g + 1) * pieces, 0:16, :].reshape(GROUP, STATE)
        carried = dot(later, b_proj[:, states], ((1,), (1,)))
        grad = x_inside[span, :] + carried * per_head(rows_in[1, g], 0)
        x_grad[:, span] = jnp.transpose(grad).astype(bf16)
        b_grad[:, states] = (
            b_inside[:, states] + dot(tail_in[span, :], later, ((0,), (0,)))
        ).astype(bf16)
        dots = dots + head_sums(x_in[span, :].astype(f32) * grad)
    own = jnp.concatenate([y_dots[g] for g in range(groups)], axis=0)
    own = own - jnp.concatenate(dots, axis=0)
    after = (grid_of(tokens, tokens, 0) >= grid_of(tokens, tokens, 1)).astype(f32)
    extra = jnp.sum(back[:, 16:24, :].astype(f32), axis=1)
    extra = jnp.sum(extra.reshape(heads, extra.shape[0] // heads, STATE), axis=1)
    decay_grad[...] = exact_dot(own, after, ((1,), (0,))) + extra


def final(back, b_proj, x, x_tail, rows, x_inside, y_dots, b_inside):
    inner, tokens = x.shape
    return whole_call(
        final_kernel,
        6,
        [
            ((tokens, inner), bf16),
            (b_proj.shape, bf16),
            ((inner // HEAD_DIM, tokens), f32),
        ],
        back, b_proj, x, x_tail, rows, x_inside, y_dots, b_inside,
    )


def body(
    mixer_output,
    layer_cotangent,
    expert_choice,
    route_weight,
    gate_pre,
    up_pre,
    w_gate,
    w_up,
    w_down,
    w_out,
    norm_gain,
    scan_in,
    gate_in,
    b_proj,
    c_proj,
    log_decay,
    entry_state,
):
    experts = lax.axis_size(SP)
    _, width = mixer_output.shape
    capacity = gate_pre.shape[1] // experts
    half = width // 2
    start = lax.axis_index("tp") * half

    side = lax.axis_index("tp")[None]
    send_grads, either = route(
        side, expert_choice.T, route_weight.T, layer_cotangent, experts * capacity
    )
    hidden_half = lax.dynamic_slice_in_dim(mixer_output, start, half, 1)
    cotangent_half = lax.dynamic_slice_in_dim(layer_cotangent, start, half, 1)
    send_hidden = dot(either, hidden_half, ((1,), (0,))).astype(bf16)
    send_grads = send_grads.reshape(experts, capacity, half)
    send_hidden = send_hidden.reshape(experts, capacity, half)
    inner = scan_in.shape[1]
    gain = norm_gain.astype(f32)[:, None]
    entry = entry_state.reshape(inner, STATE)
    mixed, *saved, x_tail, local, rows, inverse, carry, cotangent_rows = forward(
        scan_in, gate_in, b_proj, c_proj, log_decay.T, entry, gain, cotangent_half
    )
    gated, silu, slope, mix, decay, x = saved
    came_grads = lax.all_to_all(send_grads, SP, 0, 0, tiled=True)
    send_hidden, came_grads = lax.optimization_barrier((send_hidden, came_grads))
    came_hidden = lax.all_to_all(send_hidden, SP, 0, 0, tiled=True)
    grads_own = came_grads.reshape(-1, half)
    grads_far = swapped(grads_own)
    active, gate_grad, up_grad, rows_own, rows_far = expert_rows(
        side, grads_own, grads_far, gate_pre[0], up_pre[0], w_down[0], w_gate[0], w_up[0]
    )
    summed = (rows_own.astype(f32) + swapped(rows_far).astype(f32)).astype(bf16)
    summed, came_hidden = lax.optimization_barrier((summed, came_hidden))
    returned = lax.all_to_all(summed.reshape(experts, capacity, half), SP, 0, 0, tiled=True)
    hidden_own = came_hidden.reshape(-1, half)
    hidden_far = swapped(hidden_own)
    down_wgrad, gate_wgrad, up_wgrad = expert_weights(
        side, active, gate_grad, up_grad, grads_own, grads_far, hidden_own, hidden_far
    )
    moe_terms = dot(returned.reshape(-1, half), either, ((0,), (0,)))
    grad_own = (cotangent_rows.astype(f32) + moe_terms).astype(bf16)
    grad_far = swapped(grad_own)
    grad_hidden = jnp.where(
        side == 0,
        jnp.concatenate([grad_own, grad_far], axis=0),
        jnp.concatenate([grad_far, grad_own], axis=0),
    )

    message, grad_gated = state_message(
        side, grad_own, grad_far, w_out, gain, gated, silu, carry, c_proj, local, rows, inverse
    )
    came_states = lax.all_to_all(message, SP, 0, 0, tiled=True)
    lead = lax.rem(lax.axis_index(SP), HEAD_DIM // 16) == 0
    back = owner_scan(lead.astype(jnp.int32)[None], came_states)
    grad_gate_in, x_inside, b_inside, grad_c_proj, y_dots = inside_grads(
        grad_gated, gated, silu, slope, mix, decay, x, b_proj, c_proj, entry, rows
    )
    back = lax.all_to_all(back, SP, 0, 0, tiled=True)
    grad_scan_in, grad_b_proj, decay_grad = final(
        back, b_proj, x, x_tail, rows, x_inside, y_dots, b_inside
    )
    grad_log_decay = decay_grad.T

    line = lax.axis_size("sp_0")
    mixed, gate_wgrad = lax.optimization_barrier((mixed, gate_wgrad))
    mixed_line = from_line([mixed] * line, "sp_0")
    grads_line = from_line(pieces_for(grad_hidden, "sp_0", 0), "sp_0")
    product = dot(
        jnp.concatenate(grads_line, axis=1), jnp.concatenate(mixed_line, axis=1), ((1,), (1,))
    ).astype(bf16)
    parts = from_line(pieces_for(product, "sp_1", 0), "sp_1")
    product = sum(part.astype(f32) for part in parts).astype(bf16)
    parts = from_line(pieces_for(product, "sp_2", 0), "sp_2")
    grad_out_proj = sum(part.astype(f32) for part in parts)

    return (
        gate_wgrad[None],
        up_wgrad[None],
        down_wgrad[None],
        grad_out_proj,
        grad_scan_in,
        grad_gate_in,
        grad_b_proj,
        grad_c_proj,
        grad_log_decay,
    )


def solution(mesh):
    split = Mesh(mesh.devices.reshape(4, 4, 4, mesh.shape["tp"]), ("sp_0", "sp_1", "sp_2", "tp"))
    return jax.shard_map(
        body,
        mesh=split,
        in_specs=(
            P(SP, None),
            P(SP, None),
            P(SP, None),
            P(SP, None),
            P(SP, None, "tp"),
            P(SP, None, "tp"),
            P(SP, None, "tp"),
            P(SP, None, "tp"),
            P(SP, "tp", None),
            P("tp", None),
            P("tp"),
            P(SP, "tp"),
            P(SP, "tp"),
            P(SP, "tp"),
            P(SP, "tp"),
            P(SP, "tp"),
            P(SP, "tp", None, None),
        ),
        out_specs=(
            P(SP, None, "tp"),
            P(SP, None, "tp"),
            P(SP, "tp", None),
            P(SP, "tp"),
            P(SP, "tp"),
            P(SP, "tp"),
            P(SP, "tp"),
            P(SP, "tp"),
            P(SP, "tp"),
        ),
        check_vma=False,
    )
```

```python
import jax
import jax.numpy as jnp
from jax import lax
from jax.sharding import Mesh
from jax.experimental import pallas as pl
from jax.experimental.pallas import tpu as pltpu
from jax.sharding import PartitionSpec as P

HEAD_DIM = 64
STATE = 128
SP = ("sp_0", "sp_1", "sp_2")


rms_epsilon = 1e-05
clamp_limit = 7.0
swish_alpha = 1.702

bf16 = jnp.bfloat16
f32 = jnp.float32


def dot(a, b, dims):
    return lax.dot_general(a, b, (dims, ((), ())), preferred_element_type=f32)


def swapped(x):
    return lax.ppermute(x, "tp", [(0, 1), (1, 0)])


def from_line(parts, axis):
    size = lax.axis_size(axis)
    return [parts[0]] + [
        lax.ppermute(parts[k], axis, [(i, (i + k) % size) for i in range(size)])
        for k in range(1, size)
    ]


def pieces_for(x, axis, dim):
    size, spot = lax.axis_size(axis), lax.axis_index(axis)
    span = x.shape[dim] // size
    return [
        lax.dynamic_slice_in_dim(x, lax.rem(spot + k, size) * span, span, dim) for k in range(size)
    ]


def expert_rows_kernel(
    side, mine, other, gate_value, up_value, down_own, down_far, gate_own, gate_far, up_own, up_far,
    active, gate_grad, up_grad, rows_own, rows_far,
):
    act_grad = dot(mine[...], down_own[...], ((1,), (1,)))
    act_grad = act_grad + dot(other[...], down_far[...], ((1,), (1,)))
    gate_full = gate_value[...].astype(f32)
    up_full = up_value[...].astype(f32)
    gate_clip = jnp.minimum(gate_full, clamp_limit)
    up_clip = jnp.clip(up_full, -clamp_limit, clamp_limit)
    sigmoid_gate = jax.nn.sigmoid(swish_alpha * gate_clip)
    swish_gate = gate_clip * sigmoid_gate
    active[...] = ((up_clip + 1.0) * swish_gate).astype(bf16)
    inside = (up_full > -clamp_limit) & (up_full < clamp_limit)
    up_side = jnp.where(inside, act_grad * swish_gate, 0.0).astype(bf16)
    slope = sigmoid_gate + swish_alpha * gate_clip * sigmoid_gate * (1.0 - sigmoid_gate)
    gate_side = jnp.where(
        gate_full < clamp_limit, act_grad * (up_clip + 1.0) * slope, 0.0
    ).astype(bf16)
    up_grad[...] = up_side
    gate_grad[...] = gate_side
    far = dot(gate_side, gate_far[...], ((1,), (1,))) + dot(up_side, up_far[...], ((1,), (1,)))
    rows_far[...] = far.astype(bf16)
    own = dot(gate_side, gate_own[...], ((1,), (1,))) + dot(up_side, up_own[...], ((1,), (1,)))
    rows_own[...] = own.astype(bf16)


def whole_block(*shape):
    return pl.BlockSpec(shape, lambda i, side: (0,) * len(shape))


def expert_rows(side, mine, other, gate_value, up_value, w_down, w_gate, w_up):
    rows, half = mine.shape
    hidden = gate_value.shape[1]
    row_block = whole_block(rows, half)
    act_block = whole_block(rows, hidden)
    down = [
        pl.BlockSpec((hidden, half), lambda i, side: (0, side[0])),
        pl.BlockSpec((hidden, half), lambda i, side: (0, 1 - side[0])),
    ]
    tall = [
        pl.BlockSpec((half, hidden), lambda i, side: (side[0], 0)),
        pl.BlockSpec((half, hidden), lambda i, side: (1 - side[0], 0)),
    ]
    act = jax.ShapeDtypeStruct((rows, hidden), bf16)
    out = jax.ShapeDtypeStruct((rows, half), bf16)
    return pl.pallas_call(
        expert_rows_kernel,
        grid_spec=pltpu.PrefetchScalarGridSpec(
            num_scalar_prefetch=1,
            grid=(1,),
            in_specs=[row_block, row_block, act_block, act_block] + down + tall + tall,
            out_specs=[act_block] * 3 + [row_block] * 2,
        ),
        out_shape=[act] * 3 + [out] * 2,
        name="expert_rows",
    )(side, mine, other, gate_value, up_value, w_down, w_down, w_gate, w_gate, w_up, w_up)


def weights_kernel(
    side, active, gate_grad, up_grad, grads_own, grads_far, hidden_own, hidden_far,
    down_out, gate_out, up_out,
):
    def write(grads, hidden):
        down_out[...] = dot(active[...], grads, ((0,), (0,))).astype(bf16)
        gate_out[...] = dot(hidden, gate_grad[...], ((0,), (0,))).astype(bf16)
        up_out[...] = dot(hidden, up_grad[...], ((0,), (0,))).astype(bf16)

    @pl.when(pl.program_id(0) < 2)
    def _():
        write(grads_own[...], hidden_own[...])

    @pl.when(pl.program_id(0) >= 2)
    def _():
        write(grads_far[...], hidden_far[...])


def expert_weights(side, active, gate_grad, up_grad, grads_own, grads_far, hidden_own, hidden_far):
    rows, half = grads_own.shape
    hidden = active.shape[1]
    own = pl.BlockSpec((rows, half // 2), lambda i, side: (0, jnp.minimum(i, 1)))
    far = pl.BlockSpec((rows, half // 2), lambda i, side: (0, jnp.maximum(i - 2, 0)))

    def place(i, side):
        return lax.rem(i + 2 * side[0], 4)

    tall = pl.BlockSpec((half // 2, hidden), lambda i, side: (place(i, side), 0))
    return pl.pallas_call(
        weights_kernel,
        grid_spec=pltpu.PrefetchScalarGridSpec(
            num_scalar_prefetch=1,
            grid=(4,),
            in_specs=[whole_block(rows, hidden)] * 3 + [own, far, own, far],
            out_specs=[
                pl.BlockSpec((hidden, half // 2), lambda i, side: (0, place(i, side))),
                tall,
                tall,
            ],
        ),
        out_shape=[jax.ShapeDtypeStruct((hidden, 2 * half), bf16)]
        + [jax.ShapeDtypeStruct((2 * half, hidden), bf16)] * 2,
        name="weights",
    )(side, active, gate_grad, up_grad, grads_own, grads_far, hidden_own, hidden_far)


def exact_dot(a, b, dims):
    return lax.dot_general(
        a, b, (dims, ((), ())), preferred_element_type=f32, precision=lax.Precision.HIGHEST
    )


def grid_of(rows, columns, axis):
    return lax.broadcasted_iota(jnp.int32, (rows, columns), axis)


def route_kernel(side, choice, weight, cotangent, grads, places):
    tokens = choice.shape[1]
    slots = places.shape[0]
    experts = slots // 8
    expert_at = grid_of(experts, tokens, 0)
    hot = [(expert_at == choice[k : k + 1, :]).astype(f32) for k in range(2)]
    before = (grid_of(tokens, tokens, 0) < grid_of(tokens, tokens, 1)).astype(bf16)
    earlier = dot((hot[0] + hot[1]).astype(bf16), before, ((1,), (0,)))
    same = (grid_of(tokens, tokens, 0) == grid_of(tokens, tokens, 1)).astype(f32)
    weights = exact_dot(same, weight[...], ((1,), (1,)))
    cotangents = cotangent[...].astype(f32)
    slot_at = grid_of(slots, tokens, 0)
    either = jnp.zeros((slots, tokens), f32)
    sent = jnp.zeros((slots, cotangent.shape[1]), f32)
    for k in range(2):
        rank = jnp.sum(earlier * hot[k], axis=0, keepdims=True).astype(jnp.int32)
        taken = (slot_at == choice[k : k + 1, :] * 8 + rank).astype(f32)
        either = either + taken
        rows = (weights[:, k : k + 1] * cotangents).astype(bf16)
        sent = sent + dot(taken.astype(bf16), rows, ((1,), (0,)))
    grads[...] = sent.astype(bf16)
    places[...] = either.astype(bf16)


def route(side, choice, weight, cotangent, slots):
    tokens, width = cotangent.shape
    half = width // 2
    return pl.pallas_call(
        route_kernel,
        grid_spec=pltpu.PrefetchScalarGridSpec(
            num_scalar_prefetch=1,
            grid=(1,),
            in_specs=[
                whole_block(*choice.shape),
                whole_block(*weight.shape),
                pl.BlockSpec((tokens, half), lambda i, side: (0, side[0])),
            ],
            out_specs=[whole_block(slots, half), whole_block(slots, tokens)],
        ),
        out_shape=[
            jax.ShapeDtypeStruct((slots, half), bf16),
            jax.ShapeDtypeStruct((slots, tokens), bf16),
        ],
        name="route",
    )(side, choice, weight, cotangent)


GROUP = 256
PER_GROUP = GROUP // HEAD_DIM


def per_head(rows, first):
    return jnp.concatenate(
        [
            jnp.broadcast_to(rows[first + r : first + r + 1, :], (HEAD_DIM, rows.shape[1]))
            for r in range(PER_GROUP)
        ],
        axis=0,
    )


def head_sums(x):
    return [
        jnp.sum(x[r * HEAD_DIM : (r + 1) * HEAD_DIM, :], axis=0, keepdims=True)
        for r in range(PER_GROUP)
    ]


def forward_kernel(
    scan_in, gate_in, b_proj, c_proj, log_decay, entry, gain, cotangent,
    mixed, gated_out, silu_out, slope_out, mix_out, decay_out, x_out, tail_out, local_out,
    rows_out, inverse_out, carry_out, cotangent_out,
):
    tokens = scan_in.shape[0]
    groups = scan_in.shape[1] // GROUP
    down, across = grid_of(tokens, tokens, 0), grid_of(tokens, tokens, 1)
    decays = log_decay[...]
    cum_rows = exact_dot(decays, (down <= across).astype(f32), ((1,), (0,)))
    cum_columns = exact_dot((across <= down).astype(f32), decays, ((1,), (1,)))
    total = cum_rows[:, tokens - 1 :]
    growth = jnp.exp(cum_rows)
    tail = jnp.exp(total - cum_rows)
    totals = jnp.broadcast_to(total, growth.shape)
    causal = down >= across
    for g in range(groups):
        span = slice(g * GROUP, (g + 1) * GROUP)
        states = slice(g * STATE, (g + 1) * STATE)
        first = g * PER_GROUP
        b_group, c_group = b_proj[:, states], c_proj[:, states]
        inner = dot(c_group, b_group, ((1,), (1,)))
        x = jnp.transpose(scan_in[:, span].astype(f32))
        x_b = x.astype(bf16)
        carried = dot(entry[span, :].astype(bf16), c_group, ((1,), (1,)))
        within = []
        for r in range(PER_GROUP):
            h = first + r
            gaps = cum_columns[:, h : h + 1] - cum_rows[h : h + 1, :]
            decay = jnp.where(causal, jnp.exp(jnp.where(causal, gaps, 0.0)), 0.0)
            decay_out[h] = decay
            mix = (inner * decay).astype(bf16)
            mix_out[h] = mix
            within.append(dot(x_b[r * HEAD_DIM : (r + 1) * HEAD_DIM, :], mix, ((1,), (1,))))
        carried = carried * per_head(growth, first)
        scan_out = jnp.concatenate(within, axis=0) + carried
        gate = jnp.transpose(gate_in[:, span].astype(f32))
        sig = jax.nn.sigmoid(gate)
        silu = gate * sig
        gated = scan_out * silu
        inverse = lax.rsqrt(jnp.mean(gated * gated, axis=0, keepdims=True) + rms_epsilon)
        mixed[span, :] = (gated * inverse * gain[span, :]).astype(bf16)
        gated_out[span, :] = gated
        silu_out[span, :] = silu
        slope_out[span, :] = scan_out * sig * (1.0 + gate * (1.0 - sig))
        carry_out[span, :] = carried * silu
        cotangent_out[span, :] = jnp.transpose(cotangent[:, span].astype(f32)).astype(bf16)
        inverse_out[g] = inverse
        for k, part in enumerate((growth, tail, totals)):
            rows_out[k, g] = part[first : first + PER_GROUP, :]
        x_out[span, :] = x_b
        x_tail = (x * per_head(tail, first)).astype(bf16)
        tail_out[span, :] = x_tail
        local_out[span, :] = dot(x_tail, b_group, ((1,), (0,))).astype(bf16)


def whole_call(kernel, limit, out_shape, *args):
    return pl.pallas_call(
        kernel,
        out_shape=[jax.ShapeDtypeStruct(*x) for x in out_shape],
        compiler_params=pltpu.CompilerParams(vmem_limit_bytes=limit),
    )(*args)


def forward(scan_in, gate_in, b_proj, c_proj, log_decay, entry, gain, cotangent):
    tokens, inner = scan_in.shape
    heads = log_decay.shape[0]
    return whole_call(
        forward_kernel,
        None,
        [
            ((inner, tokens), bf16),
            ((inner, tokens), f32),
            ((inner, tokens), f32),
            ((inner, tokens), f32),
            ((heads, tokens, tokens), bf16),
            ((heads, tokens, tokens), f32),
            ((inner, tokens), bf16),
            ((inner, tokens), bf16),
            ((inner, STATE), bf16),
            ((3, inner // GROUP, PER_GROUP, tokens), f32),
            ((inner // GROUP, 1, tokens), f32),
            ((inner, tokens), f32),
            ((cotangent.shape[1], tokens), bf16),
        ],
        scan_in, gate_in, b_proj, c_proj, log_decay, entry, gain, cotangent,
    )


def spread_parts(x, heads, pieces):
    high = x.astype(bf16)
    rest = x - high.astype(f32)
    middle = rest.astype(bf16)
    low = (rest - middle.astype(f32)).astype(bf16)
    return [
        jnp.broadcast_to(part.astype(f32)[:, None, :], (heads, pieces, STATE)).reshape(
            heads * pieces, 1, STATE
        )
        for part in (high, middle, low)
    ]


def message_kernel(
    side, grad_own, grad_far, out_own, out_far, gain, gated_in, silu_in, carry_in, c_proj, local_in,
    rows_in, inverse_in,
    message, grad_out,
):
    pieces = GROUP // 16
    grad_mixed = dot(out_own[...], grad_own[...], ((1,), (0,)))
    grad_mixed = grad_mixed + dot(out_far[...], grad_far[...], ((1,), (0,)))
    inverse = inverse_in[0]
    unit = gated_in[...] * inverse
    grad_unit = grad_mixed * gain[...]
    mean = jnp.mean(grad_unit * unit, axis=0, keepdims=True)
    grad_gated = inverse * (grad_unit - unit * mean)
    grad_out[...] = grad_gated
    grown = (grad_gated * silu_in[...] * per_head(rows_in[0, 0], 0)).astype(bf16)
    block_state = dot(grown, c_proj[...], ((1,), (0,))).astype(bf16)
    message[:, 0:16, :] = block_state.reshape(pieces, 16, STATE)
    message[:, 16:32, :] = local_in[...].reshape(pieces, 16, STATE)
    own = jnp.concatenate(head_sums(grad_gated * carry_in[...]), axis=0)
    own = jnp.broadcast_to(jnp.sum(own, axis=1, keepdims=True), (PER_GROUP, STATE))
    per = pieces // PER_GROUP
    zero = jnp.zeros((pieces, 2, STATE), f32)
    extra = jnp.concatenate(
        spread_parts(rows_in[2, 0], PER_GROUP, per) + spread_parts(own, PER_GROUP, per) + [zero],
        axis=1,
    )
    message[:, 32:40, :] = extra.astype(bf16)


def state_message(side, grad_own, grad_far, w_out, gain, gated, silu, carry, c_proj, local, rows, inverse):
    half, tokens = grad_own.shape
    inner = gain.shape[0]
    pieces = GROUP // 16
    channels = pl.BlockSpec((GROUP, tokens), lambda i, side: (i, 0))
    return pl.pallas_call(
        message_kernel,
        grid_spec=pltpu.PrefetchScalarGridSpec(
            num_scalar_prefetch=1,
            grid=(inner // GROUP,),
            in_specs=[
                whole_block(half, tokens),
                whole_block(half, tokens),
                pl.BlockSpec((GROUP, half), lambda i, side: (i, side[0])),
                pl.BlockSpec((GROUP, half), lambda i, side: (i, 1 - side[0])),
                pl.BlockSpec((GROUP, 1), lambda i, side: (i, 0)),
                channels,
                channels,
                channels,
                pl.BlockSpec((tokens, STATE), lambda i, side: (0, i)),
                pl.BlockSpec((GROUP, STATE), lambda i, side: (i, 0)),
                pl.BlockSpec((3, 1, PER_GROUP, tokens), lambda i, side: (0, i, 0, 0)),
                pl.BlockSpec((1, 1, tokens), lambda i, side: (i, 0, 0)),
            ],
            out_specs=[
                pl.BlockSpec((pieces, 40, STATE), lambda i, side: (i, 0, 0)),
                channels,
            ],
        ),
        out_shape=[
            jax.ShapeDtypeStruct((inner // 16, 40, STATE), bf16),
            jax.ShapeDtypeStruct((inner, tokens), f32),
        ],
        name="message",
    )(side, grad_own, grad_far, w_out, w_out, gain, gated, silu, carry, c_proj, local, rows, inverse)


def inside_kernel(
    grad_in, gated_in, silu_in, slope_in, mix_in, decay_in, x_in, b_proj, c_proj, entry, rows_in,
    gate_grad, x_grad, b_grad, c_grad, y_dots,
):
    tokens = x_in.shape[1]
    grad_gated = grad_in[...]
    gate_grad[...] = jnp.transpose(grad_gated * slope_in[...]).astype(bf16)
    grad_y = grad_gated * silu_in[...]
    grad_y_b = grad_y.astype(bf16)
    grown = (grad_y * per_head(rows_in[0, 0], 0)).astype(bf16)
    x = x_in[...]
    weights = jnp.zeros((tokens, tokens), f32)
    inside = []
    for r in range(PER_GROUP):
        head = slice(r * HEAD_DIM, (r + 1) * HEAD_DIM)
        inside.append(dot(grad_y_b[head, :], mix_in[r], ((1,), (0,))))
        weights = weights + decay_in[r] * dot(grad_y_b[head, :], x[head, :], ((0,), (0,)))
    x_grad[...] = jnp.concatenate(inside, axis=0)
    weights = weights.astype(bf16)
    c_grad[...] = (
        dot(weights, b_proj[...], ((1,), (0,)))
        + dot(grown, entry[...].astype(bf16), ((0,), (0,)))
    ).astype(bf16)
    b_grad[...] = dot(weights, c_proj[...], ((0,), (0,)))
    y_dots[0] = jnp.concatenate(head_sums(grad_gated * gated_in[...]), axis=0)


def inside_grads(grad, gated, silu, slope, mix, decay, x, b_proj, c_proj, entry, rows):
    inner, tokens = grad.shape
    channels = pl.BlockSpec((GROUP, tokens), lambda i: (i, 0))
    tokens_by = pl.BlockSpec((tokens, STATE), lambda i: (0, i))
    square = pl.BlockSpec((PER_GROUP, tokens, tokens), lambda i: (i, 0, 0))
    outs = [
        ((tokens, inner), bf16),
        ((inner, tokens), f32),
        (b_proj.shape, f32),
        (b_proj.shape, bf16),
        ((inner // GROUP, PER_GROUP, tokens), f32),
    ]
    return pl.pallas_call(
        inside_kernel,
        grid=(inner // GROUP,),
        in_specs=[channels] * 4
        + [square] * 2
        + [channels, tokens_by, tokens_by, pl.BlockSpec((GROUP, STATE), lambda i: (i, 0))]
        + [pl.BlockSpec((3, 1, PER_GROUP, tokens), lambda i: (0, i, 0, 0))],
        out_specs=[
            pl.BlockSpec((tokens, GROUP), lambda i: (0, i)),
            channels,
            tokens_by,
            tokens_by,
            pl.BlockSpec((1, PER_GROUP, tokens), lambda i: (i, 0, 0)),
        ],
        out_shape=[jax.ShapeDtypeStruct(*x) for x in outs],
        name="inside",
    )(grad, gated, silu, slope, mix, decay, x, b_proj, c_proj, entry, rows)


def owner_kernel(lead, came, back, values, local, later):
    blocks = came.shape[0]
    values[...] = came[:, 0:16, :].astype(f32)
    local[...] = came[:, 16:32, :].astype(f32)
    extra = came[:, 32:40, :].astype(f32)
    first, second = grid_of(blocks, blocks, 0), grid_of(blocks, blocks, 1)
    after = (second > first).astype(bf16)
    gaps = jnp.zeros((blocks, blocks), f32)
    for k in range(3):
        part = jnp.where(first < second, extra[:, k, :blocks], 0.0).astype(bf16)
        gaps = gaps + dot(after, part, ((1,), (0,)))
    weights = jnp.where(second > first, jnp.exp(gaps), 0.0)
    high = weights.astype(bf16)
    low = (weights - high.astype(f32)).astype(bf16)
    total = jnp.zeros((blocks, STATE), f32)
    for r in range(16):
        piece = values[:, r, :].astype(bf16)
        found = dot(high, piece, ((1,), (0,))) + dot(low, piece, ((1,), (0,)))
        later[:, r, :] = found
        total = total + found * local[:, r, :]
    total = jnp.broadcast_to(jnp.sum(total, axis=1, keepdims=True), (blocks, STATE))
    sums = extra[:, 3, :] + extra[:, 4, :] + extra[:, 5, :]
    own = jnp.where(lead[0] == 1, sums, 0.0) - total
    carried = exact_dot(after.astype(f32), own, ((1,), (0,)))
    back[:, 0:16, :] = later[...].astype(bf16)
    zero = jnp.zeros((blocks, 5, STATE), f32)
    back[:, 16:24, :] = jnp.concatenate(spread_parts(carried, blocks, 1) + [zero], axis=1).astype(
        bf16
    )


def owner_scan(lead, came):
    blocks = came.shape[0]
    scratch = pltpu.VMEM((blocks, 16, STATE), f32)
    return pl.pallas_call(
        owner_kernel,
        grid_spec=pltpu.PrefetchScalarGridSpec(
            num_scalar_prefetch=1,
            grid=(1,),
            in_specs=[whole_block(*came.shape)],
            out_specs=whole_block(blocks, 24, STATE),
            scratch_shapes=[scratch] * 3,
        ),
        out_shape=jax.ShapeDtypeStruct((blocks, 24, STATE), bf16),
        name="owner",
        compiler_params=pltpu.CompilerParams(vmem_limit_bytes=6 << 20),
    )(lead, came)


def final_kernel(back, b_proj, x_in, tail_in, rows_in, x_inside, y_dots, b_inside, x_grad, b_grad, decay_grad):
    groups = x_in.shape[0] // GROUP
    pieces = GROUP // 16
    tokens = x_in.shape[1]
    heads = groups * PER_GROUP
    dots = []
    for g in range(groups):
        span = slice(g * GROUP, (g + 1) * GROUP)
        states = slice(g * STATE, (g + 1) * STATE)
        later = back[g * pieces : (g + 1) * pieces, 0:16, :].reshape(GROUP, STATE)
        carried = dot(later, b_proj[:, states], ((1,), (1,)))
        grad = x_inside[span, :] + carried * per_head(rows_in[1, g], 0)
        x_grad[:, span] = jnp.transpose(grad).astype(bf16)
        b_grad[:, states] = (
            b_inside[:, states] + dot(tail_in[span, :], later, ((0,), (0,)))
        ).astype(bf16)
        dots = dots + head_sums(x_in[span, :].astype(f32) * grad)
    own = jnp.concatenate([y_dots[g] for g in range(groups)], axis=0)
    own = own - jnp.concatenate(dots, axis=0)
    after = (grid_of(tokens, tokens, 0) >= grid_of(tokens, tokens, 1)).astype(f32)
    extra = jnp.sum(back[:, 16:24, :].astype(f32), axis=1)
    extra = jnp.sum(extra.reshape(heads, extra.shape[0] // heads, STATE), axis=1)
    decay_grad[...] = exact_dot(own, after, ((1,), (0,))) + extra


def final(back, b_proj, x, x_tail, rows, x_inside, y_dots, b_inside):
    inner, tokens = x.shape
    return whole_call(
        final_kernel,
        6 << 20,
        [
            ((tokens, inner), bf16),
            (b_proj.shape, bf16),
            ((inner // HEAD_DIM, tokens), f32),
        ],
        back, b_proj, x, x_tail, rows, x_inside, y_dots, b_inside,
    )


def body(
    mixer_output,
    layer_cotangent,
    expert_choice,
    route_weight,
    gate_pre,
    up_pre,
    w_gate,
    w_up,
    w_down,
    w_out,
    norm_gain,
    scan_in,
    gate_in,
    b_proj,
    c_proj,
    log_decay,
    entry_state,
):
    experts = lax.axis_size(SP)
    _, width = mixer_output.shape
    capacity = gate_pre.shape[1] // experts
    half = width // 2
    start = lax.axis_index("tp") * half

    side = lax.axis_index("tp")[None]
    send_grads, either = route(
        side, expert_choice.T, route_weight.T, layer_cotangent, experts * capacity
    )
    hidden_half = lax.dynamic_slice_in_dim(mixer_output, start, half, 1)
    cotangent_half = lax.dynamic_slice_in_dim(layer_cotangent, start, half, 1)
    send_hidden = dot(either, hidden_half, ((1,), (0,))).astype(bf16)
    send_grads = send_grads.reshape(experts, capacity, half)
    send_hidden = send_hidden.reshape(experts, capacity, half)
    inner = scan_in.shape[1]
    gain = norm_gain.astype(f32)[:, None]
    entry = entry_state.reshape(inner, STATE)
    mixed, *saved, x_tail, local, rows, inverse, carry, cotangent_rows = forward(
        scan_in, gate_in, b_proj, c_proj, log_decay.T, entry, gain, cotangent_half
    )
    gated, silu, slope, mix, decay, x = saved
    came_grads = lax.all_to_all(send_grads, SP, 0, 0, tiled=True)
    send_hidden, came_grads = lax.optimization_barrier((send_hidden, came_grads))
    came_hidden = lax.all_to_all(send_hidden, SP, 0, 0, tiled=True)
    grads_own = came_grads.reshape(-1, half)
    grads_far = swapped(grads_own)
    active, gate_grad, up_grad, rows_own, rows_far = expert_rows(
        side, grads_own, grads_far, gate_pre[0], up_pre[0], w_down[0], w_gate[0], w_up[0]
    )
    summed = (rows_own.astype(f32) + swapped(rows_far).astype(f32)).astype(bf16)
    summed, came_hidden = lax.optimization_barrier((summed, came_hidden))
    returned = lax.all_to_all(summed.reshape(experts, capacity, half), SP, 0, 0, tiled=True)
    hidden_own = came_hidden.reshape(-1, half)
    hidden_far = swapped(hidden_own)
    down_wgrad, gate_wgrad, up_wgrad = expert_weights(
        side, active, gate_grad, up_grad, grads_own, grads_far, hidden_own, hidden_far
    )
    moe_terms = dot(returned.reshape(-1, half), either, ((0,), (0,)))
    grad_own = (cotangent_rows.astype(f32) + moe_terms).astype(bf16)
    grad_far = swapped(grad_own)
    grad_hidden = jnp.where(
        side == 0,
        jnp.concatenate([grad_own, grad_far], axis=0),
        jnp.concatenate([grad_far, grad_own], axis=0),
    )

    message, grad_gated = state_message(
        side, grad_own, grad_far, w_out, gain, gated, silu, carry, c_proj, local, rows, inverse
    )
    came_states = lax.all_to_all(message, SP, 0, 0, tiled=True)
    lead = lax.rem(lax.axis_index(SP), HEAD_DIM // 16) == 0
    back = owner_scan(lead.astype(jnp.int32)[None], came_states)
    grad_gate_in, x_inside, b_inside, grad_c_proj, y_dots = inside_grads(
        grad_gated, gated, silu, slope, mix, decay, x, b_proj, c_proj, entry, rows
    )
    back = lax.all_to_all(back, SP, 0, 0, tiled=True)
    grad_scan_in, grad_b_proj, decay_grad = final(
        back, b_proj, x, x_tail, rows, x_inside, y_dots, b_inside
    )
    grad_log_decay = decay_grad.T

    line = lax.axis_size("sp_0")
    mixed, gate_wgrad = lax.optimization_barrier((mixed, gate_wgrad))
    mixed_line = from_line([mixed] * line, "sp_0")
    grads_line = from_line(pieces_for(grad_hidden, "sp_0", 0), "sp_0")
    product = dot(
        jnp.concatenate(grads_line, axis=1), jnp.concatenate(mixed_line, axis=1), ((1,), (1,))
    ).astype(bf16)
    parts = from_line(pieces_for(product, "sp_1", 0), "sp_1")
    product = sum(part.astype(f32) for part in parts).astype(bf16)
    parts = from_line(pieces_for(product, "sp_2", 0), "sp_2")
    grad_out_proj = sum(part.astype(f32) for part in parts)

    return (
        gate_wgrad[None],
        up_wgrad[None],
        down_wgrad[None],
        grad_out_proj,
        grad_scan_in,
        grad_gate_in,
        grad_b_proj,
        grad_c_proj,
        grad_log_decay,
    )


def solution(mesh):
    split = Mesh(mesh.devices.reshape(4, 4, 4, mesh.shape["tp"]), ("sp_0", "sp_1", "sp_2", "tp"))
    return jax.shard_map(
        body,
        mesh=split,
        in_specs=(
            P(SP, None),
            P(SP, None),
            P(SP, None),
            P(SP, None),
            P(SP, None, "tp"),
            P(SP, None, "tp"),
            P(SP, None, "tp"),
            P(SP, None, "tp"),
            P(SP, "tp", None),
            P("tp", None),
            P("tp"),
            P(SP, "tp"),
            P(SP, "tp"),
            P(SP, "tp"),
            P(SP, "tp"),
            P(SP, "tp"),
            P(SP, "tp", None, None),
        ),
        out_specs=(
            P(SP, None, "tp"),
            P(SP, None, "tp"),
            P(SP, "tp", None),
            P(SP, "tp"),
            P(SP, "tp"),
            P(SP, "tp"),
            P(SP, "tp"),
            P(SP, "tp"),
            P(SP, "tp"),
        ),
        check_vma=False,
    )
```

```python
import jax
import jax.numpy as jnp
from jax import lax
from jax.sharding import Mesh
from jax.experimental import pallas as pl
from jax.experimental.pallas import tpu as pltpu
from jax.sharding import PartitionSpec as P

HEAD_DIM = 64
STATE = 128
SP = ("sp_0", "sp_1", "sp_2")


rms_epsilon = 1e-05
clamp_limit = 7.0
swish_alpha = 1.702

bf16 = jnp.bfloat16
f32 = jnp.float32


def dot(a, b, dims):
    return lax.dot_general(a, b, (dims, ((), ())), preferred_element_type=f32)


def swapped(x):
    return lax.ppermute(x, "tp", [(0, 1), (1, 0)])


def from_line(parts, axis):
    size = lax.axis_size(axis)
    return [parts[0]] + [
        lax.ppermute(parts[k], axis, [(i, (i + k) % size) for i in range(size)])
        for k in range(1, size)
    ]


def pieces_for(x, axis, dim):
    size, spot = lax.axis_size(axis), lax.axis_index(axis)
    span = x.shape[dim] // size
    return [
        lax.dynamic_slice_in_dim(x, lax.rem(spot + k, size) * span, span, dim) for k in range(size)
    ]


def expert_rows_kernel(
    side, mine, other, gate_value, up_value, down_own, down_far, gate_own, gate_far, up_own, up_far,
    active, gate_grad, up_grad, rows_own, rows_far,
):
    act_grad = dot(mine[...], down_own[...], ((1,), (1,)))
    act_grad = act_grad + dot(other[...], down_far[...], ((1,), (1,)))
    gate_full = gate_value[...].astype(f32)
    up_full = up_value[...].astype(f32)
    gate_clip = jnp.minimum(gate_full, clamp_limit)
    up_clip = jnp.clip(up_full, -clamp_limit, clamp_limit)
    sigmoid_gate = jax.nn.sigmoid(swish_alpha * gate_clip)
    swish_gate = gate_clip * sigmoid_gate
    active[...] = ((up_clip + 1.0) * swish_gate).astype(bf16)
    inside = (up_full > -clamp_limit) & (up_full < clamp_limit)
    up_side = jnp.where(inside, act_grad * swish_gate, 0.0).astype(bf16)
    slope = sigmoid_gate + swish_alpha * gate_clip * sigmoid_gate * (1.0 - sigmoid_gate)
    gate_side = jnp.where(
        gate_full < clamp_limit, act_grad * (up_clip + 1.0) * slope, 0.0
    ).astype(bf16)
    up_grad[...] = up_side
    gate_grad[...] = gate_side
    far = dot(gate_side, gate_far[...], ((1,), (1,))) + dot(up_side, up_far[...], ((1,), (1,)))
    rows_far[...] = far.astype(bf16)
    own = dot(gate_side, gate_own[...], ((1,), (1,))) + dot(up_side, up_own[...], ((1,), (1,)))
    rows_own[...] = own.astype(bf16)


def whole_block(*shape):
    return pl.BlockSpec(shape, lambda i, side: (0,) * len(shape))


def expert_rows(side, mine, other, gate_value, up_value, w_down, w_gate, w_up):
    rows, half = mine.shape
    hidden = gate_value.shape[1]
    row_block = whole_block(rows, half)
    act_block = whole_block(rows, hidden)
    down = [
        pl.BlockSpec((hidden, half), lambda i, side: (0, side[0])),
        pl.BlockSpec((hidden, half), lambda i, side: (0, 1 - side[0])),
    ]
    tall = [
        pl.BlockSpec((half, hidden), lambda i, side: (side[0], 0)),
        pl.BlockSpec((half, hidden), lambda i, side: (1 - side[0], 0)),
    ]
    act = jax.ShapeDtypeStruct((rows, hidden), bf16)
    out = jax.ShapeDtypeStruct((rows, half), bf16)
    return pl.pallas_call(
        expert_rows_kernel,
        grid_spec=pltpu.PrefetchScalarGridSpec(
            num_scalar_prefetch=1,
            grid=(1,),
            in_specs=[row_block, row_block, act_block, act_block] + down + tall + tall,
            out_specs=[act_block] * 3 + [row_block] * 2,
        ),
        out_shape=[act] * 3 + [out] * 2,
        name="expert_rows",
    )(side, mine, other, gate_value, up_value, w_down, w_down, w_gate, w_gate, w_up, w_up)


def weights_kernel(
    side, active, gate_grad, up_grad, grads_own, grads_far, hidden_own, hidden_far,
    down_out, gate_out, up_out,
):
    def write(grads, hidden):
        down_out[...] = dot(active[...], grads, ((0,), (0,))).astype(bf16)
        gate_out[...] = dot(hidden, gate_grad[...], ((0,), (0,))).astype(bf16)
        up_out[...] = dot(hidden, up_grad[...], ((0,), (0,))).astype(bf16)

    @pl.when(pl.program_id(0) < 2)
    def _():
        write(grads_own[...], hidden_own[...])

    @pl.when(pl.program_id(0) >= 2)
    def _():
        write(grads_far[...], hidden_far[...])


def expert_weights(side, active, gate_grad, up_grad, grads_own, grads_far, hidden_own, hidden_far):
    rows, half = grads_own.shape
    hidden = active.shape[1]
    own = pl.BlockSpec((rows, half // 2), lambda i, side: (0, jnp.minimum(i, 1)))
    far = pl.BlockSpec((rows, half // 2), lambda i, side: (0, jnp.maximum(i - 2, 0)))

    def place(i, side):
        return lax.rem(i + 2 * side[0], 4)

    tall = pl.BlockSpec((half // 2, hidden), lambda i, side: (place(i, side), 0))
    return pl.pallas_call(
        weights_kernel,
        grid_spec=pltpu.PrefetchScalarGridSpec(
            num_scalar_prefetch=1,
            grid=(4,),
            in_specs=[whole_block(rows, hidden)] * 3 + [own, far, own, far],
            out_specs=[
                pl.BlockSpec((hidden, half // 2), lambda i, side: (0, place(i, side))),
                tall,
                tall,
            ],
        ),
        out_shape=[jax.ShapeDtypeStruct((hidden, 2 * half), bf16)]
        + [jax.ShapeDtypeStruct((2 * half, hidden), bf16)] * 2,
        name="weights",
    )(side, active, gate_grad, up_grad, grads_own, grads_far, hidden_own, hidden_far)


def exact_dot(a, b, dims):
    return lax.dot_general(
        a, b, (dims, ((), ())), preferred_element_type=f32, precision=lax.Precision.HIGHEST
    )


def grid_of(rows, columns, axis):
    return lax.broadcasted_iota(jnp.int32, (rows, columns), axis)


def route_kernel(side, choice, weight, cotangent, grads, places):
    tokens = choice.shape[1]
    slots = places.shape[0]
    experts = slots // 8
    expert_at = grid_of(experts, tokens, 0)
    hot = [(expert_at == choice[k : k + 1, :]).astype(f32) for k in range(2)]
    before = (grid_of(tokens, tokens, 0) < grid_of(tokens, tokens, 1)).astype(bf16)
    earlier = dot((hot[0] + hot[1]).astype(bf16), before, ((1,), (0,)))
    same = (grid_of(tokens, tokens, 0) == grid_of(tokens, tokens, 1)).astype(f32)
    weights = exact_dot(same, weight[...], ((1,), (1,)))
    cotangents = cotangent[...].astype(f32)
    slot_at = grid_of(slots, tokens, 0)
    either = jnp.zeros((slots, tokens), f32)
    sent = jnp.zeros((slots, cotangent.shape[1]), f32)
    for k in range(2):
        rank = jnp.sum(earlier * hot[k], axis=0, keepdims=True).astype(jnp.int32)
        taken = (slot_at == choice[k : k + 1, :] * 8 + rank).astype(f32)
        either = either + taken
        rows = (weights[:, k : k + 1] * cotangents).astype(bf16)
        sent = sent + dot(taken.astype(bf16), rows, ((1,), (0,)))
    grads[...] = sent.astype(bf16)
    places[...] = either.astype(bf16)


def route(side, choice, weight, cotangent, slots):
    tokens, width = cotangent.shape
    half = width // 2
    return pl.pallas_call(
        route_kernel,
        grid_spec=pltpu.PrefetchScalarGridSpec(
            num_scalar_prefetch=1,
            grid=(1,),
            in_specs=[
                whole_block(*choice.shape),
                whole_block(*weight.shape),
                pl.BlockSpec((tokens, half), lambda i, side: (0, side[0])),
            ],
            out_specs=[whole_block(slots, half), whole_block(slots, tokens)],
        ),
        out_shape=[
            jax.ShapeDtypeStruct((slots, half), bf16),
            jax.ShapeDtypeStruct((slots, tokens), bf16),
        ],
        name="route",
    )(side, choice, weight, cotangent)


GROUP = 256
PER_GROUP = GROUP // HEAD_DIM


def per_head(rows, first):
    return jnp.concatenate(
        [
            jnp.broadcast_to(rows[first + r : first + r + 1, :], (HEAD_DIM, rows.shape[1]))
            for r in range(PER_GROUP)
        ],
        axis=0,
    )


def head_sums(x):
    return [
        jnp.sum(x[r * HEAD_DIM : (r + 1) * HEAD_DIM, :], axis=0, keepdims=True)
        for r in range(PER_GROUP)
    ]


def forward_kernel(
    scan_in, gate_in, b_proj, c_proj, log_decay, entry, gain, cotangent,
    mixed, gated_out, silu_out, slope_out, mix_out, decay_out, x_out, tail_out, local_out,
    rows_out, inverse_out, carry_out, cotangent_out,
):
    tokens = scan_in.shape[0]
    groups = scan_in.shape[1] // GROUP
    down, across = grid_of(tokens, tokens, 0), grid_of(tokens, tokens, 1)
    decays = log_decay[...]
    cum_rows = exact_dot(decays, (down <= across).astype(f32), ((1,), (0,)))
    cum_columns = exact_dot((across <= down).astype(f32), decays, ((1,), (1,)))
    total = cum_rows[:, tokens - 1 :]
    growth = jnp.exp(cum_rows)
    tail = jnp.exp(total - cum_rows)
    totals = jnp.broadcast_to(total, growth.shape)
    causal = down >= across
    for g in range(groups):
        span = slice(g * GROUP, (g + 1) * GROUP)
        states = slice(g * STATE, (g + 1) * STATE)
        first = g * PER_GROUP
        b_group, c_group = b_proj[:, states], c_proj[:, states]
        inner = dot(c_group, b_group, ((1,), (1,)))
        x = jnp.transpose(scan_in[:, span].astype(f32))
        x_b = x.astype(bf16)
        carried = dot(entry[span, :].astype(bf16), c_group, ((1,), (1,)))
        within = []
        for r in range(PER_GROUP):
            h = first + r
            gaps = cum_columns[:, h : h + 1] - cum_rows[h : h + 1, :]
            decay = jnp.where(causal, jnp.exp(jnp.where(causal, gaps, 0.0)), 0.0)
            decay_out[h] = decay
            mix = (inner * decay).astype(bf16)
            mix_out[h] = mix
            within.append(dot(x_b[r * HEAD_DIM : (r + 1) * HEAD_DIM, :], mix, ((1,), (1,))))
        carried = carried * per_head(growth, first)
        scan_out = jnp.concatenate(within, axis=0) + carried
        gate = jnp.transpose(gate_in[:, span].astype(f32))
        sig = jax.nn.sigmoid(gate)
        silu = gate * sig
        gated = scan_out * silu
        inverse = lax.rsqrt(jnp.mean(gated * gated, axis=0, keepdims=True) + rms_epsilon)
        mixed[span, :] = (gated * inverse * gain[span, :]).astype(bf16)
        gated_out[span, :] = gated
        silu_out[span, :] = silu
        slope_out[span, :] = scan_out * sig * (1.0 + gate * (1.0 - sig))
        carry_out[span, :] = carried * silu
        cotangent_out[span, :] = jnp.transpose(cotangent[:, span].astype(f32)).astype(bf16)
        inverse_out[g] = inverse
        for k, part in enumerate((growth, tail, totals)):
            rows_out[k, g] = part[first : first + PER_GROUP, :]
        x_out[span, :] = x_b
        x_tail = (x * per_head(tail, first)).astype(bf16)
        tail_out[span, :] = x_tail
        local_out[span, :] = dot(x_tail, b_group, ((1,), (0,))).astype(bf16)


def whole_call(kernel, limit, out_shape, *args):
    return pl.pallas_call(
        kernel,
        out_shape=[jax.ShapeDtypeStruct(*x) for x in out_shape],
        compiler_params=pltpu.CompilerParams(vmem_limit_bytes=limit),
    )(*args)


def forward(scan_in, gate_in, b_proj, c_proj, log_decay, entry, gain, cotangent):
    tokens, inner = scan_in.shape
    heads = log_decay.shape[0]
    return whole_call(
        forward_kernel,
        None,
        [
            ((inner, tokens), bf16),
            ((inner, tokens), f32),
            ((inner, tokens), f32),
            ((inner, tokens), f32),
            ((heads, tokens, tokens), bf16),
            ((heads, tokens, tokens), f32),
            ((inner, tokens), bf16),
            ((inner, tokens), bf16),
            ((inner, STATE), bf16),
            ((3, inner // GROUP, PER_GROUP, tokens), f32),
            ((inner // GROUP, 1, tokens), f32),
            ((inner, tokens), f32),
            ((cotangent.shape[1], tokens), bf16),
        ],
        scan_in, gate_in, b_proj, c_proj, log_decay, entry, gain, cotangent,
    )


def spread_parts(x, heads, pieces):
    high = x.astype(bf16)
    rest = x - high.astype(f32)
    middle = rest.astype(bf16)
    low = (rest - middle.astype(f32)).astype(bf16)
    return [
        jnp.broadcast_to(part.astype(f32)[:, None, :], (heads, pieces, STATE)).reshape(
            heads * pieces, 1, STATE
        )
        for part in (high, middle, low)
    ]


def message_kernel(
    side, grad_own, grad_far, out_own, out_far, gain, gated_in, silu_in, carry_in, c_proj, local_in,
    rows_in, inverse_in,
    message, grad_out,
):
    pieces = GROUP // 16
    grad_mixed = dot(out_own[...], grad_own[...], ((1,), (0,)))
    grad_mixed = grad_mixed + dot(out_far[...], grad_far[...], ((1,), (0,)))
    inverse = inverse_in[0]
    unit = gated_in[...] * inverse
    grad_unit = grad_mixed * gain[...]
    mean = jnp.mean(grad_unit * unit, axis=0, keepdims=True)
    grad_gated = inverse * (grad_unit - unit * mean)
    grad_out[...] = grad_gated
    grown = (grad_gated * silu_in[...] * per_head(rows_in[0, 0], 0)).astype(bf16)
    block_state = dot(grown, c_proj[...], ((1,), (0,))).astype(bf16)
    message[:, 0:16, :] = block_state.reshape(pieces, 16, STATE)
    message[:, 16:32, :] = local_in[...].reshape(pieces, 16, STATE)
    own = jnp.concatenate(head_sums(grad_gated * carry_in[...]), axis=0)
    own = jnp.broadcast_to(jnp.sum(own, axis=1, keepdims=True), (PER_GROUP, STATE))
    per = pieces // PER_GROUP
    zero = jnp.zeros((pieces, 2, STATE), f32)
    extra = jnp.concatenate(
        spread_parts(rows_in[2, 0], PER_GROUP, per) + spread_parts(own, PER_GROUP, per) + [zero],
        axis=1,
    )
    message[:, 32:40, :] = extra.astype(bf16)


def state_message(side, grad_own, grad_far, w_out, gain, gated, silu, carry, c_proj, local, rows, inverse):
    half, tokens = grad_own.shape
    inner = gain.shape[0]
    pieces = GROUP // 16
    channels = pl.BlockSpec((GROUP, tokens), lambda i, side: (i, 0))
    return pl.pallas_call(
        message_kernel,
        grid_spec=pltpu.PrefetchScalarGridSpec(
            num_scalar_prefetch=1,
            grid=(inner // GROUP,),
            in_specs=[
                whole_block(half, tokens),
                whole_block(half, tokens),
                pl.BlockSpec((GROUP, half), lambda i, side: (i, side[0])),
                pl.BlockSpec((GROUP, half), lambda i, side: (i, 1 - side[0])),
                pl.BlockSpec((GROUP, 1), lambda i, side: (i, 0)),
                channels,
                channels,
                channels,
                pl.BlockSpec((tokens, STATE), lambda i, side: (0, i)),
                pl.BlockSpec((GROUP, STATE), lambda i, side: (i, 0)),
                pl.BlockSpec((3, 1, PER_GROUP, tokens), lambda i, side: (0, i, 0, 0)),
                pl.BlockSpec((1, 1, tokens), lambda i, side: (i, 0, 0)),
            ],
            out_specs=[
                pl.BlockSpec((pieces, 40, STATE), lambda i, side: (i, 0, 0)),
                channels,
            ],
        ),
        out_shape=[
            jax.ShapeDtypeStruct((inner // 16, 40, STATE), bf16),
            jax.ShapeDtypeStruct((inner, tokens), f32),
        ],
        name="message",
    )(side, grad_own, grad_far, w_out, w_out, gain, gated, silu, carry, c_proj, local, rows, inverse)


def inside_kernel(
    grad_in, gated_in, silu_in, slope_in, mix_in, decay_in, x_in, b_proj, c_proj, entry, rows_in,
    gate_grad, x_grad, b_grad, c_grad, y_dots,
):
    tokens = x_in.shape[1]
    grad_gated = grad_in[...]
    gate_grad[...] = jnp.transpose(grad_gated * slope_in[...]).astype(bf16)
    grad_y = grad_gated * silu_in[...]
    grad_y_b = grad_y.astype(bf16)
    grown = (grad_y * per_head(rows_in[0, 0], 0)).astype(bf16)
    x = x_in[...]
    weights = jnp.zeros((tokens, tokens), f32)
    inside = []
    for r in range(PER_GROUP):
        head = slice(r * HEAD_DIM, (r + 1) * HEAD_DIM)
        inside.append(dot(grad_y_b[head, :], mix_in[r], ((1,), (0,))))
        weights = weights + decay_in[r] * dot(grad_y_b[head, :], x[head, :], ((0,), (0,)))
    x_grad[...] = jnp.concatenate(inside, axis=0)
    weights = weights.astype(bf16)
    c_grad[...] = (
        dot(weights, b_proj[...], ((1,), (0,)))
        + dot(grown, entry[...].astype(bf16), ((0,), (0,)))
    ).astype(bf16)
    b_grad[...] = dot(weights, c_proj[...], ((0,), (0,)))
    y_dots[0] = jnp.concatenate(head_sums(grad_gated * gated_in[...]), axis=0)


def inside_grads(grad, gated, silu, slope, mix, decay, x, b_proj, c_proj, entry, rows):
    inner, tokens = grad.shape
    channels = pl.BlockSpec((GROUP, tokens), lambda i: (i, 0))
    tokens_by = pl.BlockSpec((tokens, STATE), lambda i: (0, i))
    square = pl.BlockSpec((PER_GROUP, tokens, tokens), lambda i: (i, 0, 0))
    outs = [
        ((tokens, inner), bf16),
        ((inner, tokens), f32),
        (b_proj.shape, f32),
        (b_proj.shape, bf16),
        ((inner // GROUP, PER_GROUP, tokens), f32),
    ]
    return pl.pallas_call(
        inside_kernel,
        grid=(inner // GROUP,),
        in_specs=[channels] * 4
        + [square] * 2
        + [channels, tokens_by, tokens_by, pl.BlockSpec((GROUP, STATE), lambda i: (i, 0))]
        + [pl.BlockSpec((3, 1, PER_GROUP, tokens), lambda i: (0, i, 0, 0))],
        out_specs=[
            pl.BlockSpec((tokens, GROUP), lambda i: (0, i)),
            channels,
            tokens_by,
            tokens_by,
            pl.BlockSpec((1, PER_GROUP, tokens), lambda i: (i, 0, 0)),
        ],
        out_shape=[jax.ShapeDtypeStruct(*x) for x in outs],
        name="inside",
    )(grad, gated, silu, slope, mix, decay, x, b_proj, c_proj, entry, rows)


def owner_kernel(lead, came, back, values, local, later):
    blocks = came.shape[0]
    values[...] = came[:, 0:16, :].astype(f32)
    local[...] = came[:, 16:32, :].astype(f32)
    extra = came[:, 32:40, :].astype(f32)
    first, second = grid_of(blocks, blocks, 0), grid_of(blocks, blocks, 1)
    after = (second > first).astype(bf16)
    gaps = jnp.zeros((blocks, blocks), f32)
    for k in range(3):
        part = jnp.where(first < second, extra[:, k, :blocks], 0.0).astype(bf16)
        gaps = gaps + dot(after, part, ((1,), (0,)))
    weights = jnp.where(second > first, jnp.exp(gaps), 0.0)
    high = weights.astype(bf16)
    low = (weights - high.astype(f32)).astype(bf16)
    total = jnp.zeros((blocks, STATE), f32)
    for r in range(16):
        piece = values[:, r, :].astype(bf16)
        found = dot(high, piece, ((1,), (0,))) + dot(low, piece, ((1,), (0,)))
        later[:, r, :] = found
        total = total + found * local[:, r, :]
    total = jnp.broadcast_to(jnp.sum(total, axis=1, keepdims=True), (blocks, STATE))
    sums = extra[:, 3, :] + extra[:, 4, :] + extra[:, 5, :]
    own = jnp.where(lead[0] == 1, sums, 0.0) - total
    carried = exact_dot(after.astype(f32), own, ((1,), (0,)))
    back[:, 0:16, :] = later[...].astype(bf16)
    zero = jnp.zeros((blocks, 5, STATE), f32)
    back[:, 16:24, :] = jnp.concatenate(spread_parts(carried, blocks, 1) + [zero], axis=1).astype(
        bf16
    )


def owner_scan(lead, came):
    blocks = came.shape[0]
    scratch = pltpu.VMEM((blocks, 16, STATE), f32)
    return pl.pallas_call(
        owner_kernel,
        grid_spec=pltpu.PrefetchScalarGridSpec(
            num_scalar_prefetch=1,
            grid=(1,),
            in_specs=[whole_block(*came.shape)],
            out_specs=whole_block(blocks, 24, STATE),
            scratch_shapes=[scratch] * 3,
        ),
        out_shape=jax.ShapeDtypeStruct((blocks, 24, STATE), bf16),
        name="owner",
        compiler_params=pltpu.CompilerParams(vmem_limit_bytes=6 << 20),
    )(lead, came)


def final_kernel(back, b_proj, x_in, tail_in, rows_in, x_inside, y_dots, b_inside, x_grad, b_grad, decay_grad):
    groups = x_in.shape[0] // GROUP
    pieces = GROUP // 16
    tokens = x_in.shape[1]
    heads = groups * PER_GROUP
    dots = []
    for g in range(groups):
        span = slice(g * GROUP, (g + 1) * GROUP)
        states = slice(g * STATE, (g + 1) * STATE)
        later = back[g * pieces : (g + 1) * pieces, 0:16, :].reshape(GROUP, STATE)
        carried = dot(later, b_proj[:, states], ((1,), (1,)))
        grad = x_inside[span, :] + carried * per_head(rows_in[1, g], 0)
        x_grad[:, span] = jnp.transpose(grad).astype(bf16)
        b_grad[:, states] = (
            b_inside[:, states] + dot(tail_in[span, :], later, ((0,), (0,)))
        ).astype(bf16)
        dots = dots + head_sums(x_in[span, :].astype(f32) * grad)
    own = jnp.concatenate([y_dots[g] for g in range(groups)], axis=0)
    own = own - jnp.concatenate(dots, axis=0)
    after = (grid_of(tokens, tokens, 0) >= grid_of(tokens, tokens, 1)).astype(f32)
    extra = jnp.sum(back[:, 16:24, :].astype(f32), axis=1)
    extra = jnp.sum(extra.reshape(heads, extra.shape[0] // heads, STATE), axis=1)
    decay_grad[...] = exact_dot(own, after, ((1,), (0,))) + extra


def final(back, b_proj, x, x_tail, rows, x_inside, y_dots, b_inside):
    inner, tokens = x.shape
    return whole_call(
        final_kernel,
        6 << 20,
        [
            ((tokens, inner), bf16),
            (b_proj.shape, bf16),
            ((inner // HEAD_DIM, tokens), f32),
        ],
        back, b_proj, x, x_tail, rows, x_inside, y_dots, b_inside,
    )


def body(
    mixer_output,
    layer_cotangent,
    expert_choice,
    route_weight,
    gate_pre,
    up_pre,
    w_gate,
    w_up,
    w_down,
    w_out,
    norm_gain,
    scan_in,
    gate_in,
    b_proj,
    c_proj,
    log_decay,
    entry_state,
):
    experts = lax.axis_size(SP)
    _, width = mixer_output.shape
    capacity = gate_pre.shape[1] // experts
    half = width // 2
    start = lax.axis_index("tp") * half

    side = lax.axis_index("tp")[None]
    send_grads, either = route(
        side, expert_choice.T, route_weight.T, layer_cotangent, experts * capacity
    )
    hidden_half = lax.dynamic_slice_in_dim(mixer_output, start, half, 1)
    cotangent_half = lax.dynamic_slice_in_dim(layer_cotangent, start, half, 1)
    send_hidden = dot(either, hidden_half, ((1,), (0,))).astype(bf16)
    send_grads = send_grads.reshape(experts, capacity, half)
    send_hidden = send_hidden.reshape(experts, capacity, half)
    inner = scan_in.shape[1]
    gain = norm_gain.astype(f32)[:, None]
    entry = entry_state.reshape(inner, STATE)
    mixed, *saved, x_tail, local, rows, inverse, carry, cotangent_rows = forward(
        scan_in, gate_in, b_proj, c_proj, log_decay.T, entry, gain, cotangent_half
    )
    gated, silu, slope, mix, decay, x = saved
    came_grads = lax.all_to_all(send_grads, SP, 0, 0, tiled=True)
    send_hidden, came_grads = lax.optimization_barrier((send_hidden, came_grads))
    came_hidden = lax.all_to_all(send_hidden, SP, 0, 0, tiled=True)
    grads_own = came_grads.reshape(-1, half)
    grads_far = swapped(grads_own)
    active, gate_grad, up_grad, rows_own, rows_far = expert_rows(
        side, grads_own, grads_far, gate_pre[0], up_pre[0], w_down[0], w_gate[0], w_up[0]
    )
    summed = (rows_own.astype(f32) + swapped(rows_far).astype(f32)).astype(bf16)
    summed, came_hidden = lax.optimization_barrier((summed, came_hidden))
    returned = lax.all_to_all(summed.reshape(experts, capacity, half), SP, 0, 0, tiled=True)
    hidden_own = came_hidden.reshape(-1, half)
    hidden_far = swapped(hidden_own)
    down_wgrad, gate_wgrad, up_wgrad = expert_weights(
        side, active, gate_grad, up_grad, grads_own, grads_far, hidden_own, hidden_far
    )
    moe_terms = dot(returned.reshape(-1, half), either, ((0,), (0,)))
    grad_own = (cotangent_rows.astype(f32) + moe_terms).astype(bf16)
    grad_far = swapped(grad_own)
    line, spot = lax.axis_size("sp_0"), lax.axis_index("sp_0")
    span = width // line
    near = lax.axis_index("tp") * (line // 2)
    grads_line = from_line(
        [
            lax.dynamic_slice_in_dim(
                grad_own, (lax.rem(spot + k, line) - near) * span, span, 0
            )
            for k in range(line)
        ],
        "sp_0",
    )
    message, grad_gated = state_message(
        side, grad_own, grad_far, w_out, gain, gated, silu, carry, c_proj, local, rows, inverse
    )
    came_states = lax.all_to_all(message, SP, 0, 0, tiled=True)
    lead = lax.rem(lax.axis_index(SP), HEAD_DIM // 16) == 0
    back = owner_scan(lead.astype(jnp.int32)[None], came_states)
    grad_gate_in, x_inside, b_inside, grad_c_proj, y_dots = inside_grads(
        grad_gated, gated, silu, slope, mix, decay, x, b_proj, c_proj, entry, rows
    )
    back = lax.all_to_all(back, SP, 0, 0, tiled=True)
    grad_scan_in, grad_b_proj, decay_grad = final(
        back, b_proj, x, x_tail, rows, x_inside, y_dots, b_inside
    )
    grad_log_decay = decay_grad.T

    mixed, gate_wgrad = lax.optimization_barrier((mixed, gate_wgrad))
    mixed_line = from_line([mixed] * line, "sp_0")
    own_line = jnp.concatenate(grads_line, axis=1)
    far_line = swapped(own_line)
    chosen = jnp.where(spot // 2 == lax.axis_index("tp"), own_line, far_line)
    product = dot(chosen, jnp.concatenate(mixed_line, axis=1), ((1,), (1,))).astype(bf16)
    parts = from_line(pieces_for(product, "sp_1", 0), "sp_1")
    product = sum(part.astype(f32) for part in parts).astype(bf16)
    parts = from_line(pieces_for(product, "sp_2", 0), "sp_2")
    grad_out_proj = sum(part.astype(f32) for part in parts)

    return (
        gate_wgrad[None],
        up_wgrad[None],
        down_wgrad[None],
        grad_out_proj,
        grad_scan_in,
        grad_gate_in,
        grad_b_proj,
        grad_c_proj,
        grad_log_decay,
    )


def solution(mesh):
    split = Mesh(mesh.devices.reshape(4, 4, 4, mesh.shape["tp"]), ("sp_0", "sp_1", "sp_2", "tp"))
    return jax.shard_map(
        body,
        mesh=split,
        in_specs=(
            P(SP, None),
            P(SP, None),
            P(SP, None),
            P(SP, None),
            P(SP, None, "tp"),
            P(SP, None, "tp"),
            P(SP, None, "tp"),
            P(SP, None, "tp"),
            P(SP, "tp", None),
            P("tp", None),
            P("tp"),
            P(SP, "tp"),
            P(SP, "tp"),
            P(SP, "tp"),
            P(SP, "tp"),
            P(SP, "tp"),
            P(SP, "tp", None, None),
        ),
        out_specs=(
            P(SP, None, "tp"),
            P(SP, None, "tp"),
            P(SP, "tp", None),
            P(SP, "tp"),
            P(SP, "tp"),
            P(SP, "tp"),
            P(SP, "tp"),
            P(SP, "tp"),
            P(SP, "tp"),
        ),
        check_vma=False,
    )
```

```python
import jax
import jax.numpy as jnp
from jax import lax
from jax.sharding import Mesh
from jax.experimental import pallas as pl
from jax.experimental.pallas import tpu as pltpu
from jax.sharding import PartitionSpec as P

HEAD_DIM = 64
STATE = 128
SP = ("sp_0", "sp_1", "sp_2")


rms_epsilon = 1e-05
clamp_limit = 7.0
swish_alpha = 1.702

bf16 = jnp.bfloat16
f32 = jnp.float32


def dot(a, b, dims):
    return lax.dot_general(a, b, (dims, ((), ())), preferred_element_type=f32)


def swapped(x):
    return lax.ppermute(x, "tp", [(0, 1), (1, 0)])


def from_line(parts, axis):
    size = lax.axis_size(axis)
    return [parts[0]] + [
        lax.ppermute(parts[k], axis, [(i, (i + k) % size) for i in range(size)])
        for k in range(1, size)
    ]


def pieces_for(x, axis, dim):
    size, spot = lax.axis_size(axis), lax.axis_index(axis)
    span = x.shape[dim] // size
    return [
        lax.dynamic_slice_in_dim(x, lax.rem(spot + k, size) * span, span, dim) for k in range(size)
    ]


def expert_rows_kernel(
    side, mine, other, gate_value, up_value, down_own, down_far, gate_own, gate_far, up_own, up_far,
    active, gate_grad, up_grad, rows_own, rows_far,
):
    act_grad = dot(mine[...], down_own[...], ((1,), (1,)))
    act_grad = act_grad + dot(other[...], down_far[...], ((1,), (1,)))
    gate_full = gate_value[...].astype(f32)
    up_full = up_value[...].astype(f32)
    gate_clip = jnp.minimum(gate_full, clamp_limit)
    up_clip = jnp.clip(up_full, -clamp_limit, clamp_limit)
    sigmoid_gate = jax.nn.sigmoid(swish_alpha * gate_clip)
    swish_gate = gate_clip * sigmoid_gate
    active[...] = ((up_clip + 1.0) * swish_gate).astype(bf16)
    inside = (up_full > -clamp_limit) & (up_full < clamp_limit)
    up_side = jnp.where(inside, act_grad * swish_gate, 0.0).astype(bf16)
    slope = sigmoid_gate + swish_alpha * gate_clip * sigmoid_gate * (1.0 - sigmoid_gate)
    gate_side = jnp.where(
        gate_full < clamp_limit, act_grad * (up_clip + 1.0) * slope, 0.0
    ).astype(bf16)
    up_grad[...] = up_side
    gate_grad[...] = gate_side
    far = dot(gate_side, gate_far[...], ((1,), (1,))) + dot(up_side, up_far[...], ((1,), (1,)))
    rows_far[...] = far.astype(bf16)
    own = dot(gate_side, gate_own[...], ((1,), (1,))) + dot(up_side, up_own[...], ((1,), (1,)))
    rows_own[...] = own.astype(bf16)


def whole_block(*shape):
    return pl.BlockSpec(shape, lambda i, side: (0,) * len(shape))


def expert_rows(side, mine, other, gate_value, up_value, w_down, w_gate, w_up):
    rows, half = mine.shape
    hidden = gate_value.shape[1]
    row_block = whole_block(rows, half)
    act_block = whole_block(rows, hidden)
    down = [
        pl.BlockSpec((hidden, half), lambda i, side: (0, side[0])),
        pl.BlockSpec((hidden, half), lambda i, side: (0, 1 - side[0])),
    ]
    tall = [
        pl.BlockSpec((half, hidden), lambda i, side: (side[0], 0)),
        pl.BlockSpec((half, hidden), lambda i, side: (1 - side[0], 0)),
    ]
    act = jax.ShapeDtypeStruct((rows, hidden), bf16)
    out = jax.ShapeDtypeStruct((rows, half), bf16)
    return pl.pallas_call(
        expert_rows_kernel,
        grid_spec=pltpu.PrefetchScalarGridSpec(
            num_scalar_prefetch=1,
            grid=(1,),
            in_specs=[row_block, row_block, act_block, act_block] + down + tall + tall,
            out_specs=[act_block] * 3 + [row_block] * 2,
        ),
        out_shape=[act] * 3 + [out] * 2,
        name="expert_rows",
    )(side, mine, other, gate_value, up_value, w_down, w_down, w_gate, w_gate, w_up, w_up)


def weights_kernel(
    side, active, gate_grad, up_grad, grads_own, grads_far, hidden_own, hidden_far,
    down_out, gate_out, up_out,
):
    def write(grads, hidden):
        down_out[...] = dot(active[...], grads, ((0,), (0,))).astype(bf16)
        gate_out[...] = dot(hidden, gate_grad[...], ((0,), (0,))).astype(bf16)
        up_out[...] = dot(hidden, up_grad[...], ((0,), (0,))).astype(bf16)

    @pl.when(pl.program_id(0) < 2)
    def _():
        write(grads_own[...], hidden_own[...])

    @pl.when(pl.program_id(0) >= 2)
    def _():
        write(grads_far[...], hidden_far[...])


def expert_weights(side, active, gate_grad, up_grad, grads_own, grads_far, hidden_own, hidden_far):
    rows, half = grads_own.shape
    hidden = active.shape[1]
    own = pl.BlockSpec((rows, half // 2), lambda i, side: (0, jnp.minimum(i, 1)))
    far = pl.BlockSpec((rows, half // 2), lambda i, side: (0, jnp.maximum(i - 2, 0)))

    def place(i, side):
        return lax.rem(i + 2 * side[0], 4)

    tall = pl.BlockSpec((half // 2, hidden), lambda i, side: (place(i, side), 0))
    return pl.pallas_call(
        weights_kernel,
        grid_spec=pltpu.PrefetchScalarGridSpec(
            num_scalar_prefetch=1,
            grid=(4,),
            in_specs=[whole_block(rows, hidden)] * 3 + [own, far, own, far],
            out_specs=[
                pl.BlockSpec((hidden, half // 2), lambda i, side: (0, place(i, side))),
                tall,
                tall,
            ],
        ),
        out_shape=[jax.ShapeDtypeStruct((hidden, 2 * half), bf16)]
        + [jax.ShapeDtypeStruct((2 * half, hidden), bf16)] * 2,
        name="weights",
    )(side, active, gate_grad, up_grad, grads_own, grads_far, hidden_own, hidden_far)


def exact_dot(a, b, dims):
    return lax.dot_general(
        a, b, (dims, ((), ())), preferred_element_type=f32, precision=lax.Precision.HIGHEST
    )


def grid_of(rows, columns, axis):
    return lax.broadcasted_iota(jnp.int32, (rows, columns), axis)


def route_kernel(side, choice, weight, cotangent, grads, places):
    tokens = choice.shape[1]
    slots = places.shape[0]
    experts = slots // 8
    expert_at = grid_of(experts, tokens, 0)
    hot = [(expert_at == choice[k : k + 1, :]).astype(f32) for k in range(2)]
    before = (grid_of(tokens, tokens, 0) < grid_of(tokens, tokens, 1)).astype(bf16)
    earlier = dot((hot[0] + hot[1]).astype(bf16), before, ((1,), (0,)))
    same = (grid_of(tokens, tokens, 0) == grid_of(tokens, tokens, 1)).astype(f32)
    weights = exact_dot(same, weight[...], ((1,), (1,)))
    cotangents = cotangent[...].astype(f32)
    slot_at = grid_of(slots, tokens, 0)
    either = jnp.zeros((slots, tokens), f32)
    sent = jnp.zeros((slots, cotangent.shape[1]), f32)
    for k in range(2):
        rank = jnp.sum(earlier * hot[k], axis=0, keepdims=True).astype(jnp.int32)
        taken = (slot_at == choice[k : k + 1, :] * 8 + rank).astype(f32)
        either = either + taken
        rows = (weights[:, k : k + 1] * cotangents).astype(bf16)
        sent = sent + dot(taken.astype(bf16), rows, ((1,), (0,)))
    grads[...] = sent.astype(bf16)
    places[...] = either.astype(bf16)


def route(side, choice, weight, cotangent, slots):
    tokens, width = cotangent.shape
    half = width // 2
    return pl.pallas_call(
        route_kernel,
        grid_spec=pltpu.PrefetchScalarGridSpec(
            num_scalar_prefetch=1,
            grid=(1,),
            in_specs=[
                whole_block(*choice.shape),
                whole_block(*weight.shape),
                pl.BlockSpec((tokens, half), lambda i, side: (0, side[0])),
            ],
            out_specs=[whole_block(slots, half), whole_block(slots, tokens)],
        ),
        out_shape=[
            jax.ShapeDtypeStruct((slots, half), bf16),
            jax.ShapeDtypeStruct((slots, tokens), bf16),
        ],
        name="route",
    )(side, choice, weight, cotangent)


GROUP = 256
PER_GROUP = GROUP // HEAD_DIM


def per_head(rows, first):
    return jnp.concatenate(
        [
            jnp.broadcast_to(rows[first + r : first + r + 1, :], (HEAD_DIM, rows.shape[1]))
            for r in range(PER_GROUP)
        ],
        axis=0,
    )


def head_sums(x):
    return [
        jnp.sum(x[r * HEAD_DIM : (r + 1) * HEAD_DIM, :], axis=0, keepdims=True)
        for r in range(PER_GROUP)
    ]


def forward_kernel(
    scan_in, gate_in, b_proj, c_proj, log_decay, entry, gain, cotangent,
    mixed, gated_out, silu_out, slope_out, mix_out, decay_out, x_out, tail_out, local_out,
    rows_out, inverse_out, carry_out, cotangent_out,
):
    tokens = scan_in.shape[0]
    groups = scan_in.shape[1] // GROUP
    down, across = grid_of(tokens, tokens, 0), grid_of(tokens, tokens, 1)
    decays = log_decay[...]
    cum_rows = exact_dot(decays, (down <= across).astype(f32), ((1,), (0,)))
    cum_columns = exact_dot((across <= down).astype(f32), decays, ((1,), (1,)))
    total = cum_rows[:, tokens - 1 :]
    growth = jnp.exp(cum_rows)
    tail = jnp.exp(total - cum_rows)
    totals = jnp.broadcast_to(total, growth.shape)
    causal = down >= across
    for g in range(groups):
        span = slice(g * GROUP, (g + 1) * GROUP)
        states = slice(g * STATE, (g + 1) * STATE)
        first = g * PER_GROUP
        b_group, c_group = b_proj[:, states], c_proj[:, states]
        inner = dot(c_group, b_group, ((1,), (1,)))
        x = jnp.transpose(scan_in[:, span].astype(f32))
        x_b = x.astype(bf16)
        carried = dot(entry[span, :].astype(bf16), c_group, ((1,), (1,)))
        within = []
        for r in range(PER_GROUP):
            h = first + r
            gaps = cum_columns[:, h : h + 1] - cum_rows[h : h + 1, :]
            decay = jnp.where(causal, jnp.exp(jnp.where(causal, gaps, 0.0)), 0.0)
            decay_out[h] = decay
            mix = (inner * decay).astype(bf16)
            mix_out[h] = mix
            within.append(dot(x_b[r * HEAD_DIM : (r + 1) * HEAD_DIM, :], mix, ((1,), (1,))))
        carried = carried * per_head(growth, first)
        scan_out = jnp.concatenate(within, axis=0) + carried
        gate = jnp.transpose(gate_in[:, span].astype(f32))
        sig = jax.nn.sigmoid(gate)
        silu = gate * sig
        gated = scan_out * silu
        inverse = lax.rsqrt(jnp.mean(gated * gated, axis=0, keepdims=True) + rms_epsilon)
        mixed[span, :] = (gated * inverse * gain[span, :]).astype(bf16)
        gated_out[span, :] = gated
        silu_out[span, :] = silu
        slope_out[span, :] = scan_out * sig * (1.0 + gate * (1.0 - sig))
        carry_out[span, :] = carried * silu
        cotangent_out[span, :] = jnp.transpose(cotangent[:, span].astype(f32)).astype(bf16)
        inverse_out[g] = inverse
        for k, part in enumerate((growth, tail, totals)):
            rows_out[k, g] = part[first : first + PER_GROUP, :]
        x_out[span, :] = x_b
        x_tail = (x * per_head(tail, first)).astype(bf16)
        tail_out[span, :] = x_tail
        local_out[span, :] = dot(x_tail, b_group, ((1,), (0,))).astype(bf16)


def whole_call(kernel, limit, out_shape, *args):
    return pl.pallas_call(
        kernel,
        out_shape=[jax.ShapeDtypeStruct(*x) for x in out_shape],
        compiler_params=pltpu.CompilerParams(vmem_limit_bytes=limit),
    )(*args)


def forward(scan_in, gate_in, b_proj, c_proj, log_decay, entry, gain, cotangent):
    tokens, inner = scan_in.shape
    heads = log_decay.shape[0]
    return whole_call(
        forward_kernel,
        None,
        [
            ((inner, tokens), bf16),
            ((inner, tokens), f32),
            ((inner, tokens), f32),
            ((inner, tokens), f32),
            ((heads, tokens, tokens), bf16),
            ((heads, tokens, tokens), f32),
            ((inner, tokens), bf16),
            ((inner, tokens), bf16),
            ((inner, STATE), bf16),
            ((3, inner // GROUP, PER_GROUP, tokens), f32),
            ((inner // GROUP, 1, tokens), f32),
            ((inner, tokens), f32),
            ((cotangent.shape[1], tokens), bf16),
        ],
        scan_in, gate_in, b_proj, c_proj, log_decay, entry, gain, cotangent,
    )


def spread_parts(x, heads, pieces):
    high = x.astype(bf16)
    rest = x - high.astype(f32)
    middle = rest.astype(bf16)
    low = (rest - middle.astype(f32)).astype(bf16)
    return [
        jnp.broadcast_to(part.astype(f32)[:, None, :], (heads, pieces, STATE)).reshape(
            heads * pieces, 1, STATE
        )
        for part in (high, middle, low)
    ]


def message_kernel(
    side, grad_own, grad_far, out_own, out_far, gain, gated_in, silu_in, carry_in, c_proj, local_in,
    rows_in, inverse_in,
    message, grad_out,
):
    pieces = GROUP // 16
    grad_mixed = dot(out_own[...], grad_own[...], ((1,), (0,)))
    grad_mixed = grad_mixed + dot(out_far[...], grad_far[...], ((1,), (0,)))
    inverse = inverse_in[0]
    unit = gated_in[...] * inverse
    grad_unit = grad_mixed * gain[...]
    mean = jnp.mean(grad_unit * unit, axis=0, keepdims=True)
    grad_gated = inverse * (grad_unit - unit * mean)
    grad_out[...] = grad_gated
    grown = (grad_gated * silu_in[...] * per_head(rows_in[0, 0], 0)).astype(bf16)
    block_state = dot(grown, c_proj[...], ((1,), (0,))).astype(bf16)
    message[:, 0:16, :] = block_state.reshape(pieces, 16, STATE)
    message[:, 16:32, :] = local_in[...].reshape(pieces, 16, STATE)
    own = jnp.concatenate(head_sums(grad_gated * carry_in[...]), axis=0)
    own = jnp.broadcast_to(jnp.sum(own, axis=1, keepdims=True), (PER_GROUP, STATE))
    per = pieces // PER_GROUP
    zero = jnp.zeros((pieces, 2, STATE), f32)
    extra = jnp.concatenate(
        spread_parts(rows_in[2, 0], PER_GROUP, per) + spread_parts(own, PER_GROUP, per) + [zero],
        axis=1,
    )
    message[:, 32:40, :] = extra.astype(bf16)


def state_message(side, grad_own, grad_far, w_out, gain, gated, silu, carry, c_proj, local, rows, inverse):
    half, tokens = grad_own.shape
    inner = gain.shape[0]
    pieces = GROUP // 16
    channels = pl.BlockSpec((GROUP, tokens), lambda i, side: (i, 0))
    return pl.pallas_call(
        message_kernel,
        grid_spec=pltpu.PrefetchScalarGridSpec(
            num_scalar_prefetch=1,
            grid=(inner // GROUP,),
            in_specs=[
                whole_block(half, tokens),
                whole_block(half, tokens),
                pl.BlockSpec((GROUP, half), lambda i, side: (i, side[0])),
                pl.BlockSpec((GROUP, half), lambda i, side: (i, 1 - side[0])),
                pl.BlockSpec((GROUP, 1), lambda i, side: (i, 0)),
                channels,
                channels,
                channels,
                pl.BlockSpec((tokens, STATE), lambda i, side: (0, i)),
                pl.BlockSpec((GROUP, STATE), lambda i, side: (i, 0)),
                pl.BlockSpec((3, 1, PER_GROUP, tokens), lambda i, side: (0, i, 0, 0)),
                pl.BlockSpec((1, 1, tokens), lambda i, side: (i, 0, 0)),
            ],
            out_specs=[
                pl.BlockSpec((pieces, 40, STATE), lambda i, side: (i, 0, 0)),
                channels,
            ],
        ),
        out_shape=[
            jax.ShapeDtypeStruct((inner // 16, 40, STATE), bf16),
            jax.ShapeDtypeStruct((inner, tokens), f32),
        ],
        name="message",
    )(side, grad_own, grad_far, w_out, w_out, gain, gated, silu, carry, c_proj, local, rows, inverse)


def inside_kernel(
    grad_in, gated_in, silu_in, slope_in, mix_in, decay_in, x_in, b_proj, c_proj, entry, rows_in,
    gate_grad, packed, c_grad,
):
    tokens = x_in.shape[1]
    grad_gated = grad_in[...]
    gate_grad[...] = jnp.transpose(grad_gated * slope_in[...]).astype(bf16)
    grad_y = grad_gated * silu_in[...]
    grad_y_b = grad_y.astype(bf16)
    grown = (grad_y * per_head(rows_in[0, 0], 0)).astype(bf16)
    x = x_in[...]
    weights = jnp.zeros((tokens, tokens), f32)
    inside = []
    for r in range(PER_GROUP):
        head = slice(r * HEAD_DIM, (r + 1) * HEAD_DIM)
        inside.append(dot(grad_y_b[head, :], mix_in[r], ((1,), (0,))))
        weights = weights + decay_in[r] * dot(grad_y_b[head, :], x[head, :], ((0,), (0,)))
    packed[0, :GROUP, :] = jnp.concatenate(inside, axis=0)
    weights = weights.astype(bf16)
    c_grad[...] = (
        dot(weights, b_proj[...], ((1,), (0,)))
        + dot(grown, entry[...].astype(bf16), ((0,), (0,)))
    ).astype(bf16)
    packed[0, GROUP : GROUP + tokens, :] = dot(weights, c_proj[...], ((0,), (0,)))
    dots = head_sums(grad_gated * gated_in[...])
    zero = jnp.zeros((8 - PER_GROUP, tokens), f32)
    packed[0, GROUP + tokens :, :] = jnp.concatenate(dots + [zero], axis=0)


def inside_grads(grad, gated, silu, slope, mix, decay, x, b_proj, c_proj, entry, rows):
    inner, tokens = grad.shape
    channels = pl.BlockSpec((GROUP, tokens), lambda i: (i, 0))
    tokens_by = pl.BlockSpec((tokens, STATE), lambda i: (0, i))
    square = pl.BlockSpec((PER_GROUP, tokens, tokens), lambda i: (i, 0, 0))
    outs = [
        ((tokens, inner), bf16),
        ((inner // GROUP, GROUP + tokens + 8, tokens), f32),
        (b_proj.shape, bf16),
    ]
    return pl.pallas_call(
        inside_kernel,
        grid=(inner // GROUP,),
        in_specs=[channels] * 4
        + [square] * 2
        + [channels, tokens_by, tokens_by, pl.BlockSpec((GROUP, STATE), lambda i: (i, 0))]
        + [pl.BlockSpec((3, 1, PER_GROUP, tokens), lambda i: (0, i, 0, 0))],
        out_specs=[
            pl.BlockSpec((tokens, GROUP), lambda i: (0, i)),
            pl.BlockSpec((1, GROUP + tokens + 8, tokens), lambda i: (i, 0, 0)),
            tokens_by,
        ],
        out_shape=[jax.ShapeDtypeStruct(*x) for x in outs],
        name="inside",
    )(grad, gated, silu, slope, mix, decay, x, b_proj, c_proj, entry, rows)


def owner_kernel(lead, came, back, values, local, later):
    blocks = came.shape[0]
    values[...] = came[:, 0:16, :].astype(f32)
    local[...] = came[:, 16:32, :].astype(f32)
    extra = came[:, 32:40, :].astype(f32)
    first, second = grid_of(blocks, blocks, 0), grid_of(blocks, blocks, 1)
    after = (second > first).astype(bf16)
    gaps = jnp.zeros((blocks, blocks), f32)
    for k in range(3):
        part = jnp.where(first < second, extra[:, k, :blocks], 0.0).astype(bf16)
        gaps = gaps + dot(after, part, ((1,), (0,)))
    weights = jnp.where(second > first, jnp.exp(gaps), 0.0)
    high = weights.astype(bf16)
    low = (weights - high.astype(f32)).astype(bf16)
    total = jnp.zeros((blocks, STATE), f32)
    for r in range(16):
        piece = values[:, r, :].astype(bf16)
        found = dot(high, piece, ((1,), (0,))) + dot(low, piece, ((1,), (0,)))
        later[:, r, :] = found
        total = total + found * local[:, r, :]
    total = jnp.broadcast_to(jnp.sum(total, axis=1, keepdims=True), (blocks, STATE))
    sums = extra[:, 3, :] + extra[:, 4, :] + extra[:, 5, :]
    own = jnp.where(lead[0] == 1, sums, 0.0) - total
    carried = exact_dot(after.astype(f32), own, ((1,), (0,)))
    back[:, 0:16, :] = later[...].astype(bf16)
    zero = jnp.zeros((blocks, 5, STATE), f32)
    back[:, 16:24, :] = jnp.concatenate(spread_parts(carried, blocks, 1) + [zero], axis=1).astype(
        bf16
    )


def owner_scan(lead, came):
    blocks = came.shape[0]
    scratch = pltpu.VMEM((blocks, 16, STATE), f32)
    return pl.pallas_call(
        owner_kernel,
        grid_spec=pltpu.PrefetchScalarGridSpec(
            num_scalar_prefetch=1,
            grid=(1,),
            in_specs=[whole_block(*came.shape)],
            out_specs=whole_block(blocks, 24, STATE),
            scratch_shapes=[scratch] * 3,
        ),
        out_shape=jax.ShapeDtypeStruct((blocks, 24, STATE), bf16),
        name="owner",
        compiler_params=pltpu.CompilerParams(vmem_limit_bytes=6 << 20),
    )(lead, came)


def final_kernel(back, b_proj, x_in, tail_in, rows_in, packed, x_grad, b_grad, decay_grad):
    groups = x_in.shape[0] // GROUP
    pieces = GROUP // 16
    tokens = x_in.shape[1]
    heads = groups * PER_GROUP
    dots = []
    for g in range(groups):
        span = slice(g * GROUP, (g + 1) * GROUP)
        states = slice(g * STATE, (g + 1) * STATE)
        later = back[g * pieces : (g + 1) * pieces, 0:16, :].reshape(GROUP, STATE)
        carried = dot(later, b_proj[:, states], ((1,), (1,)))
        grad = packed[g, :GROUP, :] + carried * per_head(rows_in[1, g], 0)
        x_grad[:, span] = jnp.transpose(grad).astype(bf16)
        b_grad[:, states] = (
            packed[g, GROUP : GROUP + tokens, :] + dot(tail_in[span, :], later, ((0,), (0,)))
        ).astype(bf16)
        dots = dots + head_sums(x_in[span, :].astype(f32) * grad)
    lowest = GROUP + tokens
    own = jnp.concatenate(
        [packed[g, lowest : lowest + PER_GROUP, :] for g in range(groups)], axis=0
    )
    own = own - jnp.concatenate(dots, axis=0)
    after = (grid_of(tokens, tokens, 0) >= grid_of(tokens, tokens, 1)).astype(f32)
    extra = jnp.sum(back[:, 16:24, :].astype(f32), axis=1)
    extra = jnp.sum(extra.reshape(heads, extra.shape[0] // heads, STATE), axis=1)
    decay_grad[...] = exact_dot(own, after, ((1,), (0,))) + extra


def final(back, b_proj, x, x_tail, rows, packed):
    inner, tokens = x.shape
    return whole_call(
        final_kernel,
        6 << 20,
        [
            ((tokens, inner), bf16),
            (b_proj.shape, bf16),
            ((inner // HEAD_DIM, tokens), f32),
        ],
        back, b_proj, x, x_tail, rows, packed,
    )


def body(
    mixer_output,
    layer_cotangent,
    expert_choice,
    route_weight,
    gate_pre,
    up_pre,
    w_gate,
    w_up,
    w_down,
    w_out,
    norm_gain,
    scan_in,
    gate_in,
    b_proj,
    c_proj,
    log_decay,
    entry_state,
):
    experts = lax.axis_size(SP)
    _, width = mixer_output.shape
    capacity = gate_pre.shape[1] // experts
    half = width // 2
    start = lax.axis_index("tp") * half

    side = lax.axis_index("tp")[None]
    send_grads, either = route(
        side, expert_choice.T, route_weight.T, layer_cotangent, experts * capacity
    )
    hidden_half = lax.dynamic_slice_in_dim(mixer_output, start, half, 1)
    cotangent_half = lax.dynamic_slice_in_dim(layer_cotangent, start, half, 1)
    send_hidden = dot(either, hidden_half, ((1,), (0,))).astype(bf16)
    send_grads = send_grads.reshape(experts, capacity, half)
    send_hidden = send_hidden.reshape(experts, capacity, half)
    inner = scan_in.shape[1]
    gain = norm_gain.astype(f32)[:, None]
    entry = entry_state.reshape(inner, STATE)
    mixed, *saved, x_tail, local, rows, inverse, carry, cotangent_rows = forward(
        scan_in, gate_in, b_proj, c_proj, log_decay.T, entry, gain, cotangent_half
    )
    gated, silu, slope, mix, decay, x = saved
    came_grads = lax.all_to_all(send_grads, SP, 0, 0, tiled=True)
    send_hidden, came_grads = lax.optimization_barrier((send_hidden, came_grads))
    came_hidden = lax.all_to_all(send_hidden, SP, 0, 0, tiled=True)
    grads_own = came_grads.reshape(-1, half)
    grads_far = swapped(grads_own)
    active, gate_grad, up_grad, rows_own, rows_far = expert_rows(
        side, grads_own, grads_far, gate_pre[0], up_pre[0], w_down[0], w_gate[0], w_up[0]
    )
    summed = (rows_own.astype(f32) + swapped(rows_far).astype(f32)).astype(bf16)
    summed, came_hidden = lax.optimization_barrier((summed, came_hidden))
    returned = lax.all_to_all(summed.reshape(experts, capacity, half), SP, 0, 0, tiled=True)
    hidden_own = came_hidden.reshape(-1, half)
    hidden_far = swapped(hidden_own)
    down_wgrad, gate_wgrad, up_wgrad = expert_weights(
        side, active, gate_grad, up_grad, grads_own, grads_far, hidden_own, hidden_far
    )
    moe_terms = dot(returned.reshape(-1, half), either, ((0,), (0,)))
    grad_own = (cotangent_rows.astype(f32) + moe_terms).astype(bf16)
    grad_far = swapped(grad_own)
    line, spot = lax.axis_size("sp_0"), lax.axis_index("sp_0")
    span = width // line
    near = lax.axis_index("tp") * (line // 2)
    grads_line = from_line(
        [
            lax.dynamic_slice_in_dim(
                grad_own, (lax.rem(spot + k, line) - near) * span, span, 0
            )
            for k in range(line)
        ],
        "sp_0",
    )
    message, grad_gated = state_message(
        side, grad_own, grad_far, w_out, gain, gated, silu, carry, c_proj, local, rows, inverse
    )
    came_states = lax.all_to_all(message, SP, 0, 0, tiled=True)
    lead = lax.rem(lax.axis_index(SP), HEAD_DIM // 16) == 0
    back = owner_scan(lead.astype(jnp.int32)[None], came_states)
    grad_gate_in, packed, grad_c_proj = inside_grads(
        grad_gated, gated, silu, slope, mix, decay, x, b_proj, c_proj, entry, rows
    )
    back = lax.all_to_all(back, SP, 0, 0, tiled=True)
    grad_scan_in, grad_b_proj, decay_grad = final(
        back, b_proj, x, x_tail, rows, packed
    )
    grad_log_decay = decay_grad.T

    mixed, gate_wgrad = lax.optimization_barrier((mixed, gate_wgrad))
    mixed_line = from_line([mixed] * line, "sp_0")
    own_line = jnp.concatenate(grads_line, axis=1)
    far_line = swapped(own_line)
    chosen = jnp.where(spot // 2 == lax.axis_index("tp"), own_line, far_line)
    product = dot(chosen, jnp.concatenate(mixed_line, axis=1), ((1,), (1,))).astype(bf16)
    parts = from_line(pieces_for(product, "sp_1", 0), "sp_1")
    product = sum(part.astype(f32) for part in parts).astype(bf16)
    parts = from_line(pieces_for(product, "sp_2", 0), "sp_2")
    grad_out_proj = sum(part.astype(f32) for part in parts)

    return (
        gate_wgrad[None],
        up_wgrad[None],
        down_wgrad[None],
        grad_out_proj,
        grad_scan_in,
        grad_gate_in,
        grad_b_proj,
        grad_c_proj,
        grad_log_decay,
    )


def solution(mesh):
    split = Mesh(mesh.devices.reshape(4, 4, 4, mesh.shape["tp"]), ("sp_0", "sp_1", "sp_2", "tp"))
    return jax.shard_map(
        body,
        mesh=split,
        in_specs=(
            P(SP, None),
            P(SP, None),
            P(SP, None),
            P(SP, None),
            P(SP, None, "tp"),
            P(SP, None, "tp"),
            P(SP, None, "tp"),
            P(SP, None, "tp"),
            P(SP, "tp", None),
            P("tp", None),
            P("tp"),
            P(SP, "tp"),
            P(SP, "tp"),
            P(SP, "tp"),
            P(SP, "tp"),
            P(SP, "tp"),
            P(SP, "tp", None, None),
        ),
        out_specs=(
            P(SP, None, "tp"),
            P(SP, None, "tp"),
            P(SP, "tp", None),
            P(SP, "tp"),
            P(SP, "tp"),
            P(SP, "tp"),
            P(SP, "tp"),
            P(SP, "tp"),
            P(SP, "tp"),
        ),
        check_vma=False,
    )
```
